32 devices in a mesh: ep: 8 (over z, x), tp: 4 (over y, core).
Axes of the slice: x: 2, y: 2, z: 4, core: 2. Of those that a mesh axis runs over, the one named last changes fastest.
Arguments:
- pool_input: bfloat16 [4096, 1024], P('ep', 'tp'), may hold values from -6 to 6
- group_weight: bfloat16 [4, 256, 256], P('tp'), may hold values from -0.375 to 0.375
- pool_scale: float32 [1024], P('tp'), may hold values from 0.1 to 1.9
- out_weight: bfloat16 [1024, 2048], P('tp'), may hold values from -0.1875 to 0.1875
- mix_gain: float32 [2048], replicated, may hold values from 0.1 to 1.9
- expert_input: bfloat16 [8192, 2048], P(('ep', 'tp')), may hold values from -6 to 6
- routes: int32 [8192, 2], P('ep'), may hold values from 0 to 15, all different within a row; in each aligned block of 256 rows (0 to 255, 256 to 511, ...) at most 40 rows name the same one
- route_weights: float32 [8192, 2], P('ep'), may hold values from 0.2 to 2.5
- moe_in_gain: float32 [2048], replicated, may hold values from 0.1 to 1.9
- gate_weight: bfloat16 [16, 2048, 1024], P('ep', None, 'tp'), may hold values from -0.125 to 0.125
- up_weight: bfloat16 [16, 2048, 1024], P('ep', None, 'tp'), may hold values from -0.125 to 0.125
- down_weight: bfloat16 [16, 1024, 2048], P('ep', 'tp'), may hold values from -0.1875 to 0.1875
- moe_out_gain: float32 [2048], replicated, may hold values from 0.1 to 1.9
Outputs:
- mixer_out: bfloat16 [4096, 2048], P(('ep', 'tp'))
- moe_out: bfloat16 [8192, 2048], P(('ep', 'tp'))
The draws below stay inside these ranges and needn't reach their ends.
Inputs may be any that keep to these rules, and one draw needn't show every extreme that they name: `routes`: each row names 2 different experts. In each aligned block of 256 rows no expert is named by more than 40 rows, a bound that some block reaches.
All inputs are finite; a program needn't handle non-finite values.
Results may differ from the reference program's by a relative error of at most 0.013.
Values may be sent and summed in bfloat16 or wider, within the bound.
A program may use at most 128 MiB of HBM per device.

```python
import math
from functools import partial
import jax
import jax.numpy as jnp
import numpy as np
from jax import lax

D = 2048
GROUPS = 4
GW = 256
PW = 1024
FF = 1024
FF_BLK = 256
EXPERTS = 16
TOPK = 2
TOKB_DEV = 256
CAP = 40
TOKENS_A = 4096
TOKENS_B = 8192
N_TP = 4


def block_levels(key, shape, shards, smallest, high):
    gain, own = 1.0, jax.random.fold_in(key, 6)
    for dim, blocks in shards:
        steps = jnp.exp(jax.random.uniform(jax.random.fold_in(own, dim), (blocks,), jnp.float32, smallest / len(shards), high / len(shards)))
        gain = gain * jnp.repeat(steps, shape[dim] // blocks).reshape([-1 if axis == dim else 1 for axis in range(len(shape))])
    return gain


def deal_out(key, own, number, rows, number_of, top, most, slope):
    ranking = jax.random.permutation(key, number_of)
    crowded, usual = shares(number_of, rows * top, most, slope, True), shares(number_of, rows * top, most, slope, False)
    places = jnp.arange(number_of)

    def named(sizes, rotation):
        used = int((sizes > 0).sum())
        fixed = max(1, used // 4)
        passed = fixed + (places - fixed + rotation * (used - fixed)) % max(1, number_of - fixed)
        return jnp.zeros((number_of,), jnp.int32).at[ranking[jnp.where(places < fixed, places, passed)]].set(jnp.asarray(sizes, jnp.int32))

    sizes = jnp.where(number % 4 == 0, named(crowded, number // 4), named(usual, number - number // 4 - 1))
    mixed = jax.random.permutation(jax.random.fold_in(own, 3), number_of)
    donor, sink = mixed[0:number_of // 2 * 2:2], mixed[1:number_of // 2 * 2:2]
    margin = jnp.minimum(sizes[donor] - 1, most - sizes[sink]) // 2
    margin = jnp.where((donor == ranking[0]) | (sink == ranking[0]) | (sizes[sink] == 0), 0, jnp.maximum(margin, 0))
    passed = jax.random.randint(jax.random.fold_in(own, 4), (number_of // 2,), 0, 1 << 20) % (margin + 1)
    sizes = sizes.at[donor].add(-passed).at[sink].add(passed)
    items = jnp.searchsorted(jnp.cumsum(sizes), jnp.arange(rows * top), side="right").astype(jnp.int32)
    grid = items.reshape(top, rows).T
    grid = grid[jax.random.permutation(jax.random.fold_in(own, 1), rows)]
    rotation = jax.random.randint(jax.random.fold_in(own, 2), (rows, 1), 0, top)
    return jnp.take_along_axis(grid, (jnp.arange(top)[None, :] + rotation) % top, axis=1)


def shares(number_of, total, bound, skew, full):
    portions = [(1 << 20) // math.isqrt(rank ** skew) + 1 for rank in range(1, number_of + 1)]
    largest = bound if full else min(bound, max(-(-total // number_of), total * portions[0] // sum(portions)))
    least = 1 if total - largest >= number_of - 1 else 0
    given, rest = [largest] + [least] * (number_of - 1), total - largest - least * (number_of - 1)
    while rest > 0:
        movable = [i for i in range(1, number_of) if given[i] < largest] or [i for i in range(1, number_of) if given[i] < bound]
        whole, remaining = sum([portions[i] for i in movable]), rest
        for i in movable:
            more = min(bound - given[i], max(1, remaining * portions[i] // whole), rest)
            given[i] = given[i] + more
            rest = rest - more
    return np.array(given)


def scatter_about(own_key, dims, scale, bound, split=(), kind=jnp.bfloat16):
    entries = scale * jax.random.normal(own_key, dims, jnp.float32)
    if split:
        entries = entries * block_levels(own_key, dims, split, -0.22, 0.18)
    return jnp.clip(entries, -bound, bound).astype(kind)


def setup_inputs(seed: int = 0) -> dict:
    key_list = jax.random.split(jax.random.key(seed), 14)
    pool_input = scatter_about(key_list[0], (TOKENS_A, PW), 1.0, 6.0, ((0, 8), (1, 4)))
    group_weight = scatter_about(key_list[1], (GROUPS, GW, GW), GW ** -0.5, 0.375, ((0, 4),))
    pool_scale = jnp.clip(1.0 + 0.18 * jax.random.normal(key_list[2], (PW,), jnp.float32), 0.1, 1.9)
    out_weight = scatter_about(key_list[3], (PW, D), PW ** -0.5, 0.1875, ((0, 4),))
    mix_gain = jnp.clip(1.0 + 0.18 * jax.random.normal(key_list[4], (D,), jnp.float32), 0.1, 1.9)
    expert_input = scatter_about(key_list[5], (TOKENS_B, D), 1.0, 6.0, ((0, 32),))
    routes_keys = jax.random.split(jax.random.fold_in(key_list[6], 1), TOKENS_B // TOKB_DEV)
    routes_turns = jax.random.permutation(jax.random.fold_in(key_list[6], 3), TOKENS_B // TOKB_DEV)
    routes = jax.vmap(lambda own, number: deal_out(jax.random.fold_in(key_list[6], 2), own, number, TOKB_DEV, EXPERTS, TOPK, CAP, 1))(routes_keys, routes_turns).reshape((TOKENS_B, TOPK))
    route_weights = jnp.clip(jnp.exp(math.log(2.5) - 2.5257286 * jax.random.uniform(key_list[7], (TOKENS_B, TOPK), jnp.float32) ** block_levels(key_list[7], (TOKENS_B, TOPK), ((0, 8),), -0.2, 0.2)), 0.2, 2.5)
    moe_in_gain = jnp.clip(1.0 + 0.18 * jax.random.normal(key_list[8], (D,), jnp.float32), 0.1, 1.9)
    gate_weight = scatter_about(key_list[9], (EXPERTS, D, FF), D ** -0.5, 0.125, ((0, 8), (2, 4)))
    up_weight = scatter_about(key_list[10], (EXPERTS, D, FF), D ** -0.5, 0.125, ((0, 8), (2, 4)))
    down_weight = scatter_about(key_list[11], (EXPERTS, FF, D), FF ** -0.5, 0.1875, ((0, 8), (1, 4)))
    moe_out_gain = jnp.clip(1.0 + 0.18 * jax.random.normal(key_list[12], (D,), jnp.float32), 0.1, 1.9)
    return {"pool_input": pool_input, "group_weight": group_weight, "pool_scale": pool_scale, "out_weight": out_weight, "mix_gain": mix_gain, "expert_input": expert_input, "routes": routes, "route_weights": route_weights, "moe_in_gain": moe_in_gain, "gate_weight": gate_weight, "up_weight": up_weight, "down_weight": down_weight, "moe_out_gain": moe_out_gain}


NORM_EPS = 1e-06

def rms_scale(values, gain_vec):
    mean_sq = lax.optimization_barrier(jnp.mean(values * values, axis=-1, keepdims=True))
    return values * lax.rsqrt(mean_sq + NORM_EPS) * gain_vec.astype(jnp.float32)

def pool_group(block_in, window):
    row_total = block_in.shape[0]
    values = block_in.astype(jnp.float32)
    padded = jnp.pad(values, ((window - 1, 0), (0, 0)))
    summed = jnp.zeros_like(values)
    for lag_step in range(window):
        summed = summed + padded[window - 1 - lag_step:window - 1 - lag_step + row_total]
    divisor = jnp.minimum(jnp.arange(row_total) + 1, window).astype(jnp.float32)[:, None]
    return (summed / divisor - values).astype(jnp.bfloat16)

def slot_numbers(route_block, experts, capacity):
    flat_routes = route_block.reshape(-1).astype(jnp.int32)
    one_hot = (flat_routes[:, None] == jnp.arange(experts, dtype=jnp.int32)[None, :]).astype(jnp.int32)
    slot_rank = lax.optimization_barrier(jnp.sum((jnp.cumsum(one_hot, axis=0) - one_hot) * one_hot, axis=1))
    return (flat_routes * capacity + slot_rank).astype(jnp.int32)

def fill_table(slot_ids, payload, empty_value, slots_total):
    return jnp.full((slots_total,), empty_value, payload.dtype).at[slot_ids].set(payload)

def reference(pool_input, group_weight, pool_scale, out_weight, mix_gain, expert_input, routes, route_weights, moe_in_gain, gate_weight, up_weight, down_weight, moe_out_gain):
    projected = jnp.zeros((TOKENS_A, D), jnp.float32)
    for group_idx in range(GROUPS):
        lo_col = group_idx * GW
        pooled = pool_group(pool_input[:, lo_col:lo_col + GW], 2 ** (group_idx + 1))
        grouped = (jnp.dot(pooled, group_weight[group_idx], preferred_element_type=jnp.float32) * pool_scale[lo_col:lo_col + GW].astype(jnp.float32)).astype(jnp.bfloat16)
        partial_mix = jnp.dot(grouped, out_weight[lo_col:lo_col + GW], preferred_element_type=jnp.float32).astype(jnp.bfloat16)
        projected = projected + partial_mix.astype(jnp.float32)
    mixer_out = rms_scale(projected, mix_gain).astype(jnp.bfloat16)
    normed = rms_scale(expert_input.astype(jnp.float32), moe_in_gain).astype(jnp.bfloat16)
    blocks = TOKENS_B // TOKB_DEV
    pairs = TOKB_DEV * TOPK
    route_blocks = routes.reshape(blocks, TOKB_DEV, TOPK)
    slot_ids = jax.vmap(partial(slot_numbers, experts=EXPERTS, capacity=CAP))(route_blocks)
    pair_token = (jnp.arange(blocks, dtype=jnp.int32)[:, None] * TOKB_DEV + jnp.arange(pairs, dtype=jnp.int32)[None, :] // TOPK).astype(jnp.int32)
    token_table = jax.vmap(partial(fill_table, empty_value=TOKENS_B, slots_total=EXPERTS * CAP))(slot_ids, pair_token)
    weight_table = jax.vmap(partial(fill_table, empty_value=0.0, slots_total=EXPERTS * CAP))(slot_ids, route_weights.reshape(blocks, pairs))
    token_table = token_table.reshape(blocks, EXPERTS, CAP).transpose(1, 0, 2).reshape(EXPERTS, blocks * CAP)
    weight_table = weight_table.reshape(blocks, EXPERTS, CAP).transpose(1, 0, 2).reshape(EXPERTS, blocks * CAP)
    padded_rows = jnp.concatenate([normed, jnp.zeros((1, D), jnp.bfloat16)], axis=0)

    def run_expert(combined, expert_inputs):
        token_idx, slot_weight, w_gate, w_up, w_down = expert_inputs
        gathered = padded_rows[token_idx]
        gate_act = jnp.dot(gathered, w_gate, preferred_element_type=jnp.float32)
        up_act = jnp.dot(gathered, w_up, preferred_element_type=jnp.float32)
        hidden = (jax.nn.silu(gate_act) * up_act).astype(jnp.bfloat16)
        block_parts = jnp.einsum('rjf,jfd->jrd', hidden.reshape(-1, N_TP, FF_BLK).astype(jnp.float32), w_down.reshape(N_TP, FF_BLK, D).astype(jnp.float32)).astype(jnp.bfloat16)
        expert_out = lax.optimization_barrier(jnp.sum(block_parts.astype(jnp.float32), axis=0)).astype(jnp.bfloat16)
        combined = combined.at[token_idx].add(slot_weight[:, None] * expert_out.astype(jnp.float32))
        return (combined, None)
    start_sums = jnp.zeros((TOKENS_B + 1, D), jnp.float32)
    combined, ignored = lax.scan(run_expert, start_sums, (token_table, weight_table, gate_weight, up_weight, down_weight))
    moe_out = rms_scale(combined[:TOKENS_B], moe_out_gain).astype(jnp.bfloat16)
    return (mixer_out, moe_out)
```

```python
import functools

import jax
import jax.numpy as jnp
from jax import lax
from jax.experimental import pallas as pl
from jax.experimental.pallas import tpu as pltpu
from jax.sharding import PartitionSpec as P

NORM_EPS = 1e-06
MESH = pl.DeviceIdType.MESH
F32 = jnp.float32
BF16 = jnp.bfloat16
ROW_TILE = 16
COMBINE_LAG = 6


def rms_scale(values, gain_vec):
    mean_sq = jnp.mean(values * values, axis=-1, keepdims=True)
    return values * lax.rsqrt(mean_sq + NORM_EPS) * gain_vec


def fused_kernel(
    capacity,
    pool_hbm,
    group_hbm,
    pool_scale,
    out_w_hbm,
    mix_gain,
    tokens_hbm,
    routes,
    route_weights,
    in_gain,
    gate_hbm,
    up_hbm,
    down_hbm,
    out_gain,
    mixer_out,
    moe_out,
    pool,
    history,
    group_w,
    out_w,
    tokens,
    normed,
    slot_rows,
    columns_of,
    outgoing,
    arrived,
    part,
    core_in,
    chip_sum,
    cross_in,
    final,
    returned,
    total_rows,
    gate,
    up,
    down,
    mix_held,
    mix_core,
    mix_sum,
    mix_cross,
    mix_done,
    local_sem,
    hist_sem,
    dis_send,
    dis_recv,
    y1_send,
    y1_recv,
    c1_send,
    c1_recv,
    c2_send,
    c2_recv,
    y2_send,
    y2_recv,
    ret_send,
    ret_recv,
    m1_send,
    m1_recv,
    m2_send,
    m2_recv,
):
    ep_size, tp_size, rows, width = arrived.shape
    exp_dev, _, ff_dev = gate.shape
    tok_dev = tokens.shape[0]
    top_count = routes.shape[0]
    experts = exp_dev * ep_size
    rows_a = pool.shape[0]
    history_rows = history.shape[0]
    highs = tp_size // 2
    ep = lax.axis_index("ep")
    tp = lax.axis_index("tp")
    hi, lo = tp // 2, tp % 2
    other = 1 - lo

    def remote(src, dst, send, recv, to_ep, to_tp):
        return pltpu.make_async_remote_copy(
            src_ref=src,
            dst_ref=dst,
            send_sem=send,
            recv_sem=recv,
            device_id=(to_ep, to_tp),
            device_id_type=MESH,
        )

    def peer_high(k):
        return lax.rem(hi + k, highs)

    def offset_of(i):
        far = jnp.where(i == 0, 1, ep_size - i)
        return jnp.where(i == ep_size - 1, 0, far)

    def partner_ep(d):
        value = ep * 0
        bit = 1
        while bit < ep_size:
            value = value + bit * (((ep // bit) % 2 + (d // bit) % 2) % 2)
            bit *= 2
        return value

    def dispatch(d):
        peer = partner_ep(d)
        return remote(
            outgoing.at[peer], arrived.at[d, tp], dis_send.at[d], dis_recv.at[d], peer, tp
        )

    def gather_cross(d, k):
        slot = arrived.at[d, tp]
        return remote(
            slot, slot, y1_send.at[d, k], y1_recv.at[d, highs - k], ep, peer_high(k) * 2 + lo
        )

    def gather_cross_in(d, k):
        high = peer_high(k)
        slot = arrived.at[d, high * 2 + lo]
        return remote(slot, slot, y1_send.at[d, k], y1_recv.at[d, k], ep, high * 2 + lo)

    def gather_core(d, high):
        slot = arrived.at[d, high * 2 + lo]
        return remote(slot, slot, c1_send.at[d, high], c1_recv.at[d, high], ep, hi * 2 + other)

    def gather_core_in(d, high):
        slot = arrived.at[d, high * 2 + other]
        return remote(slot, slot, c1_send.at[d, high], c1_recv.at[d, high], ep, hi * 2 + other)

    def reduce_core(d, high):
        return remote(
            part.at[high * 2 + other],
            core_in.at[d, high],
            c2_send.at[d, high],
            c2_recv.at[d, high],
            ep,
            hi * 2 + other,
        )

    def reduce_cross(d, k, slot):
        high = peer_high(k)
        return remote(
            chip_sum.at[slot, high],
            cross_in.at[d, highs - k - 1],
            y2_send.at[d, k],
            y2_recv.at[d, highs - k],
            ep,
            high * 2 + lo,
        )

    def reduce_cross_in(d, k, slot):
        high = peer_high(k)
        return remote(
            chip_sum.at[slot, high],
            cross_in.at[d, k - 1],
            y2_send.at[d, k],
            y2_recv.at[d, k],
            ep,
            high * 2 + lo,
        )

    def give_back(d):
        peer = partner_ep(d)
        return remote(final.at[d], returned.at[d], ret_send.at[d], ret_recv.at[d], peer, tp)

    def mix_core_copy(high):
        return remote(
            mix_held.at[high * 2 + other],
            mix_core.at[high],
            m1_send.at[high],
            m1_recv.at[high],
            ep,
            hi * 2 + other,
        )

    def mix_cross_copy(k):
        high = peer_high(k)
        return remote(
            mix_sum.at[high],
            mix_cross.at[highs - k - 1],
            m2_send.at[k],
            m2_recv.at[highs - k],
            ep,
            high * 2 + lo,
        )

    def mix_cross_in(k):
        high = peer_high(k)
        return remote(
            mix_sum.at[high],
            mix_cross.at[k - 1],
            m2_send.at[k],
            m2_recv.at[k],
            ep,
            high * 2 + lo,
        )

    last_rows = pool.at[rows_a - history_rows :]
    send_history = remote(
        last_rows, history, hist_sem.at[0], hist_sem.at[1], jnp.minimum(ep + 1, ep_size - 1), tp
    )

    tokens_copy = pltpu.make_async_copy(tokens_hbm, tokens, local_sem.at[0])
    pool_copy = pltpu.make_async_copy(pool_hbm, pool, local_sem.at[1])
    mixer_copies = [
        pltpu.make_async_copy(group_hbm, group_w, local_sem.at[2]),
        pltpu.make_async_copy(out_w_hbm, out_w, local_sem.at[3]),
    ]
    weight_copies = [
        pltpu.make_async_copy(gate_hbm, gate, local_sem.at[4]),
        pltpu.make_async_copy(up_hbm, up, local_sem.at[5]),
        pltpu.make_async_copy(down_hbm, down, local_sem.at[6]),
    ]
    mixer_store = pltpu.make_async_copy(mix_done, mixer_out, local_sem.at[7])
    moe_store = pltpu.make_async_copy(normed, moe_out, local_sem.at[8])

    tokens_copy.start()
    pool_copy.start()

    barrier = pltpu.get_barrier_semaphore()

    def greet(d, carry):
        pl.semaphore_signal(barrier, inc=1, device_id=(partner_ep(d), tp), device_id_type=MESH)
        return carry

    lax.fori_loop(1, ep_size, greet, 0)
    for k in range(1, highs):
        pl.semaphore_signal(
            barrier, inc=1, device_id=(ep, peer_high(k) * 2 + lo), device_id_type=MESH
        )
    pl.semaphore_signal(barrier, inc=1, device_id=(ep, hi * 2 + other), device_id_type=MESH)
    for copy in mixer_copies + weight_copies:
        copy.start()

    own_tokens = pl.ds(pl.multiple_of(tp * tok_dev, tok_dev), tok_dev)
    own_routes = routes[:, own_tokens]
    own_weights = route_weights[:, own_tokens]
    expert_id = lax.broadcasted_iota(jnp.int32, (experts, tok_dev), 0)
    first_slot = (
        lax.div(expert_id, exp_dev) * rows + lax.rem(expert_id, exp_dev) * capacity
    ).astype(F32)
    earlier = (
        lax.broadcasted_iota(jnp.int32, (tok_dev, tok_dev), 0)
        < lax.broadcasted_iota(jnp.int32, (tok_dev, tok_dev), 1)
    ).astype(BF16)
    taken = jnp.zeros((experts, 1), F32)
    slot_list = []
    for k in range(top_count):
        named = (own_routes[k : k + 1, :] == expert_id).astype(F32)
        before = jnp.dot(named.astype(BF16), earlier, preferred_element_type=F32)
        slot = jnp.sum(named * (before + taken + first_slot), axis=0, keepdims=True)
        taken = taken + jnp.sum(named, axis=1, keepdims=True)
        slot_list.append(slot)
        slot_rows[k : k + 1, :] = slot.astype(jnp.int32)
    stacked = jnp.concatenate(
        slot_list
        + [own_weights[k : k + 1, :] for k in range(top_count)]
        + [jnp.zeros((columns_of.shape[1] - 2 * top_count, tok_dev), F32)],
        axis=0,
    )
    columns_of[...] = stacked.T

    tokens_copy.wait()
    normed[...] = rms_scale(tokens[...].astype(F32), in_gain[...]).astype(BF16)

    def routed_rows(owner):
        slot_id = lax.broadcasted_iota(jnp.int32, (rows, tok_dev), 0) + owner * rows
        chosen = slot_rows[0:1, :] == slot_id
        for k in range(1, top_count):
            chosen = chosen | (slot_rows[k : k + 1, :] == slot_id)
        return jnp.dot(
            chosen.astype(F32).astype(BF16), normed[...], preferred_element_type=F32
        ).astype(BF16)

    pl.semaphore_wait(barrier, ep_size - 1 + highs)

    def stage_a(d):
        for k in range(1, highs):
            gather_cross(d, k).start()
        gather_core(d, hi).start()

    pool_copy.wait()

    @pl.when(ep < ep_size - 1)
    def _():
        send_history.start()

    arrived[0, tp] = routed_rows(ep)
    stage_a(0)

    def send_out(i, carry):
        d = offset_of(i)
        peer = partner_ep(d)
        outgoing[peer] = routed_rows(peer)
        dispatch(d).start()
        return carry

    lax.fori_loop(0, ep_size - 1, send_out, 0)

    for copy in mixer_copies:
        copy.wait()

    @pl.when(ep > 0)
    def _():
        send_history.wait_recv()

    @pl.when(ep == 0)
    def _():
        history[...] = jnp.zeros(history.shape, BF16)

    values = pool[...].astype(F32)
    running = jnp.concatenate([history[...].astype(F32), values], axis=0)
    summed = None
    for group in range(tp_size):
        running = running + pltpu.roll(running, 2**group, 0)
        current = running[history_rows:]
        summed = current if summed is None else jnp.where(tp == group, current, summed)
    window = jnp.int32(1)
    for group in range(tp_size):
        window = jnp.where(tp == group, 2 ** (group + 1), window)
    position = ep * rows_a + lax.broadcasted_iota(jnp.int32, values.shape, 0)
    divisor = jnp.minimum(position + 1, window).astype(F32)
    pooled = (summed / divisor - values).astype(BF16)
    grouped = (
        jnp.dot(pooled, group_w[0], preferred_element_type=F32) * pool_scale[...]
    ).astype(BF16)
    column_step = min(width, 512)
    mix_rows = rows_a // tp_size
    for start in range(0, width, column_step):
        columns = slice(start, start + column_step)
        mix_held[:, :, columns] = (
            jnp.dot(grouped, out_w[:, columns], preferred_element_type=F32)
            .astype(BF16)
            .reshape(tp_size, mix_rows, column_step)
        )
    for high in range(highs):
        mix_core_copy(high).start()
    for high in range(highs):
        mix_core_copy(high).wait_recv()
    for high in range(highs):
        mix_sum[high] = (
            mix_held[high * 2 + lo].astype(F32) + mix_core[high].astype(F32)
        ).astype(BF16)
    for k in range(1, highs):
        mix_cross_copy(k).start()
    first = offset_of(ep * 0)
    dispatch(first).wait_recv()
    stage_a(first)
    for copy in weight_copies:
        copy.wait()
    total_rows[...] = jnp.zeros(total_rows.shape, F32)

    spans = []
    for e in range(exp_dev):
        begin = e * capacity // ROW_TILE * ROW_TILE
        end = -(-(e + 1) * capacity // ROW_TILE) * ROW_TILE
        spans.append((begin, end))
    edges = sorted({0, rows} | {edge for span in spans for edge in span})

    def experts_on(d):
        hidden = []
        for e, (begin, end) in enumerate(spans):
            count = end - begin
            block = arrived[d, :, begin:end, :].reshape(tp_size * count, width)
            gate_act = jnp.dot(block, gate[e], preferred_element_type=F32)
            up_act = jnp.dot(block, up[e], preferred_element_type=F32)
            act = gate_act / (1.0 + jnp.exp(-gate_act)) * up_act
            place = begin + lax.rem(
                lax.broadcasted_iota(jnp.int32, (tp_size * count, 1), 0), count
            )
            mine = (place >= e * capacity) & (place < (e + 1) * capacity)
            hidden.append(jnp.where(mine, act, 0.0).astype(BF16))
        for start in range(0, width, column_step):
            columns = slice(start, start + column_step)
            outs = []
            for e, (begin, end) in enumerate(spans):
                out = jnp.dot(hidden[e], down[e, :, columns], preferred_element_type=F32)
                outs.append(out.reshape(tp_size, end - begin, column_step))
            for begin, end in zip(edges[:-1], edges[1:]):
                piece = None
                for (first_row, last_row), out in zip(spans, outs):
                    if first_row <= begin and end <= last_row:
                        held = out[:, begin - first_row : end - first_row]
                        piece = held if piece is None else piece + held
                if piece is None:
                    piece = jnp.zeros((tp_size, end - begin, column_step), F32)
                part[:, begin:end, columns] = piece.astype(BF16)

    def combine(owner, block):
        slot_id = (
            lax.broadcasted_iota(jnp.int32, (tok_dev, rows), 1) + owner * rows
        ).astype(F32)
        weights = jnp.zeros((tok_dev, rows), F32)
        for k in range(top_count):
            weights = weights + jnp.where(
                columns_of[:, k : k + 1] == slot_id,
                columns_of[:, top_count + k : top_count + k + 1],
                0.0,
            )
        major = weights.astype(BF16)
        minor = (weights - major.astype(F32)).astype(BF16)
        for start in range(0, width, column_step):
            columns = slice(start, start + column_step)
            held = block[:, columns]
            total_rows[:, columns] += jnp.dot(
                major, held, preferred_element_type=F32
            ) + jnp.dot(minor, held, preferred_element_type=F32)

    def combine_from(j):
        d = offset_of(j)
        give_back(d).wait_recv()
        combine(partner_ep(d), returned.at[d])

    def step(i, carry):
        @pl.when(i + 1 < ep_size - 1)
        def _():
            d = offset_of(i + 1)
            dispatch(d).wait_recv()
            stage_a(d)

        @pl.when(i < ep_size)
        def _():
            d = offset_of(i)
            for k in range(1, highs):
                gather_cross_in(d, k).wait_recv()
                gather_core(d, peer_high(k)).start()

        @pl.when(i >= 3)
        def _():
            d = offset_of(i - 3)
            slot = (i - 3) % 2
            total = chip_sum[slot, hi].astype(F32)
            for k in range(1, highs):
                reduce_cross(d, k, slot).wait_send()
                reduce_cross_in(d, k, slot).wait_recv()
                total = total + cross_in[d, k - 1].astype(F32)
            final[d] = total.astype(BF16)

            @pl.when(i < ep_size + 2)
            def _():
                give_back(d).start()

        @pl.when((i >= 1) & (i <= ep_size))
        def _():
            d = offset_of(i - 1)
            slot = (i - 1) % 2
            for high in range(highs):
                reduce_core(d, high).wait_recv()
                reduce_core(d, high).wait_send()
                chip_sum[slot, high] = (
                    part[high * 2 + lo].astype(F32) + core_in[d, high].astype(F32)
                ).astype(BF16)
            for k in range(1, highs):
                reduce_cross(d, k, slot).start()

        @pl.when(i < ep_size)
        def _():
            d = offset_of(i)
            for high in range(highs):
                gather_core_in(d, high).wait_recv()
            experts_on(d)
            for high in range(highs):
                reduce_core(d, high).start()

        @pl.when(i == 2)
        def _():
            total = mix_sum[hi].astype(F32)
            for k in range(1, highs):
                mix_cross_in(k).wait_recv()
                total = total + mix_cross[k - 1].astype(F32)
            mix_done[...] = rms_scale(total, mix_gain[...]).astype(BF16)
            mixer_store.start()

        @pl.when(i >= COMBINE_LAG)
        def _():
            combine_from(i - COMBINE_LAG)

        return carry

    lax.fori_loop(0, ep_size + 3, step, 0)

    def late(j, carry):
        combine_from(j)
        return carry

    lax.fori_loop(max(0, ep_size + 3 - COMBINE_LAG), ep_size - 1, late, 0)
    combine(ep, final.at[0])
    normed[...] = rms_scale(total_rows[...], out_gain[...]).astype(BF16)
    moe_store.start()

    for k in range(1, highs):
        mix_cross_copy(k).wait_send()
    for high in range(highs):
        mix_core_copy(high).wait_send()

    @pl.when(ep < ep_size - 1)
    def _():
        send_history.wait_send()

    def drain_all(d, carry):
        for k in range(1, highs):
            gather_cross(d, k).wait_send()
        for high in range(highs):
            gather_core(d, high).wait_send()
        return carry

    lax.fori_loop(0, ep_size, drain_all, 0)

    def drain(d, carry):
        dispatch(d).wait_send()
        give_back(d).wait_send()
        return carry

    lax.fori_loop(1, ep_size, drain, 0)
    mixer_store.wait()
    moe_store.wait()


def on_device(
    pool_input,
    group_weight,
    pool_scale,
    out_weight,
    mix_gain,
    expert_input,
    routes,
    route_weights,
    moe_in_gain,
    gate_weight,
    up_weight,
    down_weight,
    moe_out_gain,
):
    tp_size = lax.axis_size("tp")
    ep_size = lax.axis_size("ep")
    rows_a, group_width = pool_input.shape
    width = out_weight.shape[1]
    exp_dev = gate_weight.shape[0]
    experts = exp_dev * ep_size
    tok_dev = expert_input.shape[0]
    top_count = routes.shape[1]
    capacity = max(2, 5 * tok_dev * top_count // (4 * experts))
    rows = -(-exp_dev * capacity // ROW_TILE) * ROW_TILE
    highs = tp_size // 2
    mix_rows = rows_a // tp_size
    history_rows = 2**tp_size
    any_spec = pl.BlockSpec(memory_space=pl.ANY)
    vmem_spec = pl.BlockSpec(memory_space=pltpu.VMEM)
    dma = pltpu.SemaphoreType.DMA
    pair = (ep_size, highs)
    flops = 6 * gate_weight.size * ep_size * tp_size * rows
    mixer_out, moe_out = pl.pallas_call(
        functools.partial(fused_kernel, capacity),
        out_shape=(
            jax.ShapeDtypeStruct((mix_rows, width), BF16),
            jax.ShapeDtypeStruct((tok_dev, width), BF16),
        ),
        in_specs=[
            any_spec,
            any_spec,
            vmem_spec,
            any_spec,
            vmem_spec,
            any_spec,
            vmem_spec,
            vmem_spec,
            vmem_spec,
            any_spec,
            any_spec,
            any_spec,
            vmem_spec,
        ],
        out_specs=(any_spec, any_spec),
        scratch_shapes=[
            pltpu.VMEM(pool_input.shape, BF16),
            pltpu.VMEM((history_rows, group_width), BF16),
            pltpu.VMEM(group_weight.shape, BF16),
            pltpu.VMEM(out_weight.shape, BF16),
            pltpu.VMEM(expert_input.shape, BF16),
            pltpu.VMEM(expert_input.shape, BF16),
            pltpu.VMEM((8, tok_dev), jnp.int32),
            pltpu.VMEM((tok_dev, 8), F32),
            pltpu.VMEM((ep_size, rows, width), BF16),
            pltpu.VMEM((ep_size, tp_size, rows, width), BF16),
            pltpu.VMEM((tp_size, rows, width), BF16),
            pltpu.VMEM((ep_size, highs, rows, width), BF16),
            pltpu.VMEM((2, highs, rows, width), BF16),
            pltpu.VMEM((ep_size, highs - 1, rows, width), BF16),
            pltpu.VMEM((ep_size, rows, width), BF16),
            pltpu.VMEM((ep_size, rows, width), BF16),
            pltpu.VMEM(expert_input.shape, F32),
            pltpu.VMEM(gate_weight.shape, BF16),
            pltpu.VMEM(up_weight.shape, BF16),
            pltpu.VMEM(down_weight.shape, BF16),
            pltpu.VMEM((tp_size, mix_rows, width), BF16),
            pltpu.VMEM((highs, mix_rows, width), BF16),
            pltpu.VMEM((highs, mix_rows, width), BF16),
            pltpu.VMEM((highs - 1, mix_rows, width), BF16),
            pltpu.VMEM((mix_rows, width), BF16),
            dma((9,)),
            dma((2,)),
            dma((ep_size,)),
            dma((ep_size,)),
            dma(pair),
            dma(pair),
            dma(pair),
            dma(pair),
            dma(pair),
            dma(pair),
            dma(pair),
            dma(pair),
            dma((ep_size,)),
            dma((ep_size,)),
            dma((highs,)),
            dma((highs,)),
            dma((highs,)),
            dma((highs,)),
        ],
        compiler_params=pltpu.CompilerParams(
            collective_id=0, has_side_effects=True, vmem_limit_bytes=60 * 1024 * 1024
        ),
        cost_estimate=pl.CostEstimate(
            flops=flops, bytes_accessed=8 * expert_input.size, transcendentals=0
        ),
    )(
        pool_input,
        group_weight,
        pool_scale.reshape(1, -1),
        out_weight,
        mix_gain.reshape(1, -1),
        expert_input,
        routes.T,
        route_weights.T,
        moe_in_gain.reshape(1, -1),
        gate_weight,
        up_weight,
        down_weight,
        moe_out_gain.reshape(1, -1),
    )
    return (mixer_out, moe_out)


def solution(mesh):
    in_specs = (
        P("ep", "tp"),
        P("tp", None, None),
        P("tp"),
        P("tp", None),
        P(),
        P(("ep", "tp"), None),
        P("ep", None),
        P("ep", None),
        P(),
        P("ep", None, "tp"),
        P("ep", None, "tp"),
        P("ep", "tp", None),
        P(),
    )
    out_specs = (P(("ep", "tp"), None), P(("ep", "tp"), None))
    return jax.shard_map(
        on_device, mesh=mesh, in_specs=in_specs, out_specs=out_specs, check_vma=False
    )
```

```python
import functools
import math

import jax
import jax.numpy as jnp
from jax import lax
from jax.experimental import pallas as pl
from jax.experimental.pallas import tpu as pltpu
from jax.sharding import PartitionSpec as P

NORM_EPS = 1e-06
ROOM = 56 * 1024 * 1024
SPARE = 3 * 1024 * 1024
MESH = pl.DeviceIdType.MESH
F32 = jnp.float32
BF16 = jnp.bfloat16
ROW_TILE = 16
GATHER, FORWARD, COMPUTE, REDUCE, RETURN, COMBINE, MIX, NONE = range(8)
KINDS = {
    "A": GATHER,
    "X": FORWARD,
    "C": COMPUTE,
    "R": REDUCE,
    "F": RETURN,
    "B": COMBINE,
    "M": MIX,
}
STEADY = (
    (GATHER, -1, 1),
    (FORWARD, 0, 0),
    (RETURN, 3, 0),
    (REDUCE, 1, 0),
    (COMPUTE, 0, 0),
    (COMBINE, 8, 1),
)
CODE_BITS = 6
PER_WORD = 5


def coded(*events):
    return tuple(KINDS[event[0]] * 8 + int(event[1:] or 0) for event in events)


END_EVENTS = coded(
    "A3", "A1", "A6", "A7", "X6", "C6", "R6", "A4", "X7", "C7", "R7", "A5", "F6", "X4", "C4",
    "R4", "F7", "X5", "C5", "R5", "F4", "X1", "C1", "R1", "A2", "F5", "X3", "C3", "R3", "F1",
    "X2", "C2", "R2", "F3", "X0", "C0", "R0", "M", "F2", "B6", "B7", "B4", "B5", "B1", "B3",
    "F0", "B2",
)
MIDDLE_EVENTS = coded(
    "A1", "A4", "A5", "X4", "C4", "R4", "X5", "C5", "R5", "F4", "X1", "C1", "R1", "F5", "A3",
    "A6", "X3", "C3", "R3", "F1", "X6", "C6", "R6", "A7", "A2", "F3", "F6", "X7", "C7", "R7",
    "X2", "C2", "R2", "F7", "X0", "C0", "R0", "M", "F2", "B4", "B5", "B1", "B3", "B6", "B7",
    "F0", "B2",
)
SEND_ORDER = (1, 4, 5, 6, 7, 3, 2)

def rms_scale(values, gain_vec):
    mean_sq = jnp.mean(values * values, axis=-1, keepdims=True)
    return values * lax.rsqrt(mean_sq + NORM_EPS) * gain_vec


def fused_kernel(
    capacity,
    pool_hbm,
    group_hbm,
    pool_scale_hbm,
    out_w_hbm,
    mix_gain_hbm,
    tokens_hbm,
    routes_hbm,
    route_weights_hbm,
    in_gain_hbm,
    gate_hbm,
    up_hbm,
    down_hbm,
    out_gain_hbm,
    mixer_out,
    moe_out,
    pool_scale,
    mix_gain,
    routes,
    route_weights,
    in_gain,
    out_gain,
    pool,
    history,
    group_w,
    out_w,
    tokens,
    normed,
    slot_rows,
    columns_of,
    outgoing,
    arrived,
    part,
    core_in,
    cross_in,
    returned,
    total_rows,
    gate,
    up,
    down,
    mix_held,
    mix_core,
    mix_sum,
    mix_cross,
    local_sem,
    hist_sem,
    dis_send,
    dis_recv,
    y1_send,
    y1_recv,
    c1_send,
    c1_recv,
    c2_send,
    c2_recv,
    y2_send,
    y2_recv,
    ret_send,
    ret_recv,
    m1_send,
    m1_recv,
    m2_send,
    m2_recv,
):
    ep_size, tp_size, rows, width = arrived.shape
    exp_dev, _, ff_dev = gate.shape
    tok_dev = tokens.shape[0]
    top_count = routes.shape[0]
    experts = exp_dev * ep_size
    rows_a = pool.shape[0]
    history_rows = history.shape[0]
    highs = tp_size // 2
    ep = lax.axis_index("ep")
    tp = lax.axis_index("tp")
    hi, lo = tp // 2, tp % 2
    other = 1 - lo

    def remote(src, dst, send, recv, to_ep, to_tp):
        return pltpu.make_async_remote_copy(
            src_ref=src,
            dst_ref=dst,
            send_sem=send,
            recv_sem=recv,
            device_id=(to_ep, to_tp),
            device_id_type=MESH,
        )

    def peer_high(k):
        return lax.rem(hi + k, highs)

    on_end = (ep // 2) % 2 == (ep // 4) % 2
    tabled = ep_size == 8

    def packed_at(table, i):
        words = []
        for begin in range(0, len(table), PER_WORD):
            piece = table[begin : begin + PER_WORD]
            words.append(sum(value << (CODE_BITS * at) for at, value in enumerate(piece)))
        word = jnp.int32(words[0])
        for at in range(1, len(words)):
            word = jnp.where(i >= at * PER_WORD, words[at], word)
        shift = CODE_BITS * lax.rem(i, PER_WORD)
        return lax.rem(lax.shift_right_logical(word, shift), 1 << CODE_BITS)

    def offset_of(i):
        far = jnp.where(i == 0, 1, ep_size - i)
        return jnp.where(i == ep_size - 1, 0, far)

    def sent_at(i):
        if tabled:
            return packed_at(SEND_ORDER, i)
        return offset_of(i)

    def event_at(t):
        if tabled:
            code = jnp.where(on_end, packed_at(END_EVENTS, t), packed_at(MIDDLE_EVENTS, t))
            return code // 8, code % 8
        i, slot = t // 8, t % 8
        op, j = jnp.int32(NONE), i
        for at, (kind, lag, last) in enumerate(STEADY):
            index = i - lag
            valid = (slot == at) & (index >= 0) & (index < ep_size - last)
            op = jnp.where(valid, kind, op)
            j = jnp.where(valid, index, j)
        op = jnp.where((slot == 6) & (i == 0), MIX, op)
        return op, offset_of(j)

    def partner_ep(d):
        value = ep * 0
        bit = 1
        while bit < ep_size:
            value = value + bit * (((ep // bit) % 2 + (d // bit) % 2) % 2)
            bit *= 2
        return value

    def dispatch(d):
        peer = partner_ep(d)
        return remote(
            outgoing.at[peer], arrived.at[d, tp], dis_send.at[d], dis_recv.at[d], peer, tp
        )

    def gather_cross(d, k):
        slot = arrived.at[d, tp]
        return remote(
            slot, slot, y1_send.at[d, k], y1_recv.at[d, highs - k], ep, peer_high(k) * 2 + lo
        )

    def gather_cross_in(d, k):
        high = peer_high(k)
        slot = arrived.at[d, high * 2 + lo]
        return remote(slot, slot, y1_send.at[d, k], y1_recv.at[d, k], ep, high * 2 + lo)

    def gather_core(d, high):
        slot = arrived.at[d, high * 2 + lo]
        return remote(slot, slot, c1_send.at[d, high], c1_recv.at[d, high], ep, hi * 2 + other)

    def gather_core_in(d, high):
        slot = arrived.at[d, high * 2 + other]
        return remote(slot, slot, c1_send.at[d, high], c1_recv.at[d, high], ep, hi * 2 + other)

    def reduce_core(d, high):
        return remote(
            part.at[high * 2 + other],
            core_in.at[d, high],
            c2_send.at[d, high],
            c2_recv.at[d, high],
            ep,
            hi * 2 + other,
        )

    def reduce_cross(d, k):
        high = peer_high(k)
        return remote(
            core_in.at[d, high],
            cross_in.at[d, highs - k - 1],
            y2_send.at[d, k],
            y2_recv.at[d, highs - k],
            ep,
            high * 2 + lo,
        )

    def reduce_cross_in(d, k):
        high = peer_high(k)
        return remote(
            core_in.at[d, high],
            cross_in.at[d, k - 1],
            y2_send.at[d, k],
            y2_recv.at[d, k],
            ep,
            high * 2 + lo,
        )

    def give_back(d):
        peer = partner_ep(d)
        return remote(core_in.at[d, hi], returned.at[d], ret_send.at[d], ret_recv.at[d], peer, tp)

    def mix_core_copy(high):
        return remote(
            mix_held.at[high * 2 + other],
            mix_core.at[high],
            m1_send.at[high],
            m1_recv.at[high],
            ep,
            hi * 2 + other,
        )

    def mix_cross_copy(k):
        high = peer_high(k)
        return remote(
            mix_sum.at[high],
            mix_cross.at[highs - k - 1],
            m2_send.at[k],
            m2_recv.at[highs - k],
            ep,
            high * 2 + lo,
        )

    def mix_cross_in(k):
        high = peer_high(k)
        return remote(
            mix_sum.at[high],
            mix_cross.at[k - 1],
            m2_send.at[k],
            m2_recv.at[k],
            ep,
            high * 2 + lo,
        )

    last_rows = pool.at[rows_a - history_rows :]
    send_history = remote(
        last_rows, history, hist_sem.at[0], hist_sem.at[1], jnp.minimum(ep + 1, ep_size - 1), tp
    )

    tokens_copy = pltpu.make_async_copy(tokens_hbm, tokens, local_sem.at[0])
    pool_copy = pltpu.make_async_copy(pool_hbm, pool, local_sem.at[1])
    mixer_copies = [
        pltpu.make_async_copy(group_hbm, group_w, local_sem.at[2]),
        pltpu.make_async_copy(out_w_hbm, out_w, local_sem.at[3]),
    ]
    weight_copies = [
        pltpu.make_async_copy(gate_hbm, gate, local_sem.at[4]),
        pltpu.make_async_copy(up_hbm, up, local_sem.at[5]),
        pltpu.make_async_copy(down_hbm, down, local_sem.at[6]),
    ]

    early_copies = [
        pltpu.make_async_copy(routes_hbm, routes, local_sem.at[9]),
        pltpu.make_async_copy(route_weights_hbm, route_weights, local_sem.at[10]),
        pltpu.make_async_copy(in_gain_hbm, in_gain, local_sem.at[11]),
    ]
    mixer_copies += [
        pltpu.make_async_copy(pool_scale_hbm, pool_scale, local_sem.at[12]),
        pltpu.make_async_copy(mix_gain_hbm, mix_gain, local_sem.at[13]),
        pltpu.make_async_copy(out_gain_hbm, out_gain, local_sem.at[14]),
    ]
    for copy in early_copies:
        copy.start()
    tokens_copy.start()
    pool_copy.start()

    barrier = pltpu.get_barrier_semaphore()

    def greet(d, carry):
        pl.semaphore_signal(barrier, inc=1, device_id=(partner_ep(d), tp), device_id_type=MESH)
        return carry

    lax.fori_loop(1, ep_size, greet, 0)
    for k in range(1, highs):
        pl.semaphore_signal(
            barrier, inc=1, device_id=(ep, peer_high(k) * 2 + lo), device_id_type=MESH
        )
    pl.semaphore_signal(barrier, inc=1, device_id=(ep, hi * 2 + other), device_id_type=MESH)
    for copy in mixer_copies + weight_copies:
        copy.start()

    own_tokens = pl.ds(pl.multiple_of(tp * tok_dev, tok_dev), tok_dev)
    for copy in early_copies:
        copy.wait()
    own_routes = routes[:, own_tokens]
    own_weights = route_weights[:, own_tokens]
    expert_id = lax.broadcasted_iota(jnp.int32, (experts, tok_dev), 0)
    first_slot = (
        lax.div(expert_id, exp_dev) * rows + lax.rem(expert_id, exp_dev) * capacity
    ).astype(F32)
    earlier = (
        lax.broadcasted_iota(jnp.int32, (tok_dev, tok_dev), 0)
        < lax.broadcasted_iota(jnp.int32, (tok_dev, tok_dev), 1)
    ).astype(BF16)
    taken = jnp.zeros((experts, 1), F32)
    slot_list = []
    for k in range(top_count):
        named = (own_routes[k : k + 1, :] == expert_id).astype(F32)
        before = jnp.dot(named.astype(BF16), earlier, preferred_element_type=F32)
        slot = jnp.sum(named * (before + taken + first_slot), axis=0, keepdims=True)
        taken = taken + jnp.sum(named, axis=1, keepdims=True)
        slot_list.append(slot)
        slot_rows[k : k + 1, :] = slot.astype(jnp.int32)
    stacked = jnp.concatenate(
        slot_list
        + [own_weights[k : k + 1, :] for k in range(top_count)]
        + [jnp.zeros((columns_of.shape[1] - 2 * top_count, tok_dev), F32)],
        axis=0,
    )
    columns_of[...] = stacked.T

    tokens_copy.wait()
    normed[...] = rms_scale(tokens[...].astype(F32), in_gain[...]).astype(BF16)

    def routed_rows(owner):
        slot_id = lax.broadcasted_iota(jnp.int32, (rows, tok_dev), 0) + owner * rows
        chosen = slot_rows[0:1, :] == slot_id
        for k in range(1, top_count):
            chosen = chosen | (slot_rows[k : k + 1, :] == slot_id)
        return jnp.dot(
            chosen.astype(F32).astype(BF16), normed[...], preferred_element_type=F32
        ).astype(BF16)

    column_step = min(width, 512)

    def mixer_part():
        for copy in mixer_copies:
            copy.wait()

        @pl.when(ep > 0)
        def _():
            send_history.wait_recv()

        @pl.when(ep == 0)
        def _():
            history[...] = jnp.zeros(history.shape, BF16)

        values = pool[...].astype(F32)
        running = jnp.concatenate([history[...].astype(F32), values], axis=0)
        summed = None
        for group in range(tp_size):
            running = running + pltpu.roll(running, 2**group, 0)
            current = running[history_rows:]
            summed = current if summed is None else jnp.where(tp == group, current, summed)
        window = jnp.int32(1)
        for group in range(tp_size):
            window = jnp.where(tp == group, 2 ** (group + 1), window)
        position = ep * rows_a + lax.broadcasted_iota(jnp.int32, values.shape, 0)
        divisor = jnp.minimum(position + 1, window).astype(F32)
        pooled = (summed / divisor - values).astype(BF16)
        grouped = (
            jnp.dot(pooled, group_w[0], preferred_element_type=F32) * pool_scale[...]
        ).astype(BF16)
        mix_rows = rows_a // tp_size
        for start in range(0, width, column_step):
            columns = slice(start, start + column_step)
            mix_held[:, :, columns] = (
                jnp.dot(grouped, out_w[:, columns], preferred_element_type=F32)
                .astype(BF16)
                .reshape(tp_size, mix_rows, column_step)
            )
        for high in range(highs):
            mix_core_copy(high).start()
        for high in range(highs):
            mix_core_copy(high).wait_recv()
        for high in range(highs):
            mix_sum[high] = (
                mix_held[high * 2 + lo].astype(F32) + mix_core[high].astype(F32)
            ).astype(BF16)
        for k in range(1, highs):
            mix_cross_copy(k).start()

    def stage_a(d):
        for k in range(1, highs):
            gather_cross(d, k).start()
        gather_core(d, hi).start()

    arrived[0, tp] = routed_rows(ep)
    pool_copy.wait()
    pl.semaphore_wait(barrier, ep_size - 1 + highs)

    @pl.when(ep < ep_size - 1)
    def _():
        send_history.start()

    stage_a(0)

    def send_out(i, carry):
        d = sent_at(i)
        peer = partner_ep(d)
        outgoing[peer] = routed_rows(peer)
        dispatch(d).start()
        return carry

    lax.fori_loop(0, ep_size - 1, send_out, 0)

    def gather_next(d):
        dispatch(d).wait_recv()
        stage_a(d)

    if not tabled:
        gather_next(offset_of(ep * 0))
    for copy in weight_copies:
        copy.wait()
    total_rows[...] = jnp.zeros(total_rows.shape, F32)

    spans = []
    for e in range(exp_dev):
        begin = e * capacity // ROW_TILE * ROW_TILE
        end = -(-(e + 1) * capacity // ROW_TILE) * ROW_TILE
        spans.append((begin, end))
    edges = sorted({0, rows} | {edge for span in spans for edge in span})

    def experts_on(d):
        hidden = []
        for e, (begin, end) in enumerate(spans):
            count = end - begin
            block = arrived[d, :, begin:end, :].reshape(tp_size * count, width)
            gate_act = jnp.dot(block, gate[e], preferred_element_type=F32)
            up_act = jnp.dot(block, up[e], preferred_element_type=F32)
            act = gate_act / (1.0 + jnp.exp(-gate_act)) * up_act
            place = begin + lax.rem(
                lax.broadcasted_iota(jnp.int32, (tp_size * count, 1), 0), count
            )
            mine = (place >= e * capacity) & (place < (e + 1) * capacity)
            hidden.append(jnp.where(mine, act, 0.0).astype(BF16))
        for start in range(0, width, column_step):
            columns = slice(start, start + column_step)
            outs = []
            for e, (begin, end) in enumerate(spans):
                out = jnp.dot(hidden[e], down[e, :, columns], preferred_element_type=F32)
                outs.append(out.reshape(tp_size, end - begin, column_step))
            for begin, end in zip(edges[:-1], edges[1:]):
                piece = None
                for (first_row, last_row), out in zip(spans, outs):
                    if first_row <= begin and end <= last_row:
                        held = out[:, begin - first_row : end - first_row]
                        piece = held if piece is None else piece + held
                if piece is None:
                    piece = jnp.zeros((tp_size, end - begin, column_step), F32)
                part[:, begin:end, columns] = piece.astype(BF16)

    def combine(owner, block):
        lane = lax.broadcasted_iota(jnp.int32, (tok_dev, 2 * rows), 1)
        slot_id = (lax.rem(lane, rows) + owner * rows).astype(F32)
        weights = jnp.zeros((tok_dev, 2 * rows), F32)
        for k in range(top_count):
            weights = weights + jnp.where(
                columns_of[:, k : k + 1] == slot_id,
                columns_of[:, top_count + k : top_count + k + 1],
                0.0,
            )
        major = weights.astype(BF16).astype(F32)
        split = jnp.where(lane < rows, major, weights - major).astype(BF16)
        for start in range(0, width, column_step):
            columns = slice(start, start + column_step)
            held = block[:, columns]
            twice = jnp.concatenate([held, held], axis=0)
            total_rows[:, columns] += jnp.dot(split, twice, preferred_element_type=F32)

    def combine_from(d):
        give_back(d).wait_recv()
        combine(partner_ep(d), returned.at[d])

    def forward(d):
        for k in range(1, highs):
            gather_cross_in(d, k).wait_recv()
            gather_core(d, peer_high(k)).start()

    def compute(d):
        for high in range(highs):
            gather_core_in(d, high).wait_recv()
        experts_on(d)
        for high in range(highs):
            reduce_core(d, high).start()

    def reduce(d):
        for high in range(highs):
            reduce_core(d, high).wait_recv()
            reduce_core(d, high).wait_send()
            core_in[d, high] = (
                part[high * 2 + lo].astype(F32) + core_in[d, high].astype(F32)
            ).astype(BF16)
        for k in range(1, highs):
            reduce_cross(d, k).start()

    def send_home(d):
        total = core_in[d, hi].astype(F32)
        for k in range(1, highs):
            reduce_cross_in(d, k).wait_recv()
            total = total + cross_in[d, k - 1].astype(F32)
        core_in[d, hi] = total.astype(BF16)

        @pl.when(d != 0)
        def _():
            give_back(d).start()

    def mixer_end():
        total = mix_sum[hi].astype(F32)
        for k in range(1, highs):
            mix_cross_in(k).wait_recv()
            total = total + mix_cross[k - 1].astype(F32)
        mixer_out[...] = rms_scale(total, mix_gain[...]).astype(BF16)

    actions = {
        GATHER: gather_next,
        FORWARD: forward,
        COMPUTE: compute,
        REDUCE: reduce,
        RETURN: send_home,
        COMBINE: combine_from,
        MIX: lambda d: mixer_part(),
    }

    def event(t, carry):
        op, d = event_at(t)
        for kind, action in actions.items():
            pl.when(op == kind)(functools.partial(action, d))
        return carry

    count = len(END_EVENTS) if tabled else 8 * (ep_size + 3)
    lax.fori_loop(0, count, event, 0)

    if not tabled:

        def late(j, carry):
            combine_from(offset_of(j))
            return carry

        lax.fori_loop(max(0, ep_size - 5), ep_size - 1, late, 0)
    combine(ep, core_in.at[0, hi])
    moe_out[...] = rms_scale(total_rows[...], out_gain[...]).astype(BF16)
    mixer_end()

    for k in range(1, highs):
        mix_cross_copy(k).wait_send()
    for high in range(highs):
        mix_core_copy(high).wait_send()

    @pl.when(ep < ep_size - 1)
    def _():
        send_history.wait_send()

    def drain_all(d, carry):
        for k in range(1, highs):
            gather_cross(d, k).wait_send()
            reduce_cross(d, k).wait_send()
        for high in range(highs):
            gather_core(d, high).wait_send()
        return carry

    lax.fori_loop(0, ep_size, drain_all, 0)

    def drain(d, carry):
        dispatch(d).wait_send()
        give_back(d).wait_send()
        return carry

    lax.fori_loop(1, ep_size, drain, 0)


def on_device(
    pool_input,
    group_weight,
    pool_scale,
    out_weight,
    mix_gain,
    expert_input,
    routes,
    route_weights,
    moe_in_gain,
    gate_weight,
    up_weight,
    down_weight,
    moe_out_gain,
):
    tp_size = lax.axis_size("tp")
    ep_size = lax.axis_size("ep")
    rows_a, group_width = pool_input.shape
    width = out_weight.shape[1]
    exp_dev = gate_weight.shape[0]
    experts = exp_dev * ep_size
    tok_dev = expert_input.shape[0]
    top_count = routes.shape[1]
    capacity = max(2, 5 * tok_dev * top_count // (4 * experts))
    rows = -(-exp_dev * capacity // ROW_TILE) * ROW_TILE
    highs = tp_size // 2
    mix_rows = rows_a // tp_size
    history_rows = 2**tp_size
    vmem_spec = pl.BlockSpec(memory_space=pltpu.VMEM)
    hbm_spec = pl.BlockSpec(memory_space=pltpu.HBM)
    dma = pltpu.SemaphoreType.DMA
    pair = (ep_size, highs)
    flops = 6 * gate_weight.size * ep_size * tp_size * rows
    scratch = [
        pltpu.VMEM((1, group_width), F32),
        pltpu.VMEM((1, width), F32),
        pltpu.VMEM((top_count, tok_dev * tp_size), jnp.int32),
        pltpu.VMEM((top_count, tok_dev * tp_size), F32),
        pltpu.VMEM((1, width), F32),
        pltpu.VMEM((1, width), F32),
        pltpu.VMEM(pool_input.shape, BF16),
        pltpu.VMEM((history_rows, group_width), BF16),
        pltpu.VMEM(group_weight.shape, BF16),
        pltpu.VMEM(out_weight.shape, BF16),
        pltpu.VMEM(expert_input.shape, BF16),
        pltpu.VMEM(expert_input.shape, BF16),
        pltpu.VMEM((8, tok_dev), jnp.int32),
        pltpu.VMEM((tok_dev, 8), F32),
        pltpu.VMEM((ep_size, rows, width), BF16),
        pltpu.VMEM((ep_size, tp_size, rows, width), BF16),
        pltpu.VMEM((tp_size, rows, width), BF16),
        pltpu.VMEM((ep_size, highs, rows, width), BF16),
        pltpu.VMEM((ep_size, highs - 1, rows, width), BF16),
        pltpu.VMEM((ep_size, rows, width), BF16),
        pltpu.VMEM(expert_input.shape, F32),
        pltpu.VMEM(gate_weight.shape, BF16),
        pltpu.VMEM(up_weight.shape, BF16),
        pltpu.VMEM(down_weight.shape, BF16),
        pltpu.VMEM((tp_size, mix_rows, width), BF16),
        pltpu.VMEM((highs, mix_rows, width), BF16),
        pltpu.VMEM((highs, mix_rows, width), BF16),
        pltpu.VMEM((highs - 1, mix_rows, width), BF16),
        dma((15,)),
        dma((2,)),
        dma((ep_size,)),
        dma((ep_size,)),
        dma(pair),
        dma(pair),
        dma(pair),
        dma(pair),
        dma(pair),
        dma(pair),
        dma(pair),
        dma(pair),
        dma((ep_size,)),
        dma((ep_size,)),
        dma((highs,)),
        dma((highs,)),
        dma((highs,)),
        dma((highs,)),
    ]
    held = sum(
        ref.dtype.itemsize * math.prod(ref.shape)
        for ref in scratch
        if ref.memory_space == pltpu.VMEM
    )
    mixer_out, moe_out = pl.pallas_call(
        functools.partial(fused_kernel, capacity),
        out_shape=(
            pltpu.VMEM((mix_rows, width), BF16),
            pltpu.VMEM((tok_dev, width), BF16),
        ),
        in_specs=[hbm_spec] * 13,
        out_specs=(vmem_spec, vmem_spec),
        scratch_shapes=scratch,
        compiler_params=pltpu.CompilerParams(
            collective_id=0, has_side_effects=True, vmem_limit_bytes=max(ROOM, held + SPARE)
        ),
        cost_estimate=pl.CostEstimate(
            flops=flops, bytes_accessed=8 * expert_input.size, transcendentals=0
        ),
    )(
        pool_input,
        group_weight,
        pool_scale.reshape(1, -1),
        out_weight,
        mix_gain.reshape(1, -1),
        expert_input,
        routes.T,
        route_weights.T,
        moe_in_gain.reshape(1, -1),
        gate_weight,
        up_weight,
        down_weight,
        moe_out_gain.reshape(1, -1),
    )
    return (mixer_out, moe_out)


def solution(mesh):
    in_specs = (
        P("ep", "tp"),
        P("tp", None, None),
        P("tp"),
        P("tp", None),
        P(),
        P(("ep", "tp"), None),
        P("ep", None),
        P("ep", None),
        P(),
        P("ep", None, "tp"),
        P("ep", None, "tp"),
        P("ep", "tp", None),
        P(),
    )
    out_specs = (P(("ep", "tp"), None), P(("ep", "tp"), None))
    return jax.shard_map(
        on_device, mesh=mesh, in_specs=in_specs, out_specs=out_specs, check_vma=False
    )
```

```python
import functools
import math

import jax
import jax.numpy as jnp
from jax import lax
from jax.experimental import pallas as pl
from jax.experimental.pallas import tpu as pltpu
from jax.sharding import PartitionSpec as P

NORM_EPS = 1e-06
ROOM = 56 * 1024 * 1024
SPARE = 3 * 1024 * 1024
MESH = pl.DeviceIdType.MESH
F32 = jnp.float32
BF16 = jnp.bfloat16
ROW_TILE = 16
GATHER, FORWARD, COMPUTE, REDUCE, RETURN, COMBINE, MIX, PEER, NONE = range(9)
KINDS = {
    "A": GATHER,
    "X": FORWARD,
    "C": COMPUTE,
    "R": REDUCE,
    "F": RETURN,
    "B": COMBINE,
    "M": MIX,
    "P": PEER,
}
STEADY = (
    (GATHER, -1, 1),
    (FORWARD, 0, 0),
    (RETURN, 3, 0),
    (REDUCE, 1, 0),
    (COMPUTE, 0, 0),
    (COMBINE, 8, 1),
)
CODE_BITS = 6
NEAR = 4
PER_WORD = 5


def coded(*events):
    return tuple(KINDS[event[0]] * 8 + int(event[1:] or 0) for event in events)


END_EVENTS = coded(
    "A3", "A1", "A6", "P", "A7", "X6", "C6", "R6", "X7", "C7", "R7", "A4", "A5", "F6", "F7",
    "X4", "C4", "R4", "X5", "C5", "R5", "F4", "A2", "X1", "C1", "R1", "F5", "X3", "C3", "R3",
    "F1", "X2", "C2", "R2", "F3", "X0", "C0", "R0", "M", "F2", "B6", "B7", "B4", "B5", "B1",
    "B3", "F0", "B2",
)
MIDDLE_EVENTS = coded(
    "A1", "A4", "A5", "P", "X4", "C4", "R4", "X5", "C5", "R5", "F4", "X0", "C0", "R0", "F5",
    "A6", "X1", "C1", "R1", "F0", "X6", "C6", "R6", "A7", "A3", "F1", "X3", "C3", "R3", "F6",
    "A2", "X7", "C7", "R7", "F3", "X2", "C2", "R2", "F7", "M", "B4", "B5", "F2", "B1", "B3",
    "B6", "B7", "B2",
)
SEND_ORDER = (1, 4, 5, 6, 7, 3, 2)

def rms_scale(values, gain_vec):
    mean_sq = jnp.mean(values * values, axis=-1, keepdims=True)
    return values * lax.rsqrt(mean_sq + NORM_EPS) * gain_vec


def fused_kernel(
    capacity,
    pool_hbm,
    group_hbm,
    pool_scale_hbm,
    out_w_hbm,
    mix_gain_hbm,
    tokens_hbm,
    routes_hbm,
    route_weights_hbm,
    in_gain_hbm,
    gate_hbm,
    up_hbm,
    down_hbm,
    out_gain_hbm,
    mixer_out,
    moe_out,
    pool_scale,
    mix_gain,
    routes,
    route_weights,
    in_gain,
    out_gain,
    pool,
    history,
    group_w,
    out_w,
    tokens,
    normed,
    raw,
    near_out,
    slot_rows,
    columns_of,
    outgoing,
    arrived,
    part,
    core_in,
    cross_in,
    returned,
    total_rows,
    gate,
    up,
    down,
    mix_held,
    mix_core,
    mix_sum,
    mix_cross,
    local_sem,
    hist_sem,
    raw_send,
    raw_recv,
    dis_send,
    dis_recv,
    y1_send,
    y1_recv,
    c1_send,
    c1_recv,
    c2_send,
    c2_recv,
    y2_send,
    y2_recv,
    ret_send,
    ret_recv,
    m1_send,
    m1_recv,
    m2_send,
    m2_recv,
):
    ep_size, tp_size, rows, width = arrived.shape
    exp_dev, _, ff_dev = gate.shape
    tok_dev = tokens.shape[0]
    top_count = routes.shape[0]
    experts = exp_dev * ep_size
    rows_a = pool.shape[0]
    history_rows = history.shape[0]
    highs = tp_size // 2
    ep = lax.axis_index("ep")
    tp = lax.axis_index("tp")
    hi, lo = tp // 2, tp % 2
    other = 1 - lo

    def remote(src, dst, send, recv, to_ep, to_tp):
        return pltpu.make_async_remote_copy(
            src_ref=src,
            dst_ref=dst,
            send_sem=send,
            recv_sem=recv,
            device_id=(to_ep, to_tp),
            device_id_type=MESH,
        )

    def peer_high(k):
        return lax.rem(hi + k, highs)

    on_end = (ep // 2) % 2 == (ep // 4) % 2
    tabled = ep_size == 8

    def packed_at(table, i):
        words = []
        for begin in range(0, len(table), PER_WORD):
            piece = table[begin : begin + PER_WORD]
            words.append(sum(value << (CODE_BITS * at) for at, value in enumerate(piece)))
        word = jnp.int32(words[0])
        for at in range(1, len(words)):
            word = jnp.where(i >= at * PER_WORD, words[at], word)
        shift = CODE_BITS * lax.rem(i, PER_WORD)
        return lax.rem(lax.shift_right_logical(word, shift), 1 << CODE_BITS)

    def offset_of(i):
        far = jnp.where(i == 0, 1, ep_size - i)
        return jnp.where(i == ep_size - 1, 0, far)

    def sent_at(i):
        if tabled:
            return packed_at(SEND_ORDER, i)
        return offset_of(i)

    def event_at(t):
        if tabled:
            code = jnp.where(on_end, packed_at(END_EVENTS, t), packed_at(MIDDLE_EVENTS, t))
            return code // 8, code % 8
        i, slot = t // 8, t % 8
        op, j = jnp.int32(NONE), i
        for at, (kind, lag, last) in enumerate(STEADY):
            index = i - lag
            valid = (slot == at) & (index >= 0) & (index < ep_size - last)
            op = jnp.where(valid, kind, op)
            j = jnp.where(valid, index, j)
        op = jnp.where((slot == 6) & (i == 0), MIX, op)
        return op, offset_of(j)

    def partner_ep(d):
        value = ep * 0
        bit = 1
        while bit < ep_size:
            value = value + bit * (((ep // bit) % 2 + (d // bit) % 2) % 2)
            bit *= 2
        return value

    def dispatch(d):
        peer = partner_ep(d)
        return remote(
            outgoing.at[peer], arrived.at[d, tp], dis_send.at[d], dis_recv.at[d], peer, tp
        )

    def gather_cross(d, k):
        slot = arrived.at[d, tp]
        return remote(
            slot, slot, y1_send.at[d, k], y1_recv.at[d, highs - k], ep, peer_high(k) * 2 + lo
        )

    def gather_cross_in(d, k):
        high = peer_high(k)
        slot = arrived.at[d, high * 2 + lo]
        return remote(slot, slot, y1_send.at[d, k], y1_recv.at[d, k], ep, high * 2 + lo)

    def gather_core(d, high):
        slot = arrived.at[d, high * 2 + lo]
        return remote(slot, slot, c1_send.at[d, high], c1_recv.at[d, high], ep, hi * 2 + other)

    def gather_core_in(d, high):
        slot = arrived.at[d, high * 2 + other]
        return remote(slot, slot, c1_send.at[d, high], c1_recv.at[d, high], ep, hi * 2 + other)

    def reduce_core(d, high):
        return remote(
            part.at[high * 2 + other],
            core_in.at[d, high],
            c2_send.at[d, high],
            c2_recv.at[d, high],
            ep,
            hi * 2 + other,
        )

    def reduce_cross(d, k):
        high = peer_high(k)
        return remote(
            core_in.at[d, high],
            cross_in.at[d, highs - k - 1],
            y2_send.at[d, k],
            y2_recv.at[d, highs - k],
            ep,
            high * 2 + lo,
        )

    def reduce_cross_in(d, k):
        high = peer_high(k)
        return remote(
            core_in.at[d, high],
            cross_in.at[d, k - 1],
            y2_send.at[d, k],
            y2_recv.at[d, k],
            ep,
            high * 2 + lo,
        )

    def raw_copy(k):
        return remote(
            normed,
            raw.at[highs - k - 1],
            raw_send.at[k],
            raw_recv.at[highs - k],
            ep,
            peer_high(k) * 2 + lo,
        )

    def raw_copy_in(k):
        return remote(
            normed, raw.at[k - 1], raw_send.at[k], raw_recv.at[k], ep, peer_high(k) * 2 + lo
        )

    def near_copy(d, k):
        return remote(
            near_out.at[d, k - 1],
            arrived.at[d, peer_high(k) * 2 + lo],
            y1_send.at[d, k],
            y1_recv.at[d, k],
            partner_ep(d),
            tp,
        )

    def give_back(d):
        peer = partner_ep(d)
        return remote(core_in.at[d, hi], returned.at[d], ret_send.at[d], ret_recv.at[d], peer, tp)

    def mix_core_copy(high):
        return remote(
            mix_held.at[high * 2 + other],
            mix_core.at[high],
            m1_send.at[high],
            m1_recv.at[high],
            ep,
            hi * 2 + other,
        )

    def mix_cross_copy(k):
        high = peer_high(k)
        return remote(
            mix_sum.at[high],
            mix_cross.at[highs - k - 1],
            m2_send.at[k],
            m2_recv.at[highs - k],
            ep,
            high * 2 + lo,
        )

    def mix_cross_in(k):
        high = peer_high(k)
        return remote(
            mix_sum.at[high],
            mix_cross.at[k - 1],
            m2_send.at[k],
            m2_recv.at[k],
            ep,
            high * 2 + lo,
        )

    last_rows = pool.at[rows_a - history_rows :]
    send_history = remote(
        last_rows, history, hist_sem.at[0], hist_sem.at[1], jnp.minimum(ep + 1, ep_size - 1), tp
    )

    tokens_copy = pltpu.make_async_copy(tokens_hbm, tokens, local_sem.at[0])
    pool_copy = pltpu.make_async_copy(pool_hbm, pool, local_sem.at[1])
    mixer_copies = [
        pltpu.make_async_copy(group_hbm, group_w, local_sem.at[2]),
        pltpu.make_async_copy(out_w_hbm, out_w, local_sem.at[3]),
    ]
    weight_copies = [
        pltpu.make_async_copy(gate_hbm, gate, local_sem.at[4]),
        pltpu.make_async_copy(up_hbm, up, local_sem.at[5]),
        pltpu.make_async_copy(down_hbm, down, local_sem.at[6]),
    ]

    early_copies = [
        pltpu.make_async_copy(routes_hbm, routes, local_sem.at[9]),
        pltpu.make_async_copy(route_weights_hbm, route_weights, local_sem.at[10]),
        pltpu.make_async_copy(in_gain_hbm, in_gain, local_sem.at[11]),
    ]
    mixer_copies += [
        pltpu.make_async_copy(pool_scale_hbm, pool_scale, local_sem.at[12]),
        pltpu.make_async_copy(mix_gain_hbm, mix_gain, local_sem.at[13]),
        pltpu.make_async_copy(out_gain_hbm, out_gain, local_sem.at[14]),
    ]
    for copy in early_copies:
        copy.start()
    tokens_copy.start()
    pool_copy.start()

    barrier = pltpu.get_barrier_semaphore()

    def greet(d, carry):
        pl.semaphore_signal(barrier, inc=1, device_id=(partner_ep(d), tp), device_id_type=MESH)
        return carry

    lax.fori_loop(1, ep_size, greet, 0)
    for k in range(1, highs):
        pl.semaphore_signal(
            barrier, inc=1, device_id=(ep, peer_high(k) * 2 + lo), device_id_type=MESH
        )
    pl.semaphore_signal(barrier, inc=1, device_id=(ep, hi * 2 + other), device_id_type=MESH)
    for copy in mixer_copies + weight_copies:
        copy.start()

    expert_id = lax.broadcasted_iota(jnp.int32, (experts, tok_dev), 0)
    first_slot = (
        lax.div(expert_id, exp_dev) * rows + lax.rem(expert_id, exp_dev) * capacity
    ).astype(F32)
    earlier = (
        lax.broadcasted_iota(jnp.int32, (tok_dev, tok_dev), 0)
        < lax.broadcasted_iota(jnp.int32, (tok_dev, tok_dev), 1)
    ).astype(BF16)

    def tokens_of(index):
        return pl.ds(pl.multiple_of(index * tok_dev, tok_dev), tok_dev)

    def find_slots(index, base):
        block_routes = routes[:, tokens_of(index)]
        taken = jnp.zeros((experts, 1), F32)
        found = []
        for k in range(top_count):
            named = (block_routes[k : k + 1, :] == expert_id).astype(F32)
            before = jnp.dot(named.astype(BF16), earlier, preferred_element_type=F32)
            slot = jnp.sum(named * (before + taken + first_slot), axis=0, keepdims=True)
            taken = taken + jnp.sum(named, axis=1, keepdims=True)
            found.append(slot)
            slot_rows[base + k : base + k + 1, :] = slot.astype(jnp.int32)
        return found

    for copy in early_copies:
        copy.wait()
    tokens_copy.wait()
    normed[...] = rms_scale(tokens[...].astype(F32), in_gain[...]).astype(BF16)
    pool_copy.wait()
    pl.semaphore_wait(barrier, ep_size - 1 + highs)
    if tabled:
        for k in range(1, highs):
            raw_copy(k).start()

    @pl.when(ep < ep_size - 1)
    def _():
        send_history.start()

    slot_list = find_slots(tp, 0)
    own_weights = route_weights[:, tokens_of(tp)]
    stacked = jnp.concatenate(
        slot_list
        + [own_weights[k : k + 1, :] for k in range(top_count)]
        + [jnp.zeros((columns_of.shape[1] - 2 * top_count, tok_dev), F32)],
        axis=0,
    )
    columns_of[...] = stacked.T

    def routed_rows(owner, base, source):
        slot_id = lax.broadcasted_iota(jnp.int32, (rows, tok_dev), 0) + owner * rows
        chosen = slot_rows[base : base + 1, :] == slot_id
        for k in range(1, top_count):
            chosen = chosen | (slot_rows[base + k : base + k + 1, :] == slot_id)
        return jnp.dot(
            chosen.astype(F32).astype(BF16), source[...], preferred_element_type=F32
        ).astype(BF16)

    column_step = min(width, 512)

    def mixer_part():
        for copy in mixer_copies:
            copy.wait()

        @pl.when(ep > 0)
        def _():
            send_history.wait_recv()

        @pl.when(ep == 0)
        def _():
            history[...] = jnp.zeros(history.shape, BF16)

        values = pool[...].astype(F32)
        running = jnp.concatenate([history[...].astype(F32), values], axis=0)
        summed = None
        for group in range(tp_size):
            running = running + pltpu.roll(running, 2**group, 0)
            current = running[history_rows:]
            summed = current if summed is None else jnp.where(tp == group, current, summed)
        window = jnp.int32(1)
        for group in range(tp_size):
            window = jnp.where(tp == group, 2 ** (group + 1), window)
        position = ep * rows_a + lax.broadcasted_iota(jnp.int32, values.shape, 0)
        divisor = jnp.minimum(position + 1, window).astype(F32)
        pooled = (summed / divisor - values).astype(BF16)
        grouped = (
            jnp.dot(pooled, group_w[0], preferred_element_type=F32) * pool_scale[...]
        ).astype(BF16)
        mix_rows = rows_a // tp_size
        for start in range(0, width, column_step):
            columns = slice(start, start + column_step)
            mix_held[:, :, columns] = (
                jnp.dot(grouped, out_w[:, columns], preferred_element_type=F32)
                .astype(BF16)
                .reshape(tp_size, mix_rows, column_step)
            )
        for high in range(highs):
            mix_core_copy(high).start()
        for high in range(highs):
            mix_core_copy(high).wait_recv()
        for high in range(highs):
            mix_sum[high] = (
                mix_held[high * 2 + lo].astype(F32) + mix_core[high].astype(F32)
            ).astype(BF16)
        for k in range(1, highs):
            mix_cross_copy(k).start()

    def stage_a(d):
        def cross():
            for k in range(1, highs):
                gather_cross(d, k).start()

        if tabled:
            pl.when(d >= NEAR)(cross)
        else:
            cross()
        gather_core(d, hi).start()

    def peer_blocks():
        for k in range(1, highs):
            base = k * top_count
            source = raw.at[k - 1]
            find_slots(peer_high(k) * 2 + lo, base)
            raw_copy_in(k).wait_recv()

            def send_near(d, carry):
                near_out[d, k - 1] = routed_rows(partner_ep(d), base, source)
                near_copy(d, k).start()
                return carry

            lax.fori_loop(1, NEAR, send_near, 0)
            arrived[0, peer_high(k) * 2 + lo] = routed_rows(ep, base, source)

    arrived[0, tp] = routed_rows(ep, 0, normed)
    stage_a(jnp.int32(0))

    def send_out(i, carry):
        d = sent_at(i)
        peer = partner_ep(d)
        outgoing[peer] = routed_rows(peer, 0, normed)
        dispatch(d).start()
        return carry

    lax.fori_loop(0, ep_size - 1, send_out, 0)

    def gather_next(d):
        dispatch(d).wait_recv()
        stage_a(d)

    if not tabled:
        gather_next(offset_of(ep * 0))
    for copy in weight_copies:
        copy.wait()
    total_rows[...] = jnp.zeros(total_rows.shape, F32)

    spans = []
    for e in range(exp_dev):
        begin = e * capacity // ROW_TILE * ROW_TILE
        end = -(-(e + 1) * capacity // ROW_TILE) * ROW_TILE
        spans.append((begin, end))
    edges = sorted({0, rows} | {edge for span in spans for edge in span})

    def experts_on(d):
        hidden = []
        for e, (begin, end) in enumerate(spans):
            count = end - begin
            block = arrived[d, :, begin:end, :].reshape(tp_size * count, width)
            gate_act = jnp.dot(block, gate[e], preferred_element_type=F32)
            up_act = jnp.dot(block, up[e], preferred_element_type=F32)
            act = gate_act / (1.0 + jnp.exp(-gate_act)) * up_act
            place = begin + lax.rem(
                lax.broadcasted_iota(jnp.int32, (tp_size * count, 1), 0), count
            )
            mine = (place >= e * capacity) & (place < (e + 1) * capacity)
            hidden.append(jnp.where(mine, act, 0.0).astype(BF16))
        for start in range(0, width, column_step):
            columns = slice(start, start + column_step)
            outs = []
            for e, (begin, end) in enumerate(spans):
                out = jnp.dot(hidden[e], down[e, :, columns], preferred_element_type=F32)
                outs.append(out.reshape(tp_size, end - begin, column_step))
            for begin, end in zip(edges[:-1], edges[1:]):
                piece = None
                for (first_row, last_row), out in zip(spans, outs):
                    if first_row <= begin and end <= last_row:
                        held = out[:, begin - first_row : end - first_row]
                        piece = held if piece is None else piece + held
                if piece is None:
                    piece = jnp.zeros((tp_size, end - begin, column_step), F32)
                part[:, begin:end, columns] = piece.astype(BF16)

    def combine(owner, block):
        lane = lax.broadcasted_iota(jnp.int32, (tok_dev, 2 * rows), 1)
        slot_id = (lax.rem(lane, rows) + owner * rows).astype(F32)
        weights = jnp.zeros((tok_dev, 2 * rows), F32)
        for k in range(top_count):
            weights = weights + jnp.where(
                columns_of[:, k : k + 1] == slot_id,
                columns_of[:, top_count + k : top_count + k + 1],
                0.0,
            )
        major = weights.astype(BF16).astype(F32)
        split = jnp.where(lane < rows, major, weights - major).astype(BF16)
        for start in range(0, width, column_step):
            columns = slice(start, start + column_step)
            held = block[:, columns]
            twice = jnp.concatenate([held, held], axis=0)
            total_rows[:, columns] += jnp.dot(split, twice, preferred_element_type=F32)

    def combine_from(d):
        give_back(d).wait_recv()
        combine(partner_ep(d), returned.at[d])

    def forward(d):
        for k in range(1, highs):

            def arrival():
                gather_cross_in(d, k).wait_recv()

            if tabled:
                pl.when(d != 0)(arrival)
            else:
                arrival()
            gather_core(d, peer_high(k)).start()

    def compute(d):
        for high in range(highs):
            gather_core_in(d, high).wait_recv()
        experts_on(d)
        for high in range(highs):
            reduce_core(d, high).start()

    def reduce(d):
        for high in range(highs):
            reduce_core(d, high).wait_recv()
            reduce_core(d, high).wait_send()
            core_in[d, high] = (
                part[high * 2 + lo].astype(F32) + core_in[d, high].astype(F32)
            ).astype(BF16)
        for k in range(1, highs):
            reduce_cross(d, k).start()

    def send_home(d):
        total = core_in[d, hi].astype(F32)
        for k in range(1, highs):
            reduce_cross_in(d, k).wait_recv()
            total = total + cross_in[d, k - 1].astype(F32)
        core_in[d, hi] = total.astype(BF16)

        @pl.when(d != 0)
        def _():
            give_back(d).start()

    def mixer_end():
        total = mix_sum[hi].astype(F32)
        for k in range(1, highs):
            mix_cross_in(k).wait_recv()
            total = total + mix_cross[k - 1].astype(F32)
        mixer_out[...] = rms_scale(total, mix_gain[...]).astype(BF16)

    actions = {
        GATHER: gather_next,
        FORWARD: forward,
        COMPUTE: compute,
        REDUCE: reduce,
        RETURN: send_home,
        COMBINE: combine_from,
        MIX: lambda d: mixer_part(),
        PEER: lambda d: peer_blocks(),
    }

    if not tabled:
        del actions[PEER]

    def event(t, carry):
        op, d = event_at(t)
        for kind, action in actions.items():
            pl.when(op == kind)(functools.partial(action, d))
        return carry

    count = len(END_EVENTS) if tabled else 8 * (ep_size + 3)
    lax.fori_loop(0, count, event, 0)

    if not tabled:

        def late(j, carry):
            combine_from(offset_of(j))
            return carry

        lax.fori_loop(max(0, ep_size - 5), ep_size - 1, late, 0)
    combine(ep, core_in.at[0, hi])
    moe_out[...] = rms_scale(total_rows[...], out_gain[...]).astype(BF16)

    for high in range(highs):
        mix_core_copy(high).wait_send()

    @pl.when(ep < ep_size - 1)
    def _():
        send_history.wait_send()

    if tabled:
        for k in range(1, highs):
            raw_copy(k).wait_send()

    def drain_all(d, carry):
        for k in range(1, highs):

            def gathered():
                gather_cross(d, k).wait_send()

            if tabled:
                pl.when(d != 0)(gathered)
            else:
                gathered()
            reduce_cross(d, k).wait_send()
        for high in range(highs):
            gather_core(d, high).wait_send()
        return carry

    lax.fori_loop(0, ep_size, drain_all, 0)

    def drain(d, carry):
        dispatch(d).wait_send()
        give_back(d).wait_send()
        return carry

    lax.fori_loop(1, ep_size, drain, 0)
    mixer_end()
    for k in range(1, highs):
        mix_cross_copy(k).wait_send()


def on_device(
    pool_input,
    group_weight,
    pool_scale,
    out_weight,
    mix_gain,
    expert_input,
    routes,
    route_weights,
    moe_in_gain,
    gate_weight,
    up_weight,
    down_weight,
    moe_out_gain,
):
    tp_size = lax.axis_size("tp")
    ep_size = lax.axis_size("ep")
    rows_a, group_width = pool_input.shape
    width = out_weight.shape[1]
    exp_dev = gate_weight.shape[0]
    experts = exp_dev * ep_size
    tok_dev = expert_input.shape[0]
    top_count = routes.shape[1]
    capacity = max(2, 5 * tok_dev * top_count // (4 * experts))
    rows = -(-exp_dev * capacity // ROW_TILE) * ROW_TILE
    highs = tp_size // 2
    mix_rows = rows_a // tp_size
    history_rows = 2**tp_size
    tabled = ep_size == 8
    raw_rows = tok_dev if tabled else ROW_TILE
    near_rows = rows if tabled else ROW_TILE
    vmem_spec = pl.BlockSpec(memory_space=pltpu.VMEM)
    hbm_spec = pl.BlockSpec(memory_space=pltpu.HBM)
    dma = pltpu.SemaphoreType.DMA
    pair = (ep_size, highs)
    flops = 6 * gate_weight.size * ep_size * tp_size * rows
    scratch = [
        pltpu.VMEM((1, group_width), F32),
        pltpu.VMEM((1, width), F32),
        pltpu.VMEM((top_count, tok_dev * tp_size), jnp.int32),
        pltpu.VMEM((top_count, tok_dev * tp_size), F32),
        pltpu.VMEM((1, width), F32),
        pltpu.VMEM((1, width), F32),
        pltpu.VMEM(pool_input.shape, BF16),
        pltpu.VMEM((history_rows, group_width), BF16),
        pltpu.VMEM(group_weight.shape, BF16),
        pltpu.VMEM(out_weight.shape, BF16),
        pltpu.VMEM(expert_input.shape, BF16),
        pltpu.VMEM(expert_input.shape, BF16),
        pltpu.VMEM((highs - 1, raw_rows, width), BF16),
        pltpu.VMEM((NEAR, highs - 1, near_rows, width), BF16),
        pltpu.VMEM((8, tok_dev), jnp.int32),
        pltpu.VMEM((tok_dev, 8), F32),
        pltpu.VMEM((ep_size, rows, width), BF16),
        pltpu.VMEM((ep_size, tp_size, rows, width), BF16),
        pltpu.VMEM((tp_size, rows, width), BF16),
        pltpu.VMEM((ep_size, highs, rows, width), BF16),
        pltpu.VMEM((ep_size, highs - 1, rows, width), BF16),
        pltpu.VMEM((ep_size, rows, width), BF16),
        pltpu.VMEM(expert_input.shape, F32),
        pltpu.VMEM(gate_weight.shape, BF16),
        pltpu.VMEM(up_weight.shape, BF16),
        pltpu.VMEM(down_weight.shape, BF16),
        pltpu.VMEM((tp_size, mix_rows, width), BF16),
        pltpu.VMEM((highs, mix_rows, width), BF16),
        pltpu.VMEM((highs, mix_rows, width), BF16),
        pltpu.VMEM((highs - 1, mix_rows, width), BF16),
        dma((15,)),
        dma((2,)),
        dma((highs,)),
        dma((highs,)),
        dma((ep_size,)),
        dma((ep_size,)),
        dma(pair),
        dma(pair),
        dma(pair),
        dma(pair),
        dma(pair),
        dma(pair),
        dma(pair),
        dma(pair),
        dma((ep_size,)),
        dma((ep_size,)),
        dma((highs,)),
        dma((highs,)),
        dma((highs,)),
        dma((highs,)),
    ]
    held = sum(
        ref.dtype.itemsize * math.prod(ref.shape)
        for ref in scratch
        if ref.memory_space == pltpu.VMEM
    )
    mixer_out, moe_out = pl.pallas_call(
        functools.partial(fused_kernel, capacity),
        out_shape=(
            pltpu.VMEM((mix_rows, width), BF16),
            pltpu.VMEM((tok_dev, width), BF16),
        ),
        in_specs=[hbm_spec] * 13,
        out_specs=(vmem_spec, vmem_spec),
        scratch_shapes=scratch,
        compiler_params=pltpu.CompilerParams(
            collective_id=0, has_side_effects=True, vmem_limit_bytes=max(ROOM, held + SPARE)
        ),
        cost_estimate=pl.CostEstimate(
            flops=flops, bytes_accessed=8 * expert_input.size, transcendentals=0
        ),
    )(
        pool_input,
        group_weight,
        pool_scale.reshape(1, -1),
        out_weight,
        mix_gain.reshape(1, -1),
        expert_input,
        routes.T,
        route_weights.T,
        moe_in_gain.reshape(1, -1),
        gate_weight,
        up_weight,
        down_weight,
        moe_out_gain.reshape(1, -1),
    )
    return (mixer_out, moe_out)


def solution(mesh):
    in_specs = (
        P("ep", "tp"),
        P("tp", None, None),
        P("tp"),
        P("tp", None),
        P(),
        P(("ep", "tp"), None),
        P("ep", None),
        P("ep", None),
        P(),
        P("ep", None, "tp"),
        P("ep", None, "tp"),
        P("ep", "tp", None),
        P(),
    )
    out_specs = (P(("ep", "tp"), None), P(("ep", "tp"), None))
    return jax.shard_map(
        on_device, mesh=mesh, in_specs=in_specs, out_specs=out_specs, check_vma=False
    )
```

```python
import functools
import math

import jax
import jax.numpy as jnp
from jax import lax
from jax.experimental import pallas as pl
from jax.experimental.pallas import tpu as pltpu
from jax.sharding import PartitionSpec as P

NORM_EPS = 1e-06
ROOM = 56 * 1024 * 1024
SPARE = 3 * 1024 * 1024
MESH = pl.DeviceIdType.MESH
F32 = jnp.float32
BF16 = jnp.bfloat16
ROW_TILE = 16
GATHER, FORWARD, COMPUTE, REDUCE, RETURN, COMBINE, MIX, PEER, NONE = range(9)
KINDS = {
    "A": GATHER,
    "X": FORWARD,
    "C": COMPUTE,
    "R": REDUCE,
    "F": RETURN,
    "B": COMBINE,
    "M": MIX,
    "P": PEER,
}
STEADY = (
    (GATHER, -1, 1),
    (FORWARD, 0, 0),
    (RETURN, 3, 0),
    (REDUCE, 1, 0),
    (COMPUTE, 0, 0),
    (COMBINE, 8, 1),
)
CODE_BITS = 6
NEAR = 4
PER_WORD = 5


def coded(*events):
    return tuple(KINDS[event[0]] * 8 + int(event[1:] or 0) for event in events)


END_EVENTS = coded(
    "A6", "A7", "A1", "P", "A3", "X6", "C6", "R6", "X7", "C7", "R7", "F6", "A4", "F7", "A5",
    "X4", "C4", "R4", "X5", "C5", "R5", "F4", "A2", "X1", "C1", "R1", "F5", "X3", "C3", "R3",
    "F1", "X2", "C2", "R2", "F3", "X0", "C0", "R0", "M", "F2", "B6", "B7", "B4", "B5", "B1",
    "B3", "F0", "B2",
)
MIDDLE_EVENTS = coded(
    "A1", "A4", "P", "A5", "X4", "C4", "R4", "X5", "C5", "R5", "F4", "X0", "C0", "R0", "F5",
    "A6", "X1", "C1", "R1", "F0", "X6", "C6", "R6", "A7", "A3", "F1", "X3", "C3", "R3", "F6",
    "A2", "X7", "C7", "R7", "F3", "X2", "C2", "R2", "F7", "M", "B4", "B5", "F2", "B1", "B3",
    "B6", "B7", "B2",
)
END_SENDS = (1, 6, 7, 4, 5, 3, 2)
MIDDLE_SENDS = (1, 4, 5, 6, 7, 3, 2)

def rms_scale(values, gain_vec):
    mean_sq = jnp.mean(values * values, axis=-1, keepdims=True)
    return values * lax.rsqrt(mean_sq + NORM_EPS) * gain_vec


def fused_kernel(
    capacity,
    pool_hbm,
    group_hbm,
    pool_scale_hbm,
    out_w_hbm,
    mix_gain_hbm,
    tokens_hbm,
    routes_hbm,
    route_weights_hbm,
    in_gain_hbm,
    gate_hbm,
    up_hbm,
    down_hbm,
    out_gain_hbm,
    mixer_out,
    moe_out,
    pool_scale,
    mix_gain,
    routes,
    route_weights,
    in_gain,
    out_gain,
    pool,
    history,
    group_w,
    out_w,
    tokens,
    normed,
    raw,
    near_out,
    slot_rows,
    columns_of,
    outgoing,
    arrived,
    part,
    core_in,
    cross_in,
    returned,
    total_rows,
    gate,
    up,
    down,
    mix_held,
    mix_core,
    mix_sum,
    mix_cross,
    mix_done,
    local_sem,
    hist_sem,
    raw_send,
    raw_recv,
    dis_send,
    dis_recv,
    y1_send,
    y1_recv,
    c1_send,
    c1_recv,
    c2_send,
    c2_recv,
    y2_send,
    y2_recv,
    ret_send,
    ret_recv,
    m1_send,
    m1_recv,
    m2_send,
    m2_recv,
):
    ep_size, tp_size, rows, width = arrived.shape
    exp_dev, _, ff_dev = gate.shape
    tok_dev = tokens.shape[0]
    top_count = routes.shape[0]
    experts = exp_dev * ep_size
    rows_a = pool.shape[0]
    history_rows = history.shape[0]
    highs = tp_size // 2
    ep = lax.axis_index("ep")
    tp = lax.axis_index("tp")
    hi, lo = tp // 2, tp % 2
    other = 1 - lo

    def remote(src, dst, send, recv, to_ep, to_tp):
        return pltpu.make_async_remote_copy(
            src_ref=src,
            dst_ref=dst,
            send_sem=send,
            recv_sem=recv,
            device_id=(to_ep, to_tp),
            device_id_type=MESH,
        )

    def peer_high(k):
        return lax.rem(hi + k, highs)

    on_end = (ep // 2) % 2 == (ep // 4) % 2
    tabled = ep_size == 8

    def packed_at(table, i):
        words = []
        for begin in range(0, len(table), PER_WORD):
            piece = table[begin : begin + PER_WORD]
            words.append(sum(value << (CODE_BITS * at) for at, value in enumerate(piece)))
        word = jnp.int32(words[0])
        for at in range(1, len(words)):
            word = jnp.where(i >= at * PER_WORD, words[at], word)
        shift = CODE_BITS * lax.rem(i, PER_WORD)
        return lax.rem(lax.shift_right_logical(word, shift), 1 << CODE_BITS)

    def offset_of(i):
        far = jnp.where(i == 0, 1, ep_size - i)
        return jnp.where(i == ep_size - 1, 0, far)

    def sent_at(i):
        if tabled:
            return jnp.where(on_end, packed_at(END_SENDS, i), packed_at(MIDDLE_SENDS, i))
        return offset_of(i)

    def event_at(t):
        if tabled:
            code = jnp.where(on_end, packed_at(END_EVENTS, t), packed_at(MIDDLE_EVENTS, t))
            return code // 8, code % 8
        i, slot = t // 8, t % 8
        op, j = jnp.int32(NONE), i
        for at, (kind, lag, last) in enumerate(STEADY):
            index = i - lag
            valid = (slot == at) & (index >= 0) & (index < ep_size - last)
            op = jnp.where(valid, kind, op)
            j = jnp.where(valid, index, j)
        op = jnp.where((slot == 6) & (i == 0), MIX, op)
        return op, offset_of(j)

    def partner_ep(d):
        value = ep * 0
        bit = 1
        while bit < ep_size:
            value = value + bit * (((ep // bit) % 2 + (d // bit) % 2) % 2)
            bit *= 2
        return value

    def dispatch(d):
        peer = partner_ep(d)
        return remote(
            outgoing.at[peer], arrived.at[d, tp], dis_send.at[0], dis_recv.at[d], peer, tp
        )

    def gather_cross(d, k):
        slot = arrived.at[d, tp]
        return remote(
            slot, slot, y1_send.at[k - 1], y1_recv.at[d, highs - k - 1], ep, peer_high(k) * 2 + lo
        )

    def gather_cross_in(d, k):
        high = peer_high(k)
        slot = arrived.at[d, high * 2 + lo]
        return remote(slot, slot, y1_send.at[k - 1], y1_recv.at[d, k - 1], ep, high * 2 + lo)

    def gather_core(d, high):
        slot = arrived.at[d, high * 2 + lo]
        return remote(slot, slot, c1_send.at[0], c1_recv.at[d], ep, hi * 2 + other)

    def gather_core_in(d):
        slots = arrived.at[d, 0:highs]
        return remote(slots, slots, c1_send.at[0], c1_recv.at[d], ep, hi * 2 + other)

    def reduce_core(d, high):
        return remote(
            part.at[high * 2 + other],
            core_in.at[d, high],
            c2_send.at[0],
            c2_recv.at[d],
            ep,
            hi * 2 + other,
        )

    def reduce_core_all(d):
        return remote(
            part.at[0:highs],
            core_in.at[d],
            c2_send.at[0],
            c2_recv.at[d],
            ep,
            hi * 2 + other,
        )

    def reduce_cross(d, k):
        high = peer_high(k)
        return remote(
            core_in.at[d, high],
            cross_in.at[d, highs - k - 1],
            y2_send.at[k - 1],
            y2_recv.at[d, highs - k - 1],
            ep,
            high * 2 + lo,
        )

    def reduce_cross_in(d, k):
        high = peer_high(k)
        return remote(
            core_in.at[d, high],
            cross_in.at[d, k - 1],
            y2_send.at[k - 1],
            y2_recv.at[d, k - 1],
            ep,
            high * 2 + lo,
        )

    def raw_copy(k):
        return remote(
            normed,
            raw.at[highs - k - 1],
            raw_send.at[k - 1],
            raw_recv.at[highs - k - 1],
            ep,
            peer_high(k) * 2 + lo,
        )

    def raw_copy_in(k):
        return remote(
            normed, raw.at[k - 1], raw_send.at[k - 1], raw_recv.at[k - 1], ep, peer_high(k) * 2 + lo
        )

    def near_copy(d, k):
        return remote(
            near_out.at[d, k - 1],
            arrived.at[d, peer_high(k) * 2 + lo],
            y1_send.at[k - 1],
            y1_recv.at[d, k - 1],
            partner_ep(d),
            tp,
        )

    def give_back(d):
        peer = partner_ep(d)
        return remote(core_in.at[d, hi], returned.at[d], ret_send.at[0], ret_recv.at[d], peer, tp)

    def mix_core_copy(high):
        return remote(
            mix_held.at[high * 2 + other],
            mix_core.at[high],
            m1_send.at[0],
            m1_recv.at[0],
            ep,
            hi * 2 + other,
        )

    def mix_core_all():
        return remote(
            mix_held.at[0:highs], mix_core, m1_send.at[0], m1_recv.at[0], ep, hi * 2 + other
        )

    def mix_cross_copy(k):
        high = peer_high(k)
        return remote(
            mix_sum.at[high],
            mix_cross.at[highs - k - 1],
            m2_send.at[k - 1],
            m2_recv.at[highs - k - 1],
            ep,
            high * 2 + lo,
        )

    def mix_cross_in(k):
        high = peer_high(k)
        return remote(
            mix_sum.at[high],
            mix_cross.at[k - 1],
            m2_send.at[k - 1],
            m2_recv.at[k - 1],
            ep,
            high * 2 + lo,
        )

    last_rows = pool.at[rows_a - history_rows :]
    send_history = remote(
        last_rows, history, hist_sem.at[0], hist_sem.at[1], jnp.minimum(ep + 1, ep_size - 1), tp
    )

    half_rows = mix_done.shape[0] // 2
    mixer_stores = [
        pltpu.make_async_copy(
            mix_done.at[half * half_rows : (half + 1) * half_rows],
            mixer_out.at[half * half_rows : (half + 1) * half_rows],
            local_sem.at[7 + half],
        )
        for half in range(2)
    ]
    moe_store = pltpu.make_async_copy(normed, moe_out, local_sem.at[15])
    tokens_copy = pltpu.make_async_copy(tokens_hbm, tokens, local_sem.at[0])
    pool_copy = pltpu.make_async_copy(pool_hbm, pool, local_sem.at[1])
    mixer_copies = [
        pltpu.make_async_copy(group_hbm, group_w, local_sem.at[2]),
        pltpu.make_async_copy(out_w_hbm, out_w, local_sem.at[3]),
    ]
    weight_copies = [
        pltpu.make_async_copy(gate_hbm, gate, local_sem.at[4]),
        pltpu.make_async_copy(up_hbm, up, local_sem.at[5]),
        pltpu.make_async_copy(down_hbm, down, local_sem.at[6]),
    ]

    early_copies = [
        pltpu.make_async_copy(routes_hbm, routes, local_sem.at[9]),
        pltpu.make_async_copy(route_weights_hbm, route_weights, local_sem.at[10]),
        pltpu.make_async_copy(in_gain_hbm, in_gain, local_sem.at[11]),
    ]
    mixer_copies += [
        pltpu.make_async_copy(pool_scale_hbm, pool_scale, local_sem.at[12]),
        pltpu.make_async_copy(mix_gain_hbm, mix_gain, local_sem.at[13]),
        pltpu.make_async_copy(out_gain_hbm, out_gain, local_sem.at[14]),
    ]
    for copy in early_copies:
        copy.start()
    tokens_copy.start()
    pool_copy.start()

    barrier = pltpu.get_barrier_semaphore()

    def greet(d, carry):
        pl.semaphore_signal(barrier, inc=1, device_id=(partner_ep(d), tp), device_id_type=MESH)
        return carry

    lax.fori_loop(1, ep_size, greet, 0)
    for k in range(1, highs):
        pl.semaphore_signal(
            barrier, inc=1, device_id=(ep, peer_high(k) * 2 + lo), device_id_type=MESH
        )
    pl.semaphore_signal(barrier, inc=1, device_id=(ep, hi * 2 + other), device_id_type=MESH)
    for copy in mixer_copies + weight_copies:
        copy.start()

    expert_id = lax.broadcasted_iota(jnp.int32, (experts, tok_dev), 0)
    first_slot = (
        lax.div(expert_id, exp_dev) * rows + lax.rem(expert_id, exp_dev) * capacity
    ).astype(F32)
    earlier = (
        lax.broadcasted_iota(jnp.int32, (tok_dev, tok_dev), 0)
        < lax.broadcasted_iota(jnp.int32, (tok_dev, tok_dev), 1)
    ).astype(BF16)

    def tokens_of(index):
        return pl.ds(pl.multiple_of(index * tok_dev, tok_dev), tok_dev)

    def find_slots(index, base):
        block_routes = routes[:, tokens_of(index)]
        taken = jnp.zeros((experts, 1), F32)
        found = []
        for k in range(top_count):
            named = (block_routes[k : k + 1, :] == expert_id).astype(F32)
            before = jnp.dot(named.astype(BF16), earlier, preferred_element_type=F32)
            slot = jnp.sum(named * (before + taken + first_slot), axis=0, keepdims=True)
            taken = taken + jnp.sum(named, axis=1, keepdims=True)
            found.append(slot)
            slot_rows[base + k : base + k + 1, :] = slot.astype(jnp.int32)
        return found

    for copy in early_copies:
        copy.wait()
    tokens_copy.wait()
    normed[...] = rms_scale(tokens[...].astype(F32), in_gain[...]).astype(BF16)
    pool_copy.wait()
    pl.semaphore_wait(barrier, ep_size - 1 + highs)
    if tabled:
        for k in range(1, highs):
            raw_copy(k).start()

    @pl.when(ep < ep_size - 1)
    def _():
        send_history.start()

    slot_list = find_slots(tp, 0)
    own_weights = route_weights[:, tokens_of(tp)]
    stacked = jnp.concatenate(
        slot_list
        + [own_weights[k : k + 1, :] for k in range(top_count)]
        + [jnp.zeros((columns_of.shape[1] - 2 * top_count, tok_dev), F32)],
        axis=0,
    )
    columns_of[...] = stacked.T

    def routed_rows(owner, base, source):
        slot_id = lax.broadcasted_iota(jnp.int32, (rows, tok_dev), 0) + owner * rows
        chosen = slot_rows[base : base + 1, :] == slot_id
        for k in range(1, top_count):
            chosen = chosen | (slot_rows[base + k : base + k + 1, :] == slot_id)
        return jnp.dot(
            chosen.astype(F32).astype(BF16), source[...], preferred_element_type=F32
        ).astype(BF16)

    column_step = min(width, 512)

    def mixer_part():
        for copy in mixer_copies:
            copy.wait()

        @pl.when(ep > 0)
        def _():
            send_history.wait_recv()

        @pl.when(ep == 0)
        def _():
            history[...] = jnp.zeros(history.shape, BF16)

        values = pool[...].astype(F32)
        running = jnp.concatenate([history[...].astype(F32), values], axis=0)
        summed = None
        for group in range(tp_size):
            running = running + pltpu.roll(running, 2**group, 0)
            current = running[history_rows:]
            summed = current if summed is None else jnp.where(tp == group, current, summed)
        window = jnp.int32(1)
        for group in range(tp_size):
            window = jnp.where(tp == group, 2 ** (group + 1), window)
        position = ep * rows_a + lax.broadcasted_iota(jnp.int32, values.shape, 0)
        divisor = jnp.minimum(position + 1, window).astype(F32)
        pooled = (summed / divisor - values).astype(BF16)
        grouped = (
            jnp.dot(pooled, group_w[0], preferred_element_type=F32) * pool_scale[...]
        ).astype(BF16)
        mix_rows = rows_a // tp_size
        for start in range(0, width, column_step):
            columns = slice(start, start + column_step)
            mix_held[:, :, columns] = (
                jnp.dot(grouped, out_w[:, columns], preferred_element_type=F32)
                .astype(BF16)
                .reshape(tp_size, mix_rows, column_step)
            )
        for high in range(highs):
            mix_core_copy(high).start()
        mix_core_all().wait_recv()
        for high in range(highs):
            mix_sum[high] = (
                mix_held[high * 2 + lo].astype(F32) + mix_core[high].astype(F32)
            ).astype(BF16)
        for k in range(1, highs):
            mix_cross_copy(k).start()

    def stage_a(d):
        def cross():
            for k in range(1, highs):
                gather_cross(d, k).start()

        if tabled:
            pl.when(d >= NEAR)(cross)
        else:
            cross()
        gather_core(d, hi).start()

    def peer_blocks():
        for k in range(1, highs):
            base = k * top_count
            source = raw.at[k - 1]
            find_slots(peer_high(k) * 2 + lo, base)
            raw_copy_in(k).wait_recv()

            def send_near(d, carry):
                near_out[d, k - 1] = routed_rows(partner_ep(d), base, source)
                near_copy(d, k).start()
                return carry

            lax.fori_loop(1, NEAR, send_near, 0)
            arrived[0, peer_high(k) * 2 + lo] = routed_rows(ep, base, source)

    arrived[0, tp] = routed_rows(ep, 0, normed)
    stage_a(jnp.int32(0))

    def send_out(i, carry):
        d = sent_at(i)
        peer = partner_ep(d)
        outgoing[peer] = routed_rows(peer, 0, normed)
        dispatch(d).start()
        return carry

    lax.fori_loop(0, ep_size - 1, send_out, 0)

    def gather_next(d):
        dispatch(d).wait_recv()
        stage_a(d)

    if not tabled:
        gather_next(offset_of(ep * 0))
    for copy in weight_copies:
        copy.wait()
    total_rows[...] = jnp.zeros(total_rows.shape, F32)

    spans = []
    for e in range(exp_dev):
        begin = e * capacity // ROW_TILE * ROW_TILE
        end = -(-(e + 1) * capacity // ROW_TILE) * ROW_TILE
        spans.append((begin, end))
    edges = sorted({0, rows} | {edge for span in spans for edge in span})

    def experts_on(d):
        hidden = []
        for e, (begin, end) in enumerate(spans):
            count = end - begin
            block = arrived[d, :, begin:end, :].reshape(tp_size * count, width)
            gate_act = jnp.dot(block, gate[e], preferred_element_type=F32)
            up_act = jnp.dot(block, up[e], preferred_element_type=F32)
            act = gate_act / (1.0 + jnp.exp(-gate_act)) * up_act
            place = begin + lax.rem(
                lax.broadcasted_iota(jnp.int32, (tp_size * count, 1), 0), count
            )
            mine = (place >= e * capacity) & (place < (e + 1) * capacity)
            hidden.append(jnp.where(mine, act, 0.0).astype(BF16))
        for start in range(0, width, column_step):
            columns = slice(start, start + column_step)
            outs = []
            for e, (begin, end) in enumerate(spans):
                out = jnp.dot(hidden[e], down[e, :, columns], preferred_element_type=F32)
                outs.append(out.reshape(tp_size, end - begin, column_step))
            for begin, end in zip(edges[:-1], edges[1:]):
                piece = None
                for (first_row, last_row), out in zip(spans, outs):
                    if first_row <= begin and end <= last_row:
                        held = out[:, begin - first_row : end - first_row]
                        piece = held if piece is None else piece + held
                if piece is None:
                    piece = jnp.zeros((tp_size, end - begin, column_step), F32)
                part[:, begin:end, columns] = piece.astype(BF16)

    def combine(owner, block):
        lane = lax.broadcasted_iota(jnp.int32, (tok_dev, 2 * rows), 1)
        slot_id = (lax.rem(lane, rows) + owner * rows).astype(F32)
        weights = jnp.zeros((tok_dev, 2 * rows), F32)
        for k in range(top_count):
            weights = weights + jnp.where(
                columns_of[:, k : k + 1] == slot_id,
                columns_of[:, top_count + k : top_count + k + 1],
                0.0,
            )
        major = weights.astype(BF16).astype(F32)
        split = jnp.where(lane < rows, major, weights - major).astype(BF16)
        for start in range(0, width, column_step):
            columns = slice(start, start + column_step)
            held = block[:, columns]
            twice = jnp.concatenate([held, held], axis=0)
            total_rows[:, columns] += jnp.dot(split, twice, preferred_element_type=F32)

    def combine_from(d):
        give_back(d).wait_recv()
        combine(partner_ep(d), returned.at[d])

    def forward(d):
        for k in range(1, highs):

            def arrival():
                gather_cross_in(d, k).wait_recv()

            if tabled:
                pl.when(d != 0)(arrival)
            else:
                arrival()
            gather_core(d, peer_high(k)).start()

    def compute(d):
        gather_core_in(d).wait_recv()
        experts_on(d)
        for high in range(highs):
            reduce_core(d, high).start()

    def reduce(d):
        reduce_core_all(d).wait_recv()
        reduce_core_all(d).wait_send()
        for high in range(highs):
            core_in[d, high] = (
                part[high * 2 + lo].astype(F32) + core_in[d, high].astype(F32)
            ).astype(BF16)
        for k in range(1, highs):
            reduce_cross(d, k).start()

    def send_home(d):
        total = core_in[d, hi].astype(F32)
        for k in range(1, highs):
            reduce_cross_in(d, k).wait_recv()
            total = total + cross_in[d, k - 1].astype(F32)
        core_in[d, hi] = total.astype(BF16)

        @pl.when(d != 0)
        def _():
            give_back(d).start()

    def mixer_end():
        for k in range(1, highs):
            mix_cross_in(k).wait_recv()
        for half, store in enumerate(mixer_stores):
            span = slice(half * half_rows, (half + 1) * half_rows)
            total = mix_sum[hi, span, :].astype(F32)
            for k in range(1, highs):
                total = total + mix_cross[k - 1, span, :].astype(F32)
            mix_done[span, :] = rms_scale(total, mix_gain[...]).astype(BF16)
            store.start()

    actions = {
        GATHER: gather_next,
        FORWARD: forward,
        COMPUTE: compute,
        REDUCE: reduce,
        RETURN: send_home,
        COMBINE: combine_from,
        MIX: lambda d: mixer_part(),
        PEER: lambda d: peer_blocks(),
    }

    if not tabled:
        del actions[PEER]

    def event(t, carry):
        op, d = event_at(t)
        for kind, action in actions.items():
            pl.when(op == kind)(functools.partial(action, d))
        return carry

    count = len(END_EVENTS) if tabled else 8 * (ep_size + 3)
    lax.fori_loop(0, count, event, 0)

    if not tabled:

        def late(j, carry):
            combine_from(offset_of(j))
            return carry

        lax.fori_loop(max(0, ep_size - 5), ep_size - 1, late, 0)
    combine(ep, core_in.at[0, hi])
    if tabled:
        for k in range(1, highs):
            raw_copy(k).wait_send()
    normed[...] = rms_scale(total_rows[...], out_gain[...]).astype(BF16)
    moe_store.start()

    mix_core_all().wait_send()

    @pl.when(ep < ep_size - 1)
    def _():
        send_history.wait_send()

    def drain(blocks, sem):
        remote(blocks, blocks, sem, dis_recv.at[0], ep, hi * 2 + other).wait_send()

    others = outgoing.at[0 : ep_size - 1]
    for k in range(1, highs):
        drain(others if tabled else outgoing, y1_send.at[k - 1])
        drain(outgoing, y2_send.at[k - 1])
    drain(core_in, c1_send.at[0])
    drain(others, dis_send.at[0])
    drain(others, ret_send.at[0])
    mixer_end()
    for k in range(1, highs):
        mix_cross_copy(k).wait_send()
    moe_store.wait()
    for store in mixer_stores:
        store.wait()


def on_device(
    pool_input,
    group_weight,
    pool_scale,
    out_weight,
    mix_gain,
    expert_input,
    routes,
    route_weights,
    moe_in_gain,
    gate_weight,
    up_weight,
    down_weight,
    moe_out_gain,
):
    tp_size = lax.axis_size("tp")
    ep_size = lax.axis_size("ep")
    rows_a, group_width = pool_input.shape
    width = out_weight.shape[1]
    exp_dev = gate_weight.shape[0]
    experts = exp_dev * ep_size
    tok_dev = expert_input.shape[0]
    top_count = routes.shape[1]
    capacity = max(2, 5 * tok_dev * top_count // (4 * experts))
    rows = -(-exp_dev * capacity // ROW_TILE) * ROW_TILE
    highs = tp_size // 2
    mix_rows = rows_a // tp_size
    history_rows = 2**tp_size
    tabled = ep_size == 8
    raw_rows = tok_dev if tabled else ROW_TILE
    near_rows = rows if tabled else ROW_TILE
    any_spec = pl.BlockSpec(memory_space=pl.ANY)
    hbm_spec = pl.BlockSpec(memory_space=pltpu.HBM)
    dma = pltpu.SemaphoreType.DMA
    flops = 6 * gate_weight.size * ep_size * tp_size * rows
    scratch = [
        pltpu.VMEM((1, group_width), F32),
        pltpu.VMEM((1, width), F32),
        pltpu.VMEM((top_count, tok_dev * tp_size), jnp.int32),
        pltpu.VMEM((top_count, tok_dev * tp_size), F32),
        pltpu.VMEM((1, width), F32),
        pltpu.VMEM((1, width), F32),
        pltpu.VMEM(pool_input.shape, BF16),
        pltpu.VMEM((history_rows, group_width), BF16),
        pltpu.VMEM(group_weight.shape, BF16),
        pltpu.VMEM(out_weight.shape, BF16),
        pltpu.VMEM(expert_input.shape, BF16),
        pltpu.VMEM(expert_input.shape, BF16),
        pltpu.VMEM((highs - 1, raw_rows, width), BF16),
        pltpu.VMEM((NEAR, highs - 1, near_rows, width), BF16),
        pltpu.VMEM((8, tok_dev), jnp.int32),
        pltpu.VMEM((tok_dev, 8), F32),
        pltpu.VMEM((ep_size, rows, width), BF16),
        pltpu.VMEM((ep_size, tp_size, rows, width), BF16),
        pltpu.VMEM((tp_size, rows, width), BF16),
        pltpu.VMEM((ep_size, highs, rows, width), BF16),
        pltpu.VMEM((ep_size, highs - 1, rows, width), BF16),
        pltpu.VMEM((ep_size, rows, width), BF16),
        pltpu.VMEM(expert_input.shape, F32),
        pltpu.VMEM(gate_weight.shape, BF16),
        pltpu.VMEM(up_weight.shape, BF16),
        pltpu.VMEM(down_weight.shape, BF16),
        pltpu.VMEM((tp_size, mix_rows, width), BF16),
        pltpu.VMEM((highs, mix_rows, width), BF16),
        pltpu.VMEM((highs, mix_rows, width), BF16),
        pltpu.VMEM((highs - 1, mix_rows, width), BF16),
        pltpu.VMEM((mix_rows, width), BF16),
        dma((16,)),
        dma((2,)),
        dma((highs - 1,)),
        dma((highs - 1,)),
        dma((1,)),
        dma((ep_size,)),
        dma((highs - 1,)),
        dma((ep_size, highs - 1)),
        dma((1,)),
        dma((ep_size,)),
        dma((1,)),
        dma((ep_size,)),
        dma((highs - 1,)),
        dma((ep_size, highs - 1)),
        dma((1,)),
        dma((ep_size,)),
        dma((1,)),
        dma((1,)),
        dma((highs - 1,)),
        dma((highs - 1,)),
    ]
    held = sum(
        ref.dtype.itemsize * math.prod(ref.shape)
        for ref in scratch
        if ref.memory_space == pltpu.VMEM
    )
    mixer_out, moe_out = pl.pallas_call(
        functools.partial(fused_kernel, capacity),
        out_shape=(
            pltpu.VMEM((mix_rows, width), BF16),
            pltpu.VMEM((tok_dev, width), BF16),
        ),
        in_specs=[hbm_spec] * 13,
        out_specs=(any_spec, any_spec),
        scratch_shapes=scratch,
        compiler_params=pltpu.CompilerParams(
            collective_id=0, has_side_effects=True, vmem_limit_bytes=max(ROOM, held + SPARE)
        ),
        cost_estimate=pl.CostEstimate(
            flops=flops, bytes_accessed=8 * expert_input.size, transcendentals=0
        ),
    )(
        pool_input,
        group_weight,
        pool_scale.reshape(1, -1),
        out_weight,
        mix_gain.reshape(1, -1),
        expert_input,
        routes.T,
        route_weights.T,
        moe_in_gain.reshape(1, -1),
        gate_weight,
        up_weight,
        down_weight,
        moe_out_gain.reshape(1, -1),
    )
    return (mixer_out, moe_out)


def solution(mesh):
    in_specs = (
        P("ep", "tp"),
        P("tp", None, None),
        P("tp"),
        P("tp", None),
        P(),
        P(("ep", "tp"), None),
        P("ep", None),
        P("ep", None),
        P(),
        P("ep", None, "tp"),
        P("ep", None, "tp"),
        P("ep", "tp", None),
        P(),
    )
    out_specs = (P(("ep", "tp"), None), P(("ep", "tp"), None))
    return jax.shard_map(
        on_device, mesh=mesh, in_specs=in_specs, out_specs=out_specs, check_vma=False
    )
```

```python
import functools
import math

import jax
import jax.numpy as jnp
from jax import lax
from jax.experimental import pallas as pl
from jax.experimental.pallas import tpu as pltpu
from jax.sharding import PartitionSpec as P

NORM_EPS = 1e-06
ROOM = 56 * 1024 * 1024
SPARE = 3 * 1024 * 1024
MESH = pl.DeviceIdType.MESH
F32 = jnp.float32
BF16 = jnp.bfloat16
ROW_TILE = 16
GATHER, FORWARD, COMPUTE, REDUCE, RETURN, COMBINE, MIX, PEER, NONE = range(9)
KINDS = {
    "A": GATHER,
    "X": FORWARD,
    "C": COMPUTE,
    "R": REDUCE,
    "F": RETURN,
    "B": COMBINE,
    "M": MIX,
    "P": PEER,
}
STEADY = (
    (GATHER, -1, 1),
    (FORWARD, 0, 0),
    (RETURN, 3, 0),
    (REDUCE, 1, 0),
    (COMPUTE, 0, 0),
    (COMBINE, 8, 1),
)
CODE_BITS = 6
NEAR = 4
PER_WORD = 5


def coded(*events):
    return tuple(KINDS[event[0]] * 8 + int(event[1:] or 0) for event in events)


END_EVENTS = coded(
    "A6", "A1", "P", "A7", "A3", "X6", "C6", "R6", "X7", "C7", "R7", "F6", "A4", "F7", "A5",
    "X4", "C4", "R4", "X5", "C5", "R5", "F4", "A2", "X1", "C1", "R1", "F5", "X3", "C3", "R3",
    "F1", "X2", "C2", "R2", "F3", "X0", "C0", "R0", "M", "F2", "B6", "B7", "B4", "B5", "B1",
    "B3", "F0", "B2",
)
MIDDLE_EVENTS = coded(
    "A1", "A4", "P", "A5", "X4", "C4", "R4", "X5", "C5", "R5", "F4", "X0", "C0", "R0", "F5",
    "A6", "X1", "C1", "R1", "F0", "X6", "C6", "R6", "A7", "A3", "F1", "X3", "C3", "R3", "F6",
    "A2", "X7", "C7", "R7", "F3", "X2", "C2", "R2", "F7", "M", "B4", "B5", "F2", "B1", "B3",
    "B6", "B7", "B2",
)
END_SENDS = (1, 6, 7, 4, 5, 3, 2)
MIDDLE_SENDS = (1, 4, 5, 6, 7, 3, 2)

def rms_scale(values, gain_vec):
    mean_sq = jnp.mean(values * values, axis=-1, keepdims=True)
    return values * lax.rsqrt(mean_sq + NORM_EPS) * gain_vec


def fused_kernel(
    capacity,
    pool_hbm,
    group_hbm,
    pool_scale_hbm,
    out_w_hbm,
    mix_gain_hbm,
    tokens_hbm,
    routes_hbm,
    route_weights_hbm,
    in_gain_hbm,
    gate_hbm,
    up_hbm,
    down_hbm,
    out_gain_hbm,
    mixer_out,
    moe_out,
    pool_scale,
    mix_gain,
    routes,
    route_weights,
    in_gain,
    out_gain,
    pool,
    history,
    group_w,
    out_w,
    tokens,
    normed,
    raw,
    near_out,
    slot_rows,
    columns_of,
    outgoing,
    arrived,
    part,
    core_in,
    cross_in,
    returned,
    total_rows,
    gate,
    up,
    down,
    mix_held,
    mix_core,
    mix_sum,
    mix_cross,
    mix_done,
    local_sem,
    hist_sem,
    raw_send,
    raw_recv,
    dis_send,
    dis_recv,
    y1_send,
    y1_recv,
    c1_send,
    c1_recv,
    c2_send,
    c2_recv,
    y2_send,
    y2_recv,
    ret_send,
    ret_recv,
    m1_send,
    m1_recv,
    m2_send,
    m2_recv,
):
    ep_size, tp_size, rows, width = arrived.shape
    exp_dev, _, ff_dev = gate.shape
    tok_dev = tokens.shape[0]
    top_count = routes.shape[0]
    experts = exp_dev * ep_size
    rows_a = pool.shape[0]
    history_rows = history.shape[0]
    highs = tp_size // 2
    ep = lax.axis_index("ep")
    tp = lax.axis_index("tp")
    hi, lo = tp // 2, tp % 2
    other = 1 - lo

    def remote(src, dst, send, recv, to_ep, to_tp):
        return pltpu.make_async_remote_copy(
            src_ref=src,
            dst_ref=dst,
            send_sem=send,
            recv_sem=recv,
            device_id=(to_ep, to_tp),
            device_id_type=MESH,
        )

    def peer_high(k):
        return lax.rem(hi + k, highs)

    on_end = (ep // 2) % 2 == (ep // 4) % 2
    tabled = ep_size == 8

    def packed_at(table, i):
        words = []
        for begin in range(0, len(table), PER_WORD):
            piece = table[begin : begin + PER_WORD]
            words.append(sum(value << (CODE_BITS * at) for at, value in enumerate(piece)))
        word = jnp.int32(words[0])
        for at in range(1, len(words)):
            word = jnp.where(i >= at * PER_WORD, words[at], word)
        shift = CODE_BITS * lax.rem(i, PER_WORD)
        return lax.rem(lax.shift_right_logical(word, shift), 1 << CODE_BITS)

    def offset_of(i):
        far = jnp.where(i == 0, 1, ep_size - i)
        return jnp.where(i == ep_size - 1, 0, far)

    def sent_at(i):
        if tabled:
            return jnp.where(on_end, packed_at(END_SENDS, i), packed_at(MIDDLE_SENDS, i))
        return offset_of(i)

    def event_at(t):
        if tabled:
            code = jnp.where(on_end, packed_at(END_EVENTS, t), packed_at(MIDDLE_EVENTS, t))
            return code // 8, code % 8
        i, slot = t // 8, t % 8
        op, j = jnp.int32(NONE), i
        for at, (kind, lag, last) in enumerate(STEADY):
            index = i - lag
            valid = (slot == at) & (index >= 0) & (index < ep_size - last)
            op = jnp.where(valid, kind, op)
            j = jnp.where(valid, index, j)
        op = jnp.where((slot == 6) & (i == 0), MIX, op)
        return op, offset_of(j)

    def partner_ep(d):
        value = ep * 0
        bit = 1
        while bit < ep_size:
            value = value + bit * (((ep // bit) % 2 + (d // bit) % 2) % 2)
            bit *= 2
        return value

    def dispatch(d):
        peer = partner_ep(d)
        return remote(
            outgoing.at[peer], arrived.at[d, tp], dis_send.at[0], dis_recv.at[d], peer, tp
        )

    def gather_cross(d, k):
        slot = arrived.at[d, tp]
        return remote(
            slot, slot, y1_send.at[k - 1], y1_recv.at[d, highs - k - 1], ep, peer_high(k) * 2 + lo
        )

    def gather_cross_in(d, k):
        high = peer_high(k)
        slot = arrived.at[d, high * 2 + lo]
        return remote(slot, slot, y1_send.at[k - 1], y1_recv.at[d, k - 1], ep, high * 2 + lo)

    def gather_core(d, high):
        slot = arrived.at[d, high * 2 + lo]
        return remote(slot, slot, c1_send.at[0], c1_recv.at[d], ep, hi * 2 + other)

    def gather_core_in(d):
        slots = arrived.at[d, 0:highs]
        return remote(slots, slots, c1_send.at[0], c1_recv.at[d], ep, hi * 2 + other)

    def reduce_core(d, high):
        return remote(
            part.at[high * 2 + other],
            core_in.at[d, high],
            c2_send.at[0],
            c2_recv.at[d],
            ep,
            hi * 2 + other,
        )

    def reduce_core_all(d):
        return remote(
            part.at[0:highs],
            core_in.at[d],
            c2_send.at[0],
            c2_recv.at[d],
            ep,
            hi * 2 + other,
        )

    def reduce_cross(d, k):
        high = peer_high(k)
        return remote(
            core_in.at[d, high],
            cross_in.at[d, highs - k - 1],
            y2_send.at[k - 1],
            y2_recv.at[d, highs - k - 1],
            ep,
            high * 2 + lo,
        )

    def reduce_cross_in(d, k):
        high = peer_high(k)
        return remote(
            core_in.at[d, high],
            cross_in.at[d, k - 1],
            y2_send.at[k - 1],
            y2_recv.at[d, k - 1],
            ep,
            high * 2 + lo,
        )

    def raw_copy(k):
        return remote(
            normed,
            raw.at[highs - k - 1],
            raw_send.at[k - 1],
            raw_recv.at[highs - k - 1],
            ep,
            peer_high(k) * 2 + lo,
        )

    def raw_copy_in(k):
        return remote(
            normed, raw.at[k - 1], raw_send.at[k - 1], raw_recv.at[k - 1], ep, peer_high(k) * 2 + lo
        )

    def near_copy(d, k):
        return remote(
            near_out.at[d, k - 1],
            arrived.at[d, peer_high(k) * 2 + lo],
            y1_send.at[k - 1],
            y1_recv.at[d, k - 1],
            partner_ep(d),
            tp,
        )

    def give_back(d):
        peer = partner_ep(d)
        return remote(core_in.at[d, hi], returned.at[d], ret_send.at[0], ret_recv.at[d], peer, tp)

    def mix_core_copy(high):
        return remote(
            mix_held.at[high * 2 + other],
            mix_core.at[high],
            m1_send.at[0],
            m1_recv.at[0],
            ep,
            hi * 2 + other,
        )

    def mix_core_all():
        return remote(
            mix_held.at[0:highs], mix_core, m1_send.at[0], m1_recv.at[0], ep, hi * 2 + other
        )

    def mix_cross_copy(k):
        high = peer_high(k)
        return remote(
            mix_sum.at[high],
            mix_cross.at[highs - k - 1],
            m2_send.at[k - 1],
            m2_recv.at[highs - k - 1],
            ep,
            high * 2 + lo,
        )

    def mix_cross_in(k):
        high = peer_high(k)
        return remote(
            mix_sum.at[high],
            mix_cross.at[k - 1],
            m2_send.at[k - 1],
            m2_recv.at[k - 1],
            ep,
            high * 2 + lo,
        )

    last_rows = pool.at[rows_a - history_rows :]
    send_history = remote(
        last_rows, history, hist_sem.at[0], hist_sem.at[1], jnp.minimum(ep + 1, ep_size - 1), tp
    )

    half_rows = mix_done.shape[0] // 2
    mixer_stores = [
        pltpu.make_async_copy(
            mix_done.at[half * half_rows : (half + 1) * half_rows],
            mixer_out.at[half * half_rows : (half + 1) * half_rows],
            local_sem.at[7 + half],
        )
        for half in range(2)
    ]
    moe_store = pltpu.make_async_copy(normed, moe_out, local_sem.at[15])
    tokens_copy = pltpu.make_async_copy(tokens_hbm, tokens, local_sem.at[0])
    pool_copy = pltpu.make_async_copy(pool_hbm, pool, local_sem.at[1])
    mixer_copies = [
        pltpu.make_async_copy(group_hbm, group_w, local_sem.at[2]),
        pltpu.make_async_copy(out_w_hbm, out_w, local_sem.at[3]),
    ]
    weight_copies = [
        pltpu.make_async_copy(gate_hbm, gate, local_sem.at[4]),
        pltpu.make_async_copy(up_hbm, up, local_sem.at[5]),
        pltpu.make_async_copy(down_hbm, down, local_sem.at[6]),
    ]

    early_copies = [
        pltpu.make_async_copy(routes_hbm, routes, local_sem.at[9]),
        pltpu.make_async_copy(route_weights_hbm, route_weights, local_sem.at[10]),
        pltpu.make_async_copy(in_gain_hbm, in_gain, local_sem.at[11]),
    ]
    mixer_copies += [
        pltpu.make_async_copy(pool_scale_hbm, pool_scale, local_sem.at[12]),
        pltpu.make_async_copy(mix_gain_hbm, mix_gain, local_sem.at[13]),
        pltpu.make_async_copy(out_gain_hbm, out_gain, local_sem.at[14]),
    ]
    tokens_copy.start()
    early_copies[2].start()
    barrier = pltpu.get_barrier_semaphore()

    def greet(d, carry):
        pl.semaphore_signal(barrier, inc=1, device_id=(partner_ep(d), tp), device_id_type=MESH)
        return carry

    lax.fori_loop(1, ep_size, greet, 0)
    for k in range(1, highs):
        pl.semaphore_signal(
            barrier, inc=1, device_id=(ep, peer_high(k) * 2 + lo), device_id_type=MESH
        )
    pl.semaphore_signal(barrier, inc=1, device_id=(ep, hi * 2 + other), device_id_type=MESH)
    for copy in early_copies[:2]:
        copy.start()
    pool_copy.start()


    expert_id = lax.broadcasted_iota(jnp.int32, (experts, tok_dev), 0)
    first_slot = (
        lax.div(expert_id, exp_dev) * rows + lax.rem(expert_id, exp_dev) * capacity
    ).astype(F32)
    earlier = (
        lax.broadcasted_iota(jnp.int32, (tok_dev, tok_dev), 0)
        < lax.broadcasted_iota(jnp.int32, (tok_dev, tok_dev), 1)
    ).astype(BF16)

    def tokens_of(index):
        return pl.ds(pl.multiple_of(index * tok_dev, tok_dev), tok_dev)

    def find_slots(index, base):
        block_routes = routes[:, tokens_of(index)]
        taken = jnp.zeros((experts, 1), F32)
        found = []
        for k in range(top_count):
            named = (block_routes[k : k + 1, :] == expert_id).astype(F32)
            before = jnp.dot(named.astype(BF16), earlier, preferred_element_type=F32)
            slot = jnp.sum(named * (before + taken + first_slot), axis=0, keepdims=True)
            taken = taken + jnp.sum(named, axis=1, keepdims=True)
            found.append(slot)
            slot_rows[base + k : base + k + 1, :] = slot.astype(jnp.int32)
        return found

    early_copies[2].wait()
    tokens_copy.wait()
    for copy in mixer_copies + weight_copies:
        copy.start()
    normed[...] = rms_scale(tokens[...].astype(F32), in_gain[...]).astype(BF16)
    pool_copy.wait()
    pl.semaphore_wait(barrier, ep_size - 1 + highs)
    if tabled:
        for k in range(1, highs):
            raw_copy(k).start()

    @pl.when(ep < ep_size - 1)
    def _():
        send_history.start()

    def routed_rows(owner, base, source):
        slot_id = lax.broadcasted_iota(jnp.int32, (rows, tok_dev), 0) + owner * rows
        chosen = slot_rows[base : base + 1, :] == slot_id
        for k in range(1, top_count):
            chosen = chosen | (slot_rows[base + k : base + k + 1, :] == slot_id)
        return jnp.dot(
            chosen.astype(F32).astype(BF16), source[...], preferred_element_type=F32
        ).astype(BF16)

    column_step = min(width, 512)

    def mixer_part():
        for copy in mixer_copies:
            copy.wait()

        @pl.when(ep > 0)
        def _():
            send_history.wait_recv()

        @pl.when(ep == 0)
        def _():
            history[...] = jnp.zeros(history.shape, BF16)

        values = pool[...].astype(F32)
        running = jnp.concatenate([history[...].astype(F32), values], axis=0)
        summed = None
        for group in range(tp_size):
            running = running + pltpu.roll(running, 2**group, 0)
            current = running[history_rows:]
            summed = current if summed is None else jnp.where(tp == group, current, summed)
        window = jnp.int32(1)
        for group in range(tp_size):
            window = jnp.where(tp == group, 2 ** (group + 1), window)
        position = ep * rows_a + lax.broadcasted_iota(jnp.int32, values.shape, 0)
        divisor = jnp.minimum(position + 1, window).astype(F32)
        pooled = (summed / divisor - values).astype(BF16)
        grouped = (
            jnp.dot(pooled, group_w[0], preferred_element_type=F32) * pool_scale[...]
        ).astype(BF16)
        mix_rows = rows_a // tp_size
        for start in range(0, width, column_step):
            columns = slice(start, start + column_step)
            mix_held[:, :, columns] = (
                jnp.dot(grouped, out_w[:, columns], preferred_element_type=F32)
                .astype(BF16)
                .reshape(tp_size, mix_rows, column_step)
            )
        for high in range(highs):
            mix_core_copy(high).start()
        mix_core_all().wait_recv()
        for high in range(highs):
            mix_sum[high] = (
                mix_held[high * 2 + lo].astype(F32) + mix_core[high].astype(F32)
            ).astype(BF16)
        for k in range(1, highs):
            mix_cross_copy(k).start()

    def stage_a(d):
        def cross():
            for k in range(1, highs):
                gather_cross(d, k).start()

        if tabled:
            pl.when(d >= NEAR)(cross)
        else:
            cross()
        gather_core(d, hi).start()

    def peer_blocks():
        for k in range(1, highs):
            base = k * top_count
            source = raw.at[k - 1]
            find_slots(peer_high(k) * 2 + lo, base)
            raw_copy_in(k).wait_recv()

            def send_near(d, carry):
                near_out[d, k - 1] = routed_rows(partner_ep(d), base, source)
                near_copy(d, k).start()
                return carry

            lax.fori_loop(1, NEAR, send_near, 0)
            arrived[0, peer_high(k) * 2 + lo] = routed_rows(ep, base, source)

    for copy in early_copies[:2]:
        copy.wait()
    slot_list = find_slots(tp, 0)

    def send_out(i, carry):
        d = sent_at(i)
        peer = partner_ep(d)
        outgoing[peer] = routed_rows(peer, 0, normed)
        dispatch(d).start()
        return carry

    lax.fori_loop(0, ep_size - 1, send_out, 0)
    arrived[0, tp] = routed_rows(ep, 0, normed)
    stage_a(jnp.int32(0))
    own_weights = route_weights[:, tokens_of(tp)]
    stacked = jnp.concatenate(
        slot_list
        + [own_weights[k : k + 1, :] for k in range(top_count)]
        + [jnp.zeros((columns_of.shape[1] - 2 * top_count, tok_dev), F32)],
        axis=0,
    )
    columns_of[...] = stacked.T

    def gather_next(d):
        dispatch(d).wait_recv()
        stage_a(d)

    if not tabled:
        gather_next(offset_of(ep * 0))
    for copy in weight_copies:
        copy.wait()
    total_rows[...] = jnp.zeros(total_rows.shape, F32)

    spans = []
    for e in range(exp_dev):
        begin = e * capacity // ROW_TILE * ROW_TILE
        end = -(-(e + 1) * capacity // ROW_TILE) * ROW_TILE
        spans.append((begin, end))
    edges = sorted({0, rows} | {edge for span in spans for edge in span})

    def experts_on(d):
        hidden = []
        for e, (begin, end) in enumerate(spans):
            count = end - begin
            block = arrived[d, :, begin:end, :].reshape(tp_size * count, width)
            gate_act = jnp.dot(block, gate[e], preferred_element_type=F32)
            up_act = jnp.dot(block, up[e], preferred_element_type=F32)
            act = gate_act / (1.0 + jnp.exp(-gate_act)) * up_act
            place = begin + lax.rem(
                lax.broadcasted_iota(jnp.int32, (tp_size * count, 1), 0), count
            )
            mine = (place >= e * capacity) & (place < (e + 1) * capacity)
            hidden.append(jnp.where(mine, act, 0.0).astype(BF16))
        for start in range(0, width, column_step):
            columns = slice(start, start + column_step)
            outs = []
            for e, (begin, end) in enumerate(spans):
                out = jnp.dot(hidden[e], down[e, :, columns], preferred_element_type=F32)
                outs.append(out.reshape(tp_size, end - begin, column_step))
            for begin, end in zip(edges[:-1], edges[1:]):
                piece = None
                for (first_row, last_row), out in zip(spans, outs):
                    if first_row <= begin and end <= last_row:
                        held = out[:, begin - first_row : end - first_row]
                        piece = held if piece is None else piece + held
                if piece is None:
                    piece = jnp.zeros((tp_size, end - begin, column_step), F32)
                part[:, begin:end, columns] = piece.astype(BF16)

    def combine(owner, block):
        lane = lax.broadcasted_iota(jnp.int32, (tok_dev, 2 * rows), 1)
        slot_id = (lax.rem(lane, rows) + owner * rows).astype(F32)
        weights = jnp.zeros((tok_dev, 2 * rows), F32)
        for k in range(top_count):
            weights = weights + jnp.where(
                columns_of[:, k : k + 1] == slot_id,
                columns_of[:, top_count + k : top_count + k + 1],
                0.0,
            )
        major = weights.astype(BF16).astype(F32)
        split = jnp.where(lane < rows, major, weights - major).astype(BF16)
        for start in range(0, width, column_step):
            columns = slice(start, start + column_step)
            held = block[:, columns]
            twice = jnp.concatenate([held, held], axis=0)
            total_rows[:, columns] += jnp.dot(split, twice, preferred_element_type=F32)

    def combine_from(d):
        give_back(d).wait_recv()
        combine(partner_ep(d), returned.at[d])

    def forward(d):
        for k in range(1, highs):

            def arrival():
                gather_cross_in(d, k).wait_recv()

            if tabled:
                pl.when(d != 0)(arrival)
            else:
                arrival()
            gather_core(d, peer_high(k)).start()

    def compute(d):
        gather_core_in(d).wait_recv()
        experts_on(d)
        for high in range(highs):
            reduce_core(d, high).start()

    def reduce(d):
        reduce_core_all(d).wait_recv()
        reduce_core_all(d).wait_send()
        for high in range(highs):
            core_in[d, high] = (
                part[high * 2 + lo].astype(F32) + core_in[d, high].astype(F32)
            ).astype(BF16)
        for k in range(1, highs):
            reduce_cross(d, k).start()

    def send_home(d):
        total = core_in[d, hi].astype(F32)
        for k in range(1, highs):
            reduce_cross_in(d, k).wait_recv()
            total = total + cross_in[d, k - 1].astype(F32)
        core_in[d, hi] = total.astype(BF16)

        @pl.when(d != 0)
        def _():
            give_back(d).start()

    def mixer_end():
        for k in range(1, highs):
            mix_cross_in(k).wait_recv()
        for half, store in enumerate(mixer_stores):
            span = slice(half * half_rows, (half + 1) * half_rows)
            total = mix_sum[hi, span, :].astype(F32)
            for k in range(1, highs):
                total = total + mix_cross[k - 1, span, :].astype(F32)
            mix_done[span, :] = rms_scale(total, mix_gain[...]).astype(BF16)
            store.start()

    actions = {
        GATHER: gather_next,
        FORWARD: forward,
        COMPUTE: compute,
        REDUCE: reduce,
        RETURN: send_home,
        COMBINE: combine_from,
        MIX: lambda d: mixer_part(),
        PEER: lambda d: peer_blocks(),
    }

    if not tabled:
        del actions[PEER]

    def event(t, carry):
        op, d = event_at(t)
        for kind, action in actions.items():
            pl.when(op == kind)(functools.partial(action, d))
        return carry

    count = len(END_EVENTS) if tabled else 8 * (ep_size + 3)
    lax.fori_loop(0, count, event, 0)

    if not tabled:

        def late(j, carry):
            combine_from(offset_of(j))
            return carry

        lax.fori_loop(max(0, ep_size - 5), ep_size - 1, late, 0)
    combine(ep, core_in.at[0, hi])
    if tabled:
        for k in range(1, highs):
            raw_copy(k).wait_send()
    normed[...] = rms_scale(total_rows[...], out_gain[...]).astype(BF16)
    moe_store.start()

    mix_core_all().wait_send()

    @pl.when(ep < ep_size - 1)
    def _():
        send_history.wait_send()

    def drain(blocks, sem):
        remote(blocks, blocks, sem, dis_recv.at[0], ep, hi * 2 + other).wait_send()

    others = outgoing.at[0 : ep_size - 1]
    for k in range(1, highs):
        drain(others if tabled else outgoing, y1_send.at[k - 1])
        drain(outgoing, y2_send.at[k - 1])
    drain(core_in, c1_send.at[0])
    drain(others, dis_send.at[0])
    drain(others, ret_send.at[0])
    mixer_end()
    for k in range(1, highs):
        mix_cross_copy(k).wait_send()
    moe_store.wait()
    for store in mixer_stores:
        store.wait()


def on_device(
    pool_input,
    group_weight,
    pool_scale,
    out_weight,
    mix_gain,
    expert_input,
    routes,
    route_weights,
    moe_in_gain,
    gate_weight,
    up_weight,
    down_weight,
    moe_out_gain,
):
    tp_size = lax.axis_size("tp")
    ep_size = lax.axis_size("ep")
    rows_a, group_width = pool_input.shape
    width = out_weight.shape[1]
    exp_dev = gate_weight.shape[0]
    experts = exp_dev * ep_size
    tok_dev = expert_input.shape[0]
    top_count = routes.shape[1]
    capacity = max(2, 5 * tok_dev * top_count // (4 * experts))
    rows = -(-exp_dev * capacity // ROW_TILE) * ROW_TILE
    highs = tp_size // 2
    mix_rows = rows_a // tp_size
    history_rows = 2**tp_size
    tabled = ep_size == 8
    raw_rows = tok_dev if tabled else ROW_TILE
    near_rows = rows if tabled else ROW_TILE
    any_spec = pl.BlockSpec(memory_space=pl.ANY)
    hbm_spec = pl.BlockSpec(memory_space=pltpu.HBM)
    dma = pltpu.SemaphoreType.DMA
    flops = 6 * gate_weight.size * ep_size * tp_size * rows
    scratch = [
        pltpu.VMEM((1, group_width), F32),
        pltpu.VMEM((1, width), F32),
        pltpu.VMEM((top_count, tok_dev * tp_size), jnp.int32),
        pltpu.VMEM((top_count, tok_dev * tp_size), F32),
        pltpu.VMEM((1, width), F32),
        pltpu.VMEM((1, width), F32),
        pltpu.VMEM(pool_input.shape, BF16),
        pltpu.VMEM((history_rows, group_width), BF16),
        pltpu.VMEM(group_weight.shape, BF16),
        pltpu.VMEM(out_weight.shape, BF16),
        pltpu.VMEM(expert_input.shape, BF16),
        pltpu.VMEM(expert_input.shape, BF16),
        pltpu.VMEM((highs - 1, raw_rows, width), BF16),
        pltpu.VMEM((NEAR, highs - 1, near_rows, width), BF16),
        pltpu.VMEM((8, tok_dev), jnp.int32),
        pltpu.VMEM((tok_dev, 8), F32),
        pltpu.VMEM((ep_size, rows, width), BF16),
        pltpu.VMEM((ep_size, tp_size, rows, width), BF16),
        pltpu.VMEM((tp_size, rows, width), BF16),
        pltpu.VMEM((ep_size, highs, rows, width), BF16),
        pltpu.VMEM((ep_size, highs - 1, rows, width), BF16),
        pltpu.VMEM((ep_size, rows, width), BF16),
        pltpu.VMEM(expert_input.shape, F32),
        pltpu.VMEM(gate_weight.shape, BF16),
        pltpu.VMEM(up_weight.shape, BF16),
        pltpu.VMEM(down_weight.shape, BF16),
        pltpu.VMEM((tp_size, mix_rows, width), BF16),
        pltpu.VMEM((highs, mix_rows, width), BF16),
        pltpu.VMEM((highs, mix_rows, width), BF16),
        pltpu.VMEM((highs - 1, mix_rows, width), BF16),
        pltpu.VMEM((mix_rows, width), BF16),
        dma((16,)),
        dma((2,)),
        dma((highs - 1,)),
        dma((highs - 1,)),
        dma((1,)),
        dma((ep_size,)),
        dma((highs - 1,)),
        dma((ep_size, highs - 1)),
        dma((1,)),
        dma((ep_size,)),
        dma((1,)),
        dma((ep_size,)),
        dma((highs - 1,)),
        dma((ep_size, highs - 1)),
        dma((1,)),
        dma((ep_size,)),
        dma((1,)),
        dma((1,)),
        dma((highs - 1,)),
        dma((highs - 1,)),
    ]
    held = sum(
        ref.dtype.itemsize * math.prod(ref.shape)
        for ref in scratch
        if ref.memory_space == pltpu.VMEM
    )
    mixer_out, moe_out = pl.pallas_call(
        functools.partial(fused_kernel, capacity),
        out_shape=(
            pltpu.VMEM((mix_rows, width), BF16),
            pltpu.VMEM((tok_dev, width), BF16),
        ),
        in_specs=[hbm_spec] * 13,
        out_specs=(any_spec, any_spec),
        scratch_shapes=scratch,
        compiler_params=pltpu.CompilerParams(
            collective_id=0, has_side_effects=True, vmem_limit_bytes=max(ROOM, held + SPARE)
        ),
        cost_estimate=pl.CostEstimate(
            flops=flops, bytes_accessed=8 * expert_input.size, transcendentals=0
        ),
    )(
        pool_input,
        group_weight,
        pool_scale.reshape(1, -1),
        out_weight,
        mix_gain.reshape(1, -1),
        expert_input,
        routes.T,
        route_weights.T,
        moe_in_gain.reshape(1, -1),
        gate_weight,
        up_weight,
        down_weight,
        moe_out_gain.reshape(1, -1),
    )
    return (mixer_out, moe_out)


def solution(mesh):
    in_specs = (
        P("ep", "tp"),
        P("tp", None, None),
        P("tp"),
        P("tp", None),
        P(),
        P(("ep", "tp"), None),
        P("ep", None),
        P("ep", None),
        P(),
        P("ep", None, "tp"),
        P("ep", None, "tp"),
        P("ep", "tp", None),
        P(),
    )
    out_specs = (P(("ep", "tp"), None), P(("ep", "tp"), None))
    return jax.shard_map(
        on_device, mesh=mesh, in_specs=in_specs, out_specs=out_specs, check_vma=False
    )
```

```python
import functools
import math

import jax
import jax.numpy as jnp
from jax import lax
from jax.experimental import pallas as pl
from jax.experimental.pallas import tpu as pltpu
from jax.sharding import PartitionSpec as P

NORM_EPS = 1e-06
ROOM = 56 * 1024 * 1024
SPARE = 3 * 1024 * 1024
MESH = pl.DeviceIdType.MESH
F32 = jnp.float32
BF16 = jnp.bfloat16
ROW_TILE = 16
GATHER, FORWARD, COMPUTE, REDUCE, RETURN, COMBINE, MIX, PEER, NONE = range(9)
KINDS = {
    "A": GATHER,
    "X": FORWARD,
    "C": COMPUTE,
    "R": REDUCE,
    "F": RETURN,
    "B": COMBINE,
    "M": MIX,
    "P": PEER,
}
STEADY = (
    (GATHER, -1, 1),
    (FORWARD, 0, 0),
    (RETURN, 3, 0),
    (REDUCE, 1, 0),
    (COMPUTE, 0, 0),
    (COMBINE, 8, 1),
)
CODE_BITS = 6
NEAR = 4
PER_WORD = 5


def coded(*events):
    return tuple(KINDS[event[0]] * 8 + int(event[1:] or 0) for event in events)


END_EVENTS = coded(
    "A6", "A1", "P", "A7", "A3", "X6", "C6", "R6", "X7", "C7", "R7", "F6", "A4", "F7", "A5",
    "X4", "C4", "R4", "X5", "C5", "R5", "F4", "A2", "X1", "C1", "R1", "F5", "X3", "C3", "R3",
    "F1", "X2", "C2", "R2", "F3", "X0", "C0", "R0", "M", "F2", "B6", "B7", "B4", "B5", "B1",
    "B3", "F0", "B2",
)
MIDDLE_EVENTS = coded(
    "A1", "A4", "P", "A5", "X4", "C4", "R4", "X5", "C5", "R5", "F4", "X0", "C0", "R0", "F5",
    "A6", "X1", "C1", "R1", "F0", "X6", "C6", "R6", "A7", "A3", "F1", "X3", "C3", "R3", "F6",
    "A2", "X7", "C7", "R7", "F3", "X2", "C2", "R2", "F7", "M", "B4", "B5", "F2", "B1", "B3",
    "B6", "B7", "B2",
)
END_SENDS = (1, 6, 7, 4, 5, 3, 2)
MIDDLE_SENDS = (1, 4, 5, 6, 7, 3, 2)

def rms_scale(values, gain_vec):
    mean_sq = jnp.mean(values * values, axis=-1, keepdims=True)
    return values * lax.rsqrt(mean_sq + NORM_EPS) * gain_vec


def fused_kernel(
    capacity,
    pool_hbm,
    group_hbm,
    pool_scale_hbm,
    out_w_hbm,
    mix_gain_hbm,
    tokens_hbm,
    routes_hbm,
    route_weights_hbm,
    in_gain_hbm,
    gate_hbm,
    up_hbm,
    down_hbm,
    out_gain_hbm,
    mixer_out,
    moe_out,
    pool_scale,
    mix_gain,
    routes,
    route_weights,
    in_gain,
    out_gain,
    pool,
    history,
    group_w,
    out_w,
    tokens,
    normed,
    raw,
    near_out,
    slot_rows,
    columns_of,
    outgoing,
    arrived,
    part,
    core_in,
    cross_in,
    returned,
    total_rows,
    gate,
    up,
    down,
    mix_held,
    mix_core,
    mix_sum,
    mix_cross,
    mix_done,
    local_sem,
    hist_sem,
    raw_send,
    raw_recv,
    dis_send,
    dis_recv,
    y1_send,
    y1_recv,
    c1_send,
    c1_recv,
    c2_send,
    c2_recv,
    y2_send,
    y2_recv,
    ret_send,
    ret_recv,
    m1_send,
    m1_recv,
    m2_send,
    m2_recv,
):
    ep_size, tp_size, rows, width = arrived.shape
    exp_dev, _, ff_dev = gate.shape
    tok_dev = tokens.shape[0]
    top_count = routes.shape[0]
    experts = exp_dev * ep_size
    rows_a = pool.shape[0]
    history_rows = history.shape[0]
    highs = tp_size // 2
    ep = lax.axis_index("ep")
    tp = lax.axis_index("tp")
    hi, lo = tp // 2, tp % 2
    other = 1 - lo

    def remote(src, dst, send, recv, to_ep, to_tp):
        return pltpu.make_async_remote_copy(
            src_ref=src,
            dst_ref=dst,
            send_sem=send,
            recv_sem=recv,
            device_id=(to_ep, to_tp),
            device_id_type=MESH,
        )

    def peer_high(k):
        return lax.rem(hi + k, highs)

    on_end = (ep // 2) % 2 == (ep // 4) % 2
    tabled = ep_size == 8

    def packed_at(table, i):
        words = []
        for begin in range(0, len(table), PER_WORD):
            piece = table[begin : begin + PER_WORD]
            words.append(sum(value << (CODE_BITS * at) for at, value in enumerate(piece)))
        word = jnp.int32(words[0])
        for at in range(1, len(words)):
            word = jnp.where(i >= at * PER_WORD, words[at], word)
        shift = CODE_BITS * lax.rem(i, PER_WORD)
        return lax.rem(lax.shift_right_logical(word, shift), 1 << CODE_BITS)

    def offset_of(i):
        far = jnp.where(i == 0, 1, ep_size - i)
        return jnp.where(i == ep_size - 1, 0, far)

    def sent_at(i):
        if tabled:
            return jnp.where(on_end, packed_at(END_SENDS, i), packed_at(MIDDLE_SENDS, i))
        return offset_of(i)

    def event_at(t):
        if tabled:
            code = jnp.where(on_end, packed_at(END_EVENTS, t), packed_at(MIDDLE_EVENTS, t))
            return code // 8, code % 8
        i, slot = t // 8, t % 8
        op, j = jnp.int32(NONE), i
        for at, (kind, lag, last) in enumerate(STEADY):
            index = i - lag
            valid = (slot == at) & (index >= 0) & (index < ep_size - last)
            op = jnp.where(valid, kind, op)
            j = jnp.where(valid, index, j)
        op = jnp.where((slot == 6) & (i == 0), MIX, op)
        return op, offset_of(j)

    def partner_ep(d):
        value = ep * 0
        bit = 1
        while bit < ep_size:
            value = value + bit * (((ep // bit) % 2 + (d // bit) % 2) % 2)
            bit *= 2
        return value

    def dispatch(d):
        peer = partner_ep(d)
        return remote(
            outgoing.at[peer], arrived.at[d, tp], dis_send.at[0], dis_recv.at[d], peer, tp
        )

    def gather_cross(d, k):
        slot = arrived.at[d, tp]
        return remote(
            slot, slot, y1_send.at[k - 1], y1_recv.at[d, highs - k - 1], ep, peer_high(k) * 2 + lo
        )

    def gather_cross_in(d, k):
        high = peer_high(k)
        slot = arrived.at[d, high * 2 + lo]
        return remote(slot, slot, y1_send.at[k - 1], y1_recv.at[d, k - 1], ep, high * 2 + lo)

    def gather_core(d, high):
        slot = arrived.at[d, high * 2 + lo]
        return remote(slot, slot, c1_send.at[0], c1_recv.at[d], ep, hi * 2 + other)

    def gather_core_in(d):
        slots = arrived.at[d, 0:highs]
        return remote(slots, slots, c1_send.at[0], c1_recv.at[d], ep, hi * 2 + other)

    def reduce_core(d, high):
        return remote(
            part.at[high * 2 + other],
            core_in.at[d, high],
            c2_send.at[0],
            c2_recv.at[d],
            ep,
            hi * 2 + other,
        )

    def reduce_core_all(d):
        return remote(
            part.at[0:highs],
            core_in.at[d],
            c2_send.at[0],
            c2_recv.at[d],
            ep,
            hi * 2 + other,
        )

    def reduce_cross(d, k):
        high = peer_high(k)
        return remote(
            core_in.at[d, high],
            cross_in.at[d, highs - k - 1],
            y2_send.at[k - 1],
            y2_recv.at[d, highs - k - 1],
            ep,
            high * 2 + lo,
        )

    def reduce_cross_in(d, k):
        high = peer_high(k)
        return remote(
            core_in.at[d, high],
            cross_in.at[d, k - 1],
            y2_send.at[k - 1],
            y2_recv.at[d, k - 1],
            ep,
            high * 2 + lo,
        )

    def raw_copy(k):
        return remote(
            normed,
            raw.at[highs - k - 1],
            raw_send.at[k - 1],
            raw_recv.at[highs - k - 1],
            ep,
            peer_high(k) * 2 + lo,
        )

    def raw_copy_in(k):
        return remote(
            normed, raw.at[k - 1], raw_send.at[k - 1], raw_recv.at[k - 1], ep, peer_high(k) * 2 + lo
        )

    def near_copy(d, k):
        return remote(
            near_out.at[d, k - 1],
            arrived.at[d, peer_high(k) * 2 + lo],
            y1_send.at[k - 1],
            y1_recv.at[d, k - 1],
            partner_ep(d),
            tp,
        )

    def give_back(d):
        peer = partner_ep(d)
        return remote(core_in.at[d, hi], returned.at[d], ret_send.at[0], ret_recv.at[d], peer, tp)

    def mix_core_copy(high):
        return remote(
            mix_held.at[high * 2 + other],
            mix_core.at[high],
            m1_send.at[0],
            m1_recv.at[0],
            ep,
            hi * 2 + other,
        )

    def mix_core_all():
        return remote(
            mix_held.at[0:highs], mix_core, m1_send.at[0], m1_recv.at[0], ep, hi * 2 + other
        )

    def mix_cross_copy(k):
        high = peer_high(k)
        return remote(
            mix_sum.at[high],
            mix_cross.at[highs - k - 1],
            m2_send.at[k - 1],
            m2_recv.at[highs - k - 1],
            ep,
            high * 2 + lo,
        )

    def mix_cross_in(k):
        high = peer_high(k)
        return remote(
            mix_sum.at[high],
            mix_cross.at[k - 1],
            m2_send.at[k - 1],
            m2_recv.at[k - 1],
            ep,
            high * 2 + lo,
        )

    last_rows = pool.at[rows_a - history_rows :]
    send_history = remote(
        last_rows, history, hist_sem.at[0], hist_sem.at[1], jnp.minimum(ep + 1, ep_size - 1), tp
    )

    half_rows = mix_done.shape[0] // 2
    mixer_stores = [
        pltpu.make_async_copy(
            mix_done.at[half * half_rows : (half + 1) * half_rows],
            mixer_out.at[half * half_rows : (half + 1) * half_rows],
            local_sem.at[7 + half],
        )
        for half in range(2)
    ]
    moe_store = pltpu.make_async_copy(normed, moe_out, local_sem.at[15])
    tokens_copy = pltpu.make_async_copy(tokens_hbm, tokens, local_sem.at[0])
    pool_copy = pltpu.make_async_copy(pool_hbm, pool, local_sem.at[1])
    mixer_copies = [
        pltpu.make_async_copy(group_hbm, group_w, local_sem.at[2]),
        pltpu.make_async_copy(out_w_hbm, out_w, local_sem.at[3]),
    ]
    weight_copies = [
        pltpu.make_async_copy(gate_hbm, gate, local_sem.at[4]),
        pltpu.make_async_copy(up_hbm, up, local_sem.at[5]),
        pltpu.make_async_copy(down_hbm, down, local_sem.at[6]),
    ]

    early_copies = [
        pltpu.make_async_copy(routes_hbm, routes, local_sem.at[9]),
        pltpu.make_async_copy(route_weights_hbm, route_weights, local_sem.at[10]),
        pltpu.make_async_copy(in_gain_hbm, in_gain, local_sem.at[11]),
    ]
    mixer_copies += [
        pltpu.make_async_copy(pool_scale_hbm, pool_scale, local_sem.at[12]),
        pltpu.make_async_copy(mix_gain_hbm, mix_gain, local_sem.at[13]),
        pltpu.make_async_copy(out_gain_hbm, out_gain, local_sem.at[14]),
    ]
    tokens_copy.start()
    early_copies[2].start()
    barrier = pltpu.get_barrier_semaphore()

    def greet(d, carry):
        pl.semaphore_signal(barrier, inc=1, device_id=(partner_ep(d), tp), device_id_type=MESH)
        return carry

    lax.fori_loop(1, ep_size, greet, 0)
    for k in range(1, highs):
        pl.semaphore_signal(
            barrier, inc=1, device_id=(ep, peer_high(k) * 2 + lo), device_id_type=MESH
        )
    pl.semaphore_signal(barrier, inc=1, device_id=(ep, hi * 2 + other), device_id_type=MESH)
    for copy in early_copies[:2]:
        copy.start()
    pool_copy.start()


    expert_id = lax.broadcasted_iota(jnp.int32, (experts, tok_dev), 0)
    first_slot = (
        lax.div(expert_id, exp_dev) * rows + lax.rem(expert_id, exp_dev) * capacity
    ).astype(F32)
    earlier = (
        lax.broadcasted_iota(jnp.int32, (tok_dev, tok_dev), 0)
        < lax.broadcasted_iota(jnp.int32, (tok_dev, tok_dev), 1)
    ).astype(BF16)

    def tokens_of(index):
        return pl.ds(pl.multiple_of(index * tok_dev, tok_dev), tok_dev)

    def find_slots(index, base):
        block_routes = routes[:, tokens_of(index)]
        taken = jnp.zeros((experts, 1), F32)
        found = []
        for k in range(top_count):
            named = (block_routes[k : k + 1, :] == expert_id).astype(F32)
            before = jnp.dot(named.astype(BF16), earlier, preferred_element_type=F32)
            slot = jnp.sum(named * (before + taken + first_slot), axis=0, keepdims=True)
            taken = taken + jnp.sum(named, axis=1, keepdims=True)
            found.append(slot)
            slot_rows[base + k : base + k + 1, :] = slot.astype(jnp.int32)
        return found

    early_copies[2].wait()
    tokens_copy.wait()
    for copy in mixer_copies + weight_copies:
        copy.start()
    normed[...] = rms_scale(tokens[...].astype(F32), in_gain[...]).astype(BF16)
    pool_copy.wait()
    pl.semaphore_wait(barrier, ep_size - 1 + highs)
    if tabled:
        for k in range(1, highs):
            raw_copy(k).start()

    @pl.when(ep < ep_size - 1)
    def _():
        send_history.start()

    def routed_rows(owner, base, source):
        slot_id = lax.broadcasted_iota(jnp.int32, (rows, tok_dev), 0) + owner * rows
        chosen = slot_rows[base : base + 1, :] == slot_id
        for k in range(1, top_count):
            chosen = chosen | (slot_rows[base + k : base + k + 1, :] == slot_id)
        return jnp.dot(
            chosen.astype(F32).astype(BF16), source[...], preferred_element_type=F32
        ).astype(BF16)

    column_step = min(width, 512)

    def mixer_part():
        for copy in mixer_copies:
            copy.wait()

        @pl.when(ep > 0)
        def _():
            send_history.wait_recv()

        @pl.when(ep == 0)
        def _():
            history[...] = jnp.zeros(history.shape, BF16)

        values = pool[...].astype(F32)
        running = jnp.concatenate([history[...].astype(F32), values], axis=0)
        summed = None
        for group in range(tp_size):
            running = running + pltpu.roll(running, 2**group, 0)
            current = running[history_rows:]
            summed = current if summed is None else jnp.where(tp == group, current, summed)
        window = jnp.int32(1)
        for group in range(tp_size):
            window = jnp.where(tp == group, 2 ** (group + 1), window)
        position = ep * rows_a + lax.broadcasted_iota(jnp.int32, values.shape, 0)
        divisor = jnp.minimum(position + 1, window).astype(F32)
        pooled = (summed / divisor - values).astype(BF16)
        grouped = (
            jnp.dot(pooled, group_w[0], preferred_element_type=F32) * pool_scale[...]
        ).astype(BF16)
        mix_rows = rows_a // tp_size
        for start in range(0, width, column_step):
            columns = slice(start, start + column_step)
            mix_held[:, :, columns] = (
                jnp.dot(grouped, out_w[:, columns], preferred_element_type=F32)
                .astype(BF16)
                .reshape(tp_size, mix_rows, column_step)
            )
        for high in range(highs):
            mix_core_copy(high).start()
        mix_core_all().wait_recv()
        for high in range(highs):
            mix_sum[high] = (
                mix_held[high * 2 + lo].astype(F32) + mix_core[high].astype(F32)
            ).astype(BF16)
        for k in range(1, highs):
            mix_cross_copy(k).start()

    def stage_a(d):
        def cross():
            for k in range(1, highs):
                gather_cross(d, k).start()

        if tabled:
            pl.when(d >= NEAR)(cross)
        else:
            cross()
        gather_core(d, hi).start()

    def peer_blocks():
        for k in range(1, highs):
            base = k * top_count
            source = raw.at[k - 1]
            find_slots(peer_high(k) * 2 + lo, base)
            raw_copy_in(k).wait_recv()

            def send_near(d, carry):
                near_out[d, k - 1] = routed_rows(partner_ep(d), base, source)
                near_copy(d, k).start()
                return carry

            lax.fori_loop(1, NEAR, send_near, 0)
            arrived[0, peer_high(k) * 2 + lo] = routed_rows(ep, base, source)

    for copy in early_copies[:2]:
        copy.wait()
    slot_list = find_slots(tp, 0)

    def send_out(i, carry):
        d = sent_at(i)
        peer = partner_ep(d)
        outgoing[peer] = routed_rows(peer, 0, normed)
        dispatch(d).start()
        return carry

    lax.fori_loop(0, ep_size - 1, send_out, 0)
    arrived[0, tp] = routed_rows(ep, 0, normed)
    stage_a(jnp.int32(0))
    own_weights = route_weights[:, tokens_of(tp)]
    stacked = jnp.concatenate(
        slot_list
        + [own_weights[k : k + 1, :] for k in range(top_count)]
        + [jnp.zeros((columns_of.shape[1] - 2 * top_count, tok_dev), F32)],
        axis=0,
    )
    columns_of[...] = stacked.T

    def gather_next(d):
        dispatch(d).wait_recv()
        stage_a(d)

    if not tabled:
        gather_next(offset_of(ep * 0))
    for copy in weight_copies:
        copy.wait()
    total_rows[...] = jnp.zeros(total_rows.shape, F32)

    spans = []
    for e in range(exp_dev):
        begin = e * capacity // ROW_TILE * ROW_TILE
        end = -(-(e + 1) * capacity // ROW_TILE) * ROW_TILE
        spans.append((begin, end))
    edges = sorted({0, rows} | {edge for span in spans for edge in span})

    def experts_on(d):
        hidden = []
        for e, (begin, end) in enumerate(spans):
            count = end - begin
            block = arrived[d, :, begin:end, :].reshape(tp_size * count, width)
            gate_act = jnp.dot(block, gate[e], preferred_element_type=F32)
            up_act = jnp.dot(block, up[e], preferred_element_type=F32)
            act = gate_act / (1.0 + jnp.exp(-gate_act)) * up_act
            place = begin + lax.rem(
                lax.broadcasted_iota(jnp.int32, (tp_size * count, 1), 0), count
            )
            mine = (place >= e * capacity) & (place < (e + 1) * capacity)
            hidden.append(jnp.where(mine, act, 0.0).astype(BF16))
        for start in range(0, width, column_step):
            columns = slice(start, start + column_step)
            outs = []
            for e, (begin, end) in enumerate(spans):
                out = jnp.dot(hidden[e], down[e, :, columns], preferred_element_type=F32)
                outs.append(out.reshape(tp_size, end - begin, column_step))
            for begin, end in zip(edges[:-1], edges[1:]):
                piece = None
                for (first_row, last_row), out in zip(spans, outs):
                    if first_row <= begin and end <= last_row:
                        held = out[:, begin - first_row : end - first_row]
                        piece = held if piece is None else piece + held
                if piece is None:
                    piece = jnp.zeros((tp_size, end - begin, column_step), F32)
                part[:, begin:end, columns] = piece.astype(BF16)

    def combine(owner, block):
        lane = lax.broadcasted_iota(jnp.int32, (tok_dev, 2 * rows), 1)
        slot_id = (lax.rem(lane, rows) + owner * rows).astype(F32)
        weights = jnp.zeros((tok_dev, 2 * rows), F32)
        for k in range(top_count):
            weights = weights + jnp.where(
                columns_of[:, k : k + 1] == slot_id,
                columns_of[:, top_count + k : top_count + k + 1],
                0.0,
            )
        major = weights.astype(BF16).astype(F32)
        split = jnp.where(lane < rows, major, weights - major).astype(BF16)
        for start in range(0, width, column_step):
            columns = slice(start, start + column_step)
            held = block[:, columns]
            twice = jnp.concatenate([held, held], axis=0)
            total_rows[:, columns] += jnp.dot(split, twice, preferred_element_type=F32)

    def combine_from(d):
        give_back(d).wait_recv()
        combine(partner_ep(d), returned.at[d])

    def forward(d):
        for k in range(1, highs):

            def arrival():
                gather_cross_in(d, k).wait_recv()

            if tabled:
                pl.when(d != 0)(arrival)
            else:
                arrival()
            gather_core(d, peer_high(k)).start()

    def compute(d):
        gather_core_in(d).wait_recv()
        experts_on(d)
        for high in range(highs):
            reduce_core(d, high).start()

    def reduce(d):
        reduce_core_all(d).wait_recv()
        reduce_core_all(d).wait_send()

        def chip_total(high):
            core_in[d, high] = (
                part[high * 2 + lo].astype(F32) + core_in[d, high].astype(F32)
            ).astype(BF16)

        for k in range(1, highs):
            chip_total(peer_high(k))
            reduce_cross(d, k).start()
        chip_total(hi)

    def send_home(d):
        total = core_in[d, hi].astype(F32)
        for k in range(1, highs):
            reduce_cross_in(d, k).wait_recv()
            total = total + cross_in[d, k - 1].astype(F32)
        core_in[d, hi] = total.astype(BF16)

        @pl.when(d != 0)
        def _():
            give_back(d).start()

    def mixer_end():
        for k in range(1, highs):
            mix_cross_in(k).wait_recv()
        for half, store in enumerate(mixer_stores):
            span = slice(half * half_rows, (half + 1) * half_rows)
            total = mix_sum[hi, span, :].astype(F32)
            for k in range(1, highs):
                total = total + mix_cross[k - 1, span, :].astype(F32)
            mix_done[span, :] = rms_scale(total, mix_gain[...]).astype(BF16)
            store.start()

    actions = {
        GATHER: gather_next,
        FORWARD: forward,
        COMPUTE: compute,
        REDUCE: reduce,
        RETURN: send_home,
        COMBINE: combine_from,
        MIX: lambda d: mixer_part(),
        PEER: lambda d: peer_blocks(),
    }

    if not tabled:
        del actions[PEER]

    def event(t, carry):
        op, d = event_at(t)
        for kind, action in actions.items():
            pl.when(op == kind)(functools.partial(action, d))
        return carry

    count = len(END_EVENTS) if tabled else 8 * (ep_size + 3)
    lax.fori_loop(0, count, event, 0)

    if not tabled:

        def late(j, carry):
            combine_from(offset_of(j))
            return carry

        lax.fori_loop(max(0, ep_size - 5), ep_size - 1, late, 0)
    combine(ep, core_in.at[0, hi])
    if tabled:
        for k in range(1, highs):
            raw_copy(k).wait_send()
    normed[...] = rms_scale(total_rows[...], out_gain[...]).astype(BF16)
    moe_store.start()

    mix_core_all().wait_send()

    @pl.when(ep < ep_size - 1)
    def _():
        send_history.wait_send()

    def drain(blocks, sem):
        remote(blocks, blocks, sem, dis_recv.at[0], ep, hi * 2 + other).wait_send()

    others = outgoing.at[0 : ep_size - 1]
    for k in range(1, highs):
        drain(others if tabled else outgoing, y1_send.at[k - 1])
        drain(outgoing, y2_send.at[k - 1])
    drain(core_in, c1_send.at[0])
    drain(others, dis_send.at[0])
    drain(others, ret_send.at[0])
    mixer_end()
    for k in range(1, highs):
        mix_cross_copy(k).wait_send()
    moe_store.wait()
    for store in mixer_stores:
        store.wait()


def on_device(
    pool_input,
    group_weight,
    pool_scale,
    out_weight,
    mix_gain,
    expert_input,
    routes,
    route_weights,
    moe_in_gain,
    gate_weight,
    up_weight,
    down_weight,
    moe_out_gain,
):
    tp_size = lax.axis_size("tp")
    ep_size = lax.axis_size("ep")
    rows_a, group_width = pool_input.shape
    width = out_weight.shape[1]
    exp_dev = gate_weight.shape[0]
    experts = exp_dev * ep_size
    tok_dev = expert_input.shape[0]
    top_count = routes.shape[1]
    capacity = max(2, 5 * tok_dev * top_count // (4 * experts))
    rows = -(-exp_dev * capacity // ROW_TILE) * ROW_TILE
    highs = tp_size // 2
    mix_rows = rows_a // tp_size
    history_rows = 2**tp_size
    tabled = ep_size == 8
    raw_rows = tok_dev if tabled else ROW_TILE
    near_rows = rows if tabled else ROW_TILE
    any_spec = pl.BlockSpec(memory_space=pl.ANY)
    hbm_spec = pl.BlockSpec(memory_space=pltpu.HBM)
    dma = pltpu.SemaphoreType.DMA
    flops = 6 * gate_weight.size * ep_size * tp_size * rows
    scratch = [
        pltpu.VMEM((1, group_width), F32),
        pltpu.VMEM((1, width), F32),
        pltpu.VMEM((top_count, tok_dev * tp_size), jnp.int32),
        pltpu.VMEM((top_count, tok_dev * tp_size), F32),
        pltpu.VMEM((1, width), F32),
        pltpu.VMEM((1, width), F32),
        pltpu.VMEM(pool_input.shape, BF16),
        pltpu.VMEM((history_rows, group_width), BF16),
        pltpu.VMEM(group_weight.shape, BF16),
        pltpu.VMEM(out_weight.shape, BF16),
        pltpu.VMEM(expert_input.shape, BF16),
        pltpu.VMEM(expert_input.shape, BF16),
        pltpu.VMEM((highs - 1, raw_rows, width), BF16),
        pltpu.VMEM((NEAR, highs - 1, near_rows, width), BF16),
        pltpu.VMEM((8, tok_dev), jnp.int32),
        pltpu.VMEM((tok_dev, 8), F32),
        pltpu.VMEM((ep_size, rows, width), BF16),
        pltpu.VMEM((ep_size, tp_size, rows, width), BF16),
        pltpu.VMEM((tp_size, rows, width), BF16),
        pltpu.VMEM((ep_size, highs, rows, width), BF16),
        pltpu.VMEM((ep_size, highs - 1, rows, width), BF16),
        pltpu.VMEM((ep_size, rows, width), BF16),
        pltpu.VMEM(expert_input.shape, F32),
        pltpu.VMEM(gate_weight.shape, BF16),
        pltpu.VMEM(up_weight.shape, BF16),
        pltpu.VMEM(down_weight.shape, BF16),
        pltpu.VMEM((tp_size, mix_rows, width), BF16),
        pltpu.VMEM((highs, mix_rows, width), BF16),
        pltpu.VMEM((highs, mix_rows, width), BF16),
        pltpu.VMEM((highs - 1, mix_rows, width), BF16),
        pltpu.VMEM((mix_rows, width), BF16),
        dma((16,)),
        dma((2,)),
        dma((highs - 1,)),
        dma((highs - 1,)),
        dma((1,)),
        dma((ep_size,)),
        dma((highs - 1,)),
        dma((ep_size, highs - 1)),
        dma((1,)),
        dma((ep_size,)),
        dma((1,)),
        dma((ep_size,)),
        dma((highs - 1,)),
        dma((ep_size, highs - 1)),
        dma((1,)),
        dma((ep_size,)),
        dma((1,)),
        dma((1,)),
        dma((highs - 1,)),
        dma((highs - 1,)),
    ]
    held = sum(
        ref.dtype.itemsize * math.prod(ref.shape)
        for ref in scratch
        if ref.memory_space == pltpu.VMEM
    )
    mixer_out, moe_out = pl.pallas_call(
        functools.partial(fused_kernel, capacity),
        out_shape=(
            pltpu.VMEM((mix_rows, width), BF16),
            pltpu.VMEM((tok_dev, width), BF16),
        ),
        in_specs=[hbm_spec] * 13,
        out_specs=(any_spec, any_spec),
        scratch_shapes=scratch,
        compiler_params=pltpu.CompilerParams(
            collective_id=0, has_side_effects=True, vmem_limit_bytes=max(ROOM, held + SPARE)
        ),
        cost_estimate=pl.CostEstimate(
            flops=flops, bytes_accessed=8 * expert_input.size, transcendentals=0
        ),
    )(
        pool_input,
        group_weight,
        pool_scale.reshape(1, -1),
        out_weight,
        mix_gain.reshape(1, -1),
        expert_input,
        routes.T,
        route_weights.T,
        moe_in_gain.reshape(1, -1),
        gate_weight,
        up_weight,
        down_weight,
        moe_out_gain.reshape(1, -1),
    )
    return (mixer_out, moe_out)


def solution(mesh):
    in_specs = (
        P("ep", "tp"),
        P("tp", None, None),
        P("tp"),
        P("tp", None),
        P(),
        P(("ep", "tp"), None),
        P("ep", None),
        P("ep", None),
        P(),
        P("ep", None, "tp"),
        P("ep", None, "tp"),
        P("ep", "tp", None),
        P(),
    )
    out_specs = (P(("ep", "tp"), None), P(("ep", "tp"), None))
    return jax.shard_map(
        on_device, mesh=mesh, in_specs=in_specs, out_specs=out_specs, check_vma=False
    )
```

```python
import functools
import math

import jax
import jax.numpy as jnp
from jax import lax
from jax.experimental import pallas as pl
from jax.experimental.pallas import tpu as pltpu
from jax.sharding import PartitionSpec as P

NORM_EPS = 1e-06
ROOM = 56 * 1024 * 1024
SPARE = 3 * 1024 * 1024
MESH = pl.DeviceIdType.MESH
F32 = jnp.float32
BF16 = jnp.bfloat16
ROW_TILE = 16
GATHER, FORWARD, COMPUTE, REDUCE, RETURN, COMBINE, MIX, PEER, NONE = range(9)
KINDS = {
    "A": GATHER,
    "X": FORWARD,
    "C": COMPUTE,
    "R": REDUCE,
    "F": RETURN,
    "B": COMBINE,
    "M": MIX,
    "P": PEER,
}
STEADY = (
    (GATHER, -1, 1),
    (FORWARD, 0, 0),
    (RETURN, 3, 0),
    (REDUCE, 1, 0),
    (COMPUTE, 0, 0),
    (COMBINE, 8, 1),
)
CODE_BITS = 6
NEAR = 4
PER_WORD = 5


def coded(*events):
    return tuple(KINDS[event[0]] * 8 + int(event[1:] or 0) for event in events)


END_EVENTS = coded(
    "A6", "A1", "P", "A7", "A3", "X6", "C6", "R6", "X7", "C7", "R7", "F6", "A4", "F7", "A5",
    "X4", "C4", "R4", "X5", "C5", "R5", "F4", "A2", "X1", "C1", "R1", "F5", "X3", "C3", "R3",
    "F1", "X2", "C2", "R2", "F3", "X0", "C0", "R0", "M", "F2", "B6", "B7", "B4", "B5", "B1",
    "B3", "F0", "B2",
)
MIDDLE_EVENTS = coded(
    "A1", "A4", "P", "A5", "X4", "C4", "R4", "X5", "C5", "R5", "F4", "X0", "C0", "R0", "F5",
    "A6", "X1", "C1", "R1", "F0", "X6", "C6", "R6", "A7", "A3", "F1", "X3", "C3", "R3", "F6",
    "A2", "X7", "C7", "R7", "F3", "X2", "C2", "R2", "F7", "M", "B4", "B5", "F2", "B1", "B3",
    "B6", "B7", "B2",
)
END_SENDS = (1, 6, 7, 4, 5, 3, 2)
MIDDLE_SENDS = (1, 4, 5, 6, 7, 3, 2)

def rms_scale(values, gain_vec):
    mean_sq = jnp.mean(values * values, axis=-1, keepdims=True)
    return values * lax.rsqrt(mean_sq + NORM_EPS) * gain_vec


def fused_kernel(
    capacity,
    pool_hbm,
    group_hbm,
    pool_scale_hbm,
    out_w_hbm,
    mix_gain_hbm,
    tokens_hbm,
    routes_hbm,
    route_weights_hbm,
    in_gain_hbm,
    gate_hbm,
    up_hbm,
    down_hbm,
    out_gain_hbm,
    mixer_out,
    moe_out,
    pool_scale,
    mix_gain,
    routes,
    route_weights,
    in_gain,
    out_gain,
    pool,
    history,
    group_w,
    out_w,
    tokens,
    normed,
    raw,
    near_out,
    slot_rows,
    columns_of,
    outgoing,
    arrived,
    part,
    core_in,
    cross_in,
    returned,
    total_rows,
    gate,
    up,
    down,
    mix_held,
    mix_core,
    mix_sum,
    mix_cross,
    mix_done,
    local_sem,
    hist_sem,
    raw_send,
    raw_recv,
    dis_send,
    dis_recv,
    y1_send,
    y1_recv,
    c1_send,
    c1_recv,
    c2_send,
    c2_recv,
    y2_send,
    y2_recv,
    ret_send,
    ret_recv,
    m1_send,
    m1_recv,
    m2_send,
    m2_recv,
):
    ep_size, tp_size, rows, width = arrived.shape
    exp_dev, _, ff_dev = gate.shape
    tok_dev = tokens.shape[0]
    top_count = routes.shape[0]
    experts = exp_dev * ep_size
    rows_a = pool.shape[0]
    history_rows = history.shape[0]
    highs = tp_size // 2
    ep = lax.axis_index("ep")
    tp = lax.axis_index("tp")
    hi, lo = tp // 2, tp % 2
    other = 1 - lo

    def remote(src, dst, send, recv, to_ep, to_tp):
        return pltpu.make_async_remote_copy(
            src_ref=src,
            dst_ref=dst,
            send_sem=send,
            recv_sem=recv,
            device_id=(to_ep, to_tp),
            device_id_type=MESH,
        )

    def peer_high(k):
        return lax.rem(hi + k, highs)

    on_end = (ep // 2) % 2 == (ep // 4) % 2
    tabled = ep_size == 8

    def packed_at(table, i):
        words = []
        for begin in range(0, len(table), PER_WORD):
            piece = table[begin : begin + PER_WORD]
            words.append(sum(value << (CODE_BITS * at) for at, value in enumerate(piece)))
        word = jnp.int32(words[0])
        for at in range(1, len(words)):
            word = jnp.where(i >= at * PER_WORD, words[at], word)
        shift = CODE_BITS * lax.rem(i, PER_WORD)
        return lax.rem(lax.shift_right_logical(word, shift), 1 << CODE_BITS)

    def offset_of(i):
        far = jnp.where(i == 0, 1, ep_size - i)
        return jnp.where(i == ep_size - 1, 0, far)

    def sent_at(i):
        if tabled:
            return jnp.where(on_end, packed_at(END_SENDS, i), packed_at(MIDDLE_SENDS, i))
        return offset_of(i)

    def event_at(t):
        if tabled:
            code = jnp.where(on_end, packed_at(END_EVENTS, t), packed_at(MIDDLE_EVENTS, t))
            return code // 8, code % 8
        i, slot = t // 8, t % 8
        op, j = jnp.int32(NONE), i
        for at, (kind, lag, last) in enumerate(STEADY):
            index = i - lag
            valid = (slot == at) & (index >= 0) & (index < ep_size - last)
            op = jnp.where(valid, kind, op)
            j = jnp.where(valid, index, j)
        op = jnp.where((slot == 6) & (i == 0), MIX, op)
        return op, offset_of(j)

    def partner_ep(d):
        value = ep * 0
        bit = 1
        while bit < ep_size:
            value = value + bit * (((ep // bit) % 2 + (d // bit) % 2) % 2)
            bit *= 2
        return value

    def dispatch(d):
        peer = partner_ep(d)
        return remote(
            outgoing.at[peer], arrived.at[d, tp], dis_send.at[0], dis_recv.at[d], peer, tp
        )

    def gather_cross(d, k):
        slot = arrived.at[d, tp]
        return remote(
            slot, slot, y1_send.at[k - 1], y1_recv.at[d, highs - k - 1], ep, peer_high(k) * 2 + lo
        )

    def gather_cross_in(d, k):
        high = peer_high(k)
        slot = arrived.at[d, high * 2 + lo]
        return remote(slot, slot, y1_send.at[k - 1], y1_recv.at[d, k - 1], ep, high * 2 + lo)

    def gather_core(d, high):
        slot = arrived.at[d, high * 2 + lo]
        return remote(slot, slot, c1_send.at[0], c1_recv.at[d], ep, hi * 2 + other)

    def gather_core_in(d):
        slots = arrived.at[d, 0:highs]
        return remote(slots, slots, c1_send.at[0], c1_recv.at[d], ep, hi * 2 + other)

    def reduce_core(d, high):
        return remote(
            part.at[high * 2 + other],
            core_in.at[d, high],
            c2_send.at[0],
            c2_recv.at[d, high],
            ep,
            hi * 2 + other,
        )

    def reduce_core_all(d):
        return remote(
            part.at[0:highs],
            core_in.at[d],
            c2_send.at[0],
            c2_recv.at[d, 0],
            ep,
            hi * 2 + other,
        )

    def reduce_cross(d, k):
        high = peer_high(k)
        return remote(
            core_in.at[d, high],
            cross_in.at[d, highs - k - 1],
            y2_send.at[k - 1],
            y2_recv.at[d, highs - k - 1],
            ep,
            high * 2 + lo,
        )

    def reduce_cross_in(d, k):
        high = peer_high(k)
        return remote(
            core_in.at[d, high],
            cross_in.at[d, k - 1],
            y2_send.at[k - 1],
            y2_recv.at[d, k - 1],
            ep,
            high * 2 + lo,
        )

    def raw_copy(k):
        return remote(
            normed,
            raw.at[highs - k - 1],
            raw_send.at[k - 1],
            raw_recv.at[highs - k - 1],
            ep,
            peer_high(k) * 2 + lo,
        )

    def raw_copy_in(k):
        return remote(
            normed, raw.at[k - 1], raw_send.at[k - 1], raw_recv.at[k - 1], ep, peer_high(k) * 2 + lo
        )

    def near_copy(d, k):
        return remote(
            near_out.at[d, k - 1],
            arrived.at[d, peer_high(k) * 2 + lo],
            y1_send.at[k - 1],
            y1_recv.at[d, k - 1],
            partner_ep(d),
            tp,
        )

    def give_back(d):
        peer = partner_ep(d)
        return remote(core_in.at[d, hi], returned.at[d], ret_send.at[0], ret_recv.at[d], peer, tp)

    def mix_core_copy(high):
        return remote(
            mix_held.at[high * 2 + other],
            mix_core.at[high],
            m1_send.at[0],
            m1_recv.at[0],
            ep,
            hi * 2 + other,
        )

    def mix_core_all():
        return remote(
            mix_held.at[0:highs], mix_core, m1_send.at[0], m1_recv.at[0], ep, hi * 2 + other
        )

    def mix_cross_copy(k):
        high = peer_high(k)
        return remote(
            mix_sum.at[high],
            mix_cross.at[highs - k - 1],
            m2_send.at[k - 1],
            m2_recv.at[highs - k - 1],
            ep,
            high * 2 + lo,
        )

    def mix_cross_in(k):
        high = peer_high(k)
        return remote(
            mix_sum.at[high],
            mix_cross.at[k - 1],
            m2_send.at[k - 1],
            m2_recv.at[k - 1],
            ep,
            high * 2 + lo,
        )

    last_rows = pool.at[rows_a - history_rows :]
    send_history = remote(
        last_rows, history, hist_sem.at[0], hist_sem.at[1], jnp.minimum(ep + 1, ep_size - 1), tp
    )

    half_rows = mix_done.shape[0] // 2
    mixer_stores = [
        pltpu.make_async_copy(
            mix_done.at[half * half_rows : (half + 1) * half_rows],
            mixer_out.at[half * half_rows : (half + 1) * half_rows],
            local_sem.at[7 + half],
        )
        for half in range(2)
    ]
    moe_store = pltpu.make_async_copy(normed, moe_out, local_sem.at[15])
    tokens_copy = pltpu.make_async_copy(tokens_hbm, tokens, local_sem.at[0])
    pool_copy = pltpu.make_async_copy(pool_hbm, pool, local_sem.at[1])
    mixer_copies = [
        pltpu.make_async_copy(group_hbm, group_w, local_sem.at[2]),
        pltpu.make_async_copy(out_w_hbm, out_w, local_sem.at[3]),
    ]
    weight_copies = [
        pltpu.make_async_copy(gate_hbm, gate, local_sem.at[4]),
        pltpu.make_async_copy(up_hbm, up, local_sem.at[5]),
        pltpu.make_async_copy(down_hbm, down, local_sem.at[6]),
    ]

    early_copies = [
        pltpu.make_async_copy(routes_hbm, routes, local_sem.at[9]),
        pltpu.make_async_copy(route_weights_hbm, route_weights, local_sem.at[10]),
        pltpu.make_async_copy(in_gain_hbm, in_gain, local_sem.at[11]),
    ]
    mixer_copies += [
        pltpu.make_async_copy(pool_scale_hbm, pool_scale, local_sem.at[12]),
        pltpu.make_async_copy(mix_gain_hbm, mix_gain, local_sem.at[13]),
        pltpu.make_async_copy(out_gain_hbm, out_gain, local_sem.at[14]),
    ]
    tokens_copy.start()
    early_copies[2].start()
    barrier = pltpu.get_barrier_semaphore()

    def greet(d, carry):
        pl.semaphore_signal(barrier, inc=1, device_id=(partner_ep(d), tp), device_id_type=MESH)
        return carry

    lax.fori_loop(1, ep_size, greet, 0)
    for k in range(1, highs):
        pl.semaphore_signal(
            barrier, inc=1, device_id=(ep, peer_high(k) * 2 + lo), device_id_type=MESH
        )
    pl.semaphore_signal(barrier, inc=1, device_id=(ep, hi * 2 + other), device_id_type=MESH)
    for copy in early_copies[:2]:
        copy.start()
    pool_copy.start()


    expert_id = lax.broadcasted_iota(jnp.int32, (experts, tok_dev), 0)
    first_slot = (
        lax.div(expert_id, exp_dev) * rows + lax.rem(expert_id, exp_dev) * capacity
    ).astype(F32)
    earlier = (
        lax.broadcasted_iota(jnp.int32, (tok_dev, tok_dev), 0)
        < lax.broadcasted_iota(jnp.int32, (tok_dev, tok_dev), 1)
    ).astype(BF16)

    def tokens_of(index):
        return pl.ds(pl.multiple_of(index * tok_dev, tok_dev), tok_dev)

    def find_slots(index, base):
        block_routes = routes[:, tokens_of(index)]
        taken = jnp.zeros((experts, 1), F32)
        found = []
        for k in range(top_count):
            named = (block_routes[k : k + 1, :] == expert_id).astype(F32)
            before = jnp.dot(named.astype(BF16), earlier, preferred_element_type=F32)
            slot = jnp.sum(named * (before + taken + first_slot), axis=0, keepdims=True)
            taken = taken + jnp.sum(named, axis=1, keepdims=True)
            found.append(slot)
            slot_rows[base + k : base + k + 1, :] = slot.astype(jnp.int32)
        return found

    early_copies[2].wait()
    tokens_copy.wait()
    for copy in mixer_copies + weight_copies:
        copy.start()
    normed[...] = rms_scale(tokens[...].astype(F32), in_gain[...]).astype(BF16)
    pool_copy.wait()
    pl.semaphore_wait(barrier, ep_size - 1 + highs)
    if tabled:
        for k in range(1, highs):
            raw_copy(k).start()

    @pl.when(ep < ep_size - 1)
    def _():
        send_history.start()

    def routed_rows(owner, base, source):
        slot_id = lax.broadcasted_iota(jnp.int32, (rows, tok_dev), 0) + owner * rows
        chosen = slot_rows[base : base + 1, :] == slot_id
        for k in range(1, top_count):
            chosen = chosen | (slot_rows[base + k : base + k + 1, :] == slot_id)
        return jnp.dot(
            chosen.astype(F32).astype(BF16), source[...], preferred_element_type=F32
        ).astype(BF16)

    column_step = min(width, 512)

    def mixer_part():
        for copy in mixer_copies:
            copy.wait()

        @pl.when(ep > 0)
        def _():
            send_history.wait_recv()

        @pl.when(ep == 0)
        def _():
            history[...] = jnp.zeros(history.shape, BF16)

        values = pool[...].astype(F32)
        running = jnp.concatenate([history[...].astype(F32), values], axis=0)
        summed = None
        for group in range(tp_size):
            running = running + pltpu.roll(running, 2**group, 0)
            current = running[history_rows:]
            summed = current if summed is None else jnp.where(tp == group, current, summed)
        window = jnp.int32(1)
        for group in range(tp_size):
            window = jnp.where(tp == group, 2 ** (group + 1), window)
        position = ep * rows_a + lax.broadcasted_iota(jnp.int32, values.shape, 0)
        divisor = jnp.minimum(position + 1, window).astype(F32)
        pooled = (summed / divisor - values).astype(BF16)
        grouped = (
            jnp.dot(pooled, group_w[0], preferred_element_type=F32) * pool_scale[...]
        ).astype(BF16)
        mix_rows = rows_a // tp_size
        for start in range(0, width, column_step):
            columns = slice(start, start + column_step)
            mix_held[:, :, columns] = (
                jnp.dot(grouped, out_w[:, columns], preferred_element_type=F32)
                .astype(BF16)
                .reshape(tp_size, mix_rows, column_step)
            )
        for high in range(highs):
            mix_core_copy(high).start()
        mix_core_all().wait_recv()
        for high in range(highs):
            mix_sum[high] = (
                mix_held[high * 2 + lo].astype(F32) + mix_core[high].astype(F32)
            ).astype(BF16)
        for k in range(1, highs):
            mix_cross_copy(k).start()

    def stage_a(d):
        def cross():
            for k in range(1, highs):
                gather_cross(d, k).start()

        if tabled:
            pl.when(d >= NEAR)(cross)
        else:
            cross()
        gather_core(d, hi).start()

    def peer_blocks():
        for k in range(1, highs):
            base = k * top_count
            source = raw.at[k - 1]
            find_slots(peer_high(k) * 2 + lo, base)
            raw_copy_in(k).wait_recv()

            def send_near(d, carry):
                near_out[d, k - 1] = routed_rows(partner_ep(d), base, source)
                near_copy(d, k).start()
                return carry

            lax.fori_loop(1, NEAR, send_near, 0)
            arrived[0, peer_high(k) * 2 + lo] = routed_rows(ep, base, source)

    for copy in early_copies[:2]:
        copy.wait()
    slot_list = find_slots(tp, 0)

    def send_out(i, carry):
        d = sent_at(i)
        peer = partner_ep(d)
        outgoing[peer] = routed_rows(peer, 0, normed)
        dispatch(d).start()
        return carry

    lax.fori_loop(0, ep_size - 1, send_out, 0)
    arrived[0, tp] = routed_rows(ep, 0, normed)
    stage_a(jnp.int32(0))
    own_weights = route_weights[:, tokens_of(tp)]
    stacked = jnp.concatenate(
        slot_list
        + [own_weights[k : k + 1, :] for k in range(top_count)]
        + [jnp.zeros((columns_of.shape[1] - 2 * top_count, tok_dev), F32)],
        axis=0,
    )
    columns_of[...] = stacked.T

    def gather_next(d):
        dispatch(d).wait_recv()
        stage_a(d)

    if not tabled:
        gather_next(offset_of(ep * 0))
    for copy in weight_copies:
        copy.wait()
    total_rows[...] = jnp.zeros(total_rows.shape, F32)

    spans = []
    for e in range(exp_dev):
        begin = e * capacity // ROW_TILE * ROW_TILE
        end = -(-(e + 1) * capacity // ROW_TILE) * ROW_TILE
        spans.append((begin, end))
    edges = sorted({0, rows} | {edge for span in spans for edge in span})

    def experts_on(d):
        hidden = []
        for e, (begin, end) in enumerate(spans):
            count = end - begin
            block = arrived[d, :, begin:end, :].reshape(tp_size * count, width)
            gate_act = jnp.dot(block, gate[e], preferred_element_type=F32)
            up_act = jnp.dot(block, up[e], preferred_element_type=F32)
            act = gate_act / (1.0 + jnp.exp(-gate_act)) * up_act
            place = begin + lax.rem(
                lax.broadcasted_iota(jnp.int32, (tp_size * count, 1), 0), count
            )
            mine = (place >= e * capacity) & (place < (e + 1) * capacity)
            hidden.append(jnp.where(mine, act, 0.0).astype(BF16))
        for start in range(0, width, column_step):
            columns = slice(start, start + column_step)
            outs = []
            for e, (begin, end) in enumerate(spans):
                out = jnp.dot(hidden[e], down[e, :, columns], preferred_element_type=F32)
                outs.append(out.reshape(tp_size, end - begin, column_step))
            for begin, end in zip(edges[:-1], edges[1:]):
                piece = None
                for (first_row, last_row), out in zip(spans, outs):
                    if first_row <= begin and end <= last_row:
                        held = out[:, begin - first_row : end - first_row]
                        piece = held if piece is None else piece + held
                if piece is None:
                    piece = jnp.zeros((tp_size, end - begin, column_step), F32)
                part[:, begin:end, columns] = piece.astype(BF16)

    def combine(owner, block):
        lane = lax.broadcasted_iota(jnp.int32, (tok_dev, 2 * rows), 1)
        slot_id = (lax.rem(lane, rows) + owner * rows).astype(F32)
        weights = jnp.zeros((tok_dev, 2 * rows), F32)
        for k in range(top_count):
            weights = weights + jnp.where(
                columns_of[:, k : k + 1] == slot_id,
                columns_of[:, top_count + k : top_count + k + 1],
                0.0,
            )
        major = weights.astype(BF16).astype(F32)
        split = jnp.where(lane < rows, major, weights - major).astype(BF16)
        for start in range(0, width, column_step):
            columns = slice(start, start + column_step)
            held = block[:, columns]
            twice = jnp.concatenate([held, held], axis=0)
            total_rows[:, columns] += jnp.dot(split, twice, preferred_element_type=F32)

    def combine_from(d):
        give_back(d).wait_recv()
        combine(partner_ep(d), returned.at[d])

    def forward(d):
        for k in range(1, highs):

            def arrival():
                gather_cross_in(d, k).wait_recv()

            if tabled:
                pl.when(d != 0)(arrival)
            else:
                arrival()
            gather_core(d, peer_high(k)).start()

    def compute(d):
        gather_core_in(d).wait_recv()
        experts_on(d)
        for k in range(1, highs):
            reduce_core(d, peer_high(k)).start()
        reduce_core(d, hi).start()

    def reduce(d):
        def chip_total(high):
            reduce_core(d, high).wait_recv()
            core_in[d, high] = (
                part[high * 2 + lo].astype(F32) + core_in[d, high].astype(F32)
            ).astype(BF16)

        for k in range(1, highs):
            chip_total(peer_high(k))
            reduce_cross(d, k).start()
        chip_total(hi)
        reduce_core_all(d).wait_send()

    def send_home(d):
        total = core_in[d, hi].astype(F32)
        for k in range(1, highs):
            reduce_cross_in(d, k).wait_recv()
            total = total + cross_in[d, k - 1].astype(F32)
        core_in[d, hi] = total.astype(BF16)

        @pl.when(d != 0)
        def _():
            give_back(d).start()

    def mixer_end():
        for k in range(1, highs):
            mix_cross_in(k).wait_recv()
        for half, store in enumerate(mixer_stores):
            span = slice(half * half_rows, (half + 1) * half_rows)
            total = mix_sum[hi, span, :].astype(F32)
            for k in range(1, highs):
                total = total + mix_cross[k - 1, span, :].astype(F32)
            mix_done[span, :] = rms_scale(total, mix_gain[...]).astype(BF16)
            store.start()

    actions = {
        GATHER: gather_next,
        FORWARD: forward,
        COMPUTE: compute,
        REDUCE: reduce,
        RETURN: send_home,
        COMBINE: combine_from,
        MIX: lambda d: mixer_part(),
        PEER: lambda d: peer_blocks(),
    }

    if not tabled:
        del actions[PEER]

    def event(t, carry):
        op, d = event_at(t)
        for kind, action in actions.items():
            pl.when(op == kind)(functools.partial(action, d))
        return carry

    count = len(END_EVENTS) if tabled else 8 * (ep_size + 3)
    lax.fori_loop(0, count, event, 0)

    if not tabled:

        def late(j, carry):
            combine_from(offset_of(j))
            return carry

        lax.fori_loop(max(0, ep_size - 5), ep_size - 1, late, 0)
    combine(ep, core_in.at[0, hi])
    if tabled:
        for k in range(1, highs):
            raw_copy(k).wait_send()
    normed[...] = rms_scale(total_rows[...], out_gain[...]).astype(BF16)
    moe_store.start()

    mix_core_all().wait_send()

    @pl.when(ep < ep_size - 1)
    def _():
        send_history.wait_send()

    def drain(blocks, sem):
        remote(blocks, blocks, sem, dis_recv.at[0], ep, hi * 2 + other).wait_send()

    others = outgoing.at[0 : ep_size - 1]
    for k in range(1, highs):
        drain(others if tabled else outgoing, y1_send.at[k - 1])
        drain(outgoing, y2_send.at[k - 1])
    drain(core_in, c1_send.at[0])
    drain(others, dis_send.at[0])
    drain(others, ret_send.at[0])
    mixer_end()
    for k in range(1, highs):
        mix_cross_copy(k).wait_send()
    moe_store.wait()
    for store in mixer_stores:
        store.wait()


def on_device(
    pool_input,
    group_weight,
    pool_scale,
    out_weight,
    mix_gain,
    expert_input,
    routes,
    route_weights,
    moe_in_gain,
    gate_weight,
    up_weight,
    down_weight,
    moe_out_gain,
):
    tp_size = lax.axis_size("tp")
    ep_size = lax.axis_size("ep")
    rows_a, group_width = pool_input.shape
    width = out_weight.shape[1]
    exp_dev = gate_weight.shape[0]
    experts = exp_dev * ep_size
    tok_dev = expert_input.shape[0]
    top_count = routes.shape[1]
    capacity = max(2, 5 * tok_dev * top_count // (4 * experts))
    rows = -(-exp_dev * capacity // ROW_TILE) * ROW_TILE
    highs = tp_size // 2
    mix_rows = rows_a // tp_size
    history_rows = 2**tp_size
    tabled = ep_size == 8
    raw_rows = tok_dev if tabled else ROW_TILE
    near_rows = rows if tabled else ROW_TILE
    any_spec = pl.BlockSpec(memory_space=pl.ANY)
    hbm_spec = pl.BlockSpec(memory_space=pltpu.HBM)
    dma = pltpu.SemaphoreType.DMA
    flops = 6 * gate_weight.size * ep_size * tp_size * rows
    scratch = [
        pltpu.VMEM((1, group_width), F32),
        pltpu.VMEM((1, width), F32),
        pltpu.VMEM((top_count, tok_dev * tp_size), jnp.int32),
        pltpu.VMEM((top_count, tok_dev * tp_size), F32),
        pltpu.VMEM((1, width), F32),
        pltpu.VMEM((1, width), F32),
        pltpu.VMEM(pool_input.shape, BF16),
        pltpu.VMEM((history_rows, group_width), BF16),
        pltpu.VMEM(group_weight.shape, BF16),
        pltpu.VMEM(out_weight.shape, BF16),
        pltpu.VMEM(expert_input.shape, BF16),
        pltpu.VMEM(expert_input.shape, BF16),
        pltpu.VMEM((highs - 1, raw_rows, width), BF16),
        pltpu.VMEM((NEAR, highs - 1, near_rows, width), BF16),
        pltpu.VMEM((8, tok_dev), jnp.int32),
        pltpu.VMEM((tok_dev, 8), F32),
        pltpu.VMEM((ep_size, rows, width), BF16),
        pltpu.VMEM((ep_size, tp_size, rows, width), BF16),
        pltpu.VMEM((tp_size, rows, width), BF16),
        pltpu.VMEM((ep_size, highs, rows, width), BF16),
        pltpu.VMEM((ep_size, highs - 1, rows, width), BF16),
        pltpu.VMEM((ep_size, rows, width), BF16),
        pltpu.VMEM(expert_input.shape, F32),
        pltpu.VMEM(gate_weight.shape, BF16),
        pltpu.VMEM(up_weight.shape, BF16),
        pltpu.VMEM(down_weight.shape, BF16),
        pltpu.VMEM((tp_size, mix_rows, width), BF16),
        pltpu.VMEM((highs, mix_rows, width), BF16),
        pltpu.VMEM((highs, mix_rows, width), BF16),
        pltpu.VMEM((highs - 1, mix_rows, width), BF16),
        pltpu.VMEM((mix_rows, width), BF16),
        dma((16,)),
        dma((2,)),
        dma((highs - 1,)),
        dma((highs - 1,)),
        dma((1,)),
        dma((ep_size,)),
        dma((highs - 1,)),
        dma((ep_size, highs - 1)),
        dma((1,)),
        dma((ep_size,)),
        dma((1,)),
        dma((ep_size, highs)),
        dma((highs - 1,)),
        dma((ep_size, highs - 1)),
        dma((1,)),
        dma((ep_size,)),
        dma((1,)),
        dma((1,)),
        dma((highs - 1,)),
        dma((highs - 1,)),
    ]
    held = sum(
        ref.dtype.itemsize * math.prod(ref.shape)
        for ref in scratch
        if ref.memory_space == pltpu.VMEM
    )
    mixer_out, moe_out = pl.pallas_call(
        functools.partial(fused_kernel, capacity),
        out_shape=(
            pltpu.VMEM((mix_rows, width), BF16),
            pltpu.VMEM((tok_dev, width), BF16),
        ),
        in_specs=[hbm_spec] * 13,
        out_specs=(any_spec, any_spec),
        scratch_shapes=scratch,
        compiler_params=pltpu.CompilerParams(
            collective_id=0, has_side_effects=True, vmem_limit_bytes=max(ROOM, held + SPARE)
        ),
        cost_estimate=pl.CostEstimate(
            flops=flops, bytes_accessed=8 * expert_input.size, transcendentals=0
        ),
    )(
        pool_input,
        group_weight,
        pool_scale.reshape(1, -1),
        out_weight,
        mix_gain.reshape(1, -1),
        expert_input,
        routes.T,
        route_weights.T,
        moe_in_gain.reshape(1, -1),
        gate_weight,
        up_weight,
        down_weight,
        moe_out_gain.reshape(1, -1),
    )
    return (mixer_out, moe_out)


def solution(mesh):
    in_specs = (
        P("ep", "tp"),
        P("tp", None, None),
        P("tp"),
        P("tp", None),
        P(),
        P(("ep", "tp"), None),
        P("ep", None),
        P("ep", None),
        P(),
        P("ep", None, "tp"),
        P("ep", None, "tp"),
        P("ep", "tp", None),
        P(),
    )
    out_specs = (P(("ep", "tp"), None), P(("ep", "tp"), None))
    return jax.shard_map(
        on_device, mesh=mesh, in_specs=in_specs, out_specs=out_specs, check_vma=False
    )
```
